32 devices in a mesh: sp: 16 (over z, y, x), tp: 2 (over core).
Axes of the slice: x: 2, y: 2, z: 4, core: 2. Of those that a mesh axis runs over, the one named last changes fastest.
Arguments:
- queries_small: bfloat16 [4096, 1024], P('sp', 'tp'), may hold values from -160 to 160
- queries_large: bfloat16 [4096, 1024], P('sp', 'tp'), may hold values from -160 to 160
- kv_small: bfloat16 [4096, 128], P('sp'), may hold values from -4 to 4
- kv_large: bfloat16 [4096, 256], P('sp'), may hold values from -4 to 4
- cum_small: float32 [16, 4096], P('tp', 'sp'), may hold values from -514 to 0, as said below
- cum_large: float32 [8, 4096], P('tp', 'sp'), may hold values from -514 to 0, as said below
- residual: bfloat16 [4096, 2048], P(('sp', 'tp')), may hold values from -6 to 6
- out_small: bfloat16 [1024, 2048], replicated, may hold values from -0.125 to 0.125
- out_large: bfloat16 [1024, 2048], replicated, may hold values from -0.125 to 0.125
- gain_mix: float32 [2048], replicated, may hold values from 0.1 to 1.9
- gain_route: float32 [2048], replicated, may hold values from 0.1 to 1.9
- gain_blend: float32 [2048], replicated, may hold values from 0.1 to 1.9
- w_gate: bfloat16 [32, 2048, 1024], P(('sp', 'tp')), may hold values from -0.125 to 0.125
- w_up: bfloat16 [32, 2048, 1024], P(('sp', 'tp')), may hold values from -0.125 to 0.125
- w_down: bfloat16 [32, 1024, 2048], P(('sp', 'tp')), may hold values from -0.1875 to 0.1875
- route: int32 [2, 4096], P(None, ('sp', 'tp')), may hold values from 0 to 31, as said below
- route_bias: float32 [4096], P(('sp', 'tp')), may hold values from -6 to 6
Outputs:
- result: bfloat16 [4096, 2048], P(('sp', 'tp'))
The draws below stay inside these ranges and needn't reach their ends.
Inputs may be any that keep to these rules, and one draw needn't show every extreme that they name: `cum_small`: each row is non-increasing along positions. `cum_large`: each row is non-increasing along positions. route[0, t] and route[1, t] are different experts of the same group of 8 consecutive experts. Among the 128 positions of one device (aligned blocks), no expert is named by more than 16 of them; in every draw all experts of one group are named by exactly 16 positions of every device. Within one device's positions the loads of the experts of one group differ by at most 2.
All inputs are finite; a program needn't handle non-finite values.
Results may differ from the reference program's by a relative error of at most 0.014.
Values may be sent and summed in bfloat16 or wider, within the bound.
A program may use at most 128 MiB of HBM per device.

```python
import math
import jax
import jax.numpy as jnp
from jax import lax

D = 2048
HA = 16
DA = 64
HB = 8
DB = 128
FF = 1024
GROUPS = 4
TOK_DEV = 256
SEQUENCE_TOKENS = 4096
ROWS_DEV = 128
EXPERTS = 32
EPG = 8
CAP = 16
N_SP = 16
N_TP = 2


def shared_keys(root_random_key, head_size):
    return jnp.clip(jax.random.normal(jax.random.fold_in(root_random_key, 5), (SEQUENCE_TOKENS, head_size), jnp.float32), -4.0, 4.0)


def key_value_rows(key, label, head_size):
    root_random_key = jax.random.fold_in(key, label)
    key_rows = shared_keys(root_random_key, head_size)
    value_rows = jnp.clip(jax.random.normal(jax.random.fold_in(root_random_key, 6), (SEQUENCE_TOKENS, head_size), jnp.float32), -4.0, 4.0)
    return jnp.concatenate([key_rows, value_rows], axis=1).astype(jnp.bfloat16)


def query_rows(key, label, head_count, head_size):
    root_random_key = jax.random.fold_in(key, label)
    drawn = jnp.clip(jax.random.normal(jax.random.fold_in(root_random_key, 9), (SEQUENCE_TOKENS, head_count * head_size), jnp.float32), -4.0, 4.0)
    return drawn.astype(jnp.bfloat16)


def gate_totals(key, label, head_count):
    root_random_key = jax.random.fold_in(key, label)
    order = jax.random.permutation(jax.random.fold_in(root_random_key, 1), head_count)
    slow_heads = order < head_count // 2
    slow_total = jnp.exp(jax.random.uniform(jax.random.fold_in(root_random_key, 3), (head_count,), jnp.float32, math.log(0.8), math.log(1.6)))
    fast_rate = jnp.exp(jax.random.uniform(jax.random.fold_in(root_random_key, 4), (head_count,), jnp.float32, math.log(0.01), math.log(1.0 / 30.0)))
    rates = jnp.where(slow_heads, slow_total / SEQUENCE_TOKENS, fast_rate)
    factors = jnp.exp(jax.random.uniform(jax.random.fold_in(root_random_key, 5), (SEQUENCE_TOKENS // TOK_DEV,), jnp.float32, math.log(0.5), math.log(2.0)))
    factors = jnp.repeat(factors, TOK_DEV)
    rough = jax.random.uniform(jax.random.fold_in(root_random_key, 6), (head_count, SEQUENCE_TOKENS), jnp.float32, 0.5, 1.5)
    gate_logarithms = -rates[:, None] * factors[None, :] * rough
    spike_position = jax.random.randint(jax.random.fold_in(root_random_key, 7), (3,), 0, SEQUENCE_TOKENS)
    spike_penalty = jax.random.uniform(jax.random.fold_in(root_random_key, 8), (3,), jnp.float32, 0.2, 0.4)
    spot_locations = jnp.arange(SEQUENCE_TOKENS, dtype=jnp.int32)
    spike_events = jnp.sum(jnp.where(spot_locations[None, :] == spike_position[:, None], jnp.log(1.0 - spike_penalty)[:, None], 0.0), axis=0)
    gate_logarithms = gate_logarithms + spike_events[None, :]
    return jnp.cumsum(gate_logarithms, axis=1).astype(jnp.float32)


def draw_queries_small(key, part):
    return query_rows(key, 11, HA, DA)


def draw_queries_large(key, part):
    return query_rows(key, 13, HB, DB)


def draw_kv_small(key, part):
    return key_value_rows(key, 11, DA)


def draw_kv_large(key, part):
    return key_value_rows(key, 13, DB)


def draw_cum_small(key, part):
    return gate_totals(key, 31, HA)


def draw_cum_large(key, part):
    return gate_totals(key, 33, HB)


def draw_route(key, part):
    block_count = SEQUENCE_TOKENS // ROWS_DEV
    full_group = jax.random.randint(jax.random.fold_in(key, 21), (), 0, GROUPS)

    def one_block(block_index):
        block_key = jax.random.fold_in(jax.random.fold_in(key, 22), block_index)
        order = jax.random.permutation(jax.random.fold_in(block_key, 1), ROWS_DEV)
        spot_locations = jnp.arange(ROWS_DEV, dtype=jnp.int32)
        others = jax.random.randint(jax.random.fold_in(block_key, 2), (ROWS_DEV,), 0, GROUPS - 1)
        group_at = jnp.where(spot_locations < ROWS_DEV // 2, full_group, (full_group + 1 + others) % GROUPS)
        marked = (group_at[:, None] == jnp.arange(GROUPS, dtype=jnp.int32)[None, :]).astype(jnp.int32)
        ranked = jnp.sum((jnp.cumsum(marked, axis=0) - 1) * marked, axis=1)
        shifts = jax.random.randint(jax.random.fold_in(block_key, 3), (GROUPS,), 0, EPG)
        offset = ranked + shifts[group_at]
        first_inner = offset % EPG
        second_inner = (offset + 1 + ranked // EPG % (EPG - 1)) % EPG
        chosen = jnp.stack([group_at * EPG + first_inner, group_at * EPG + second_inner]).astype(jnp.int32)
        return jnp.zeros((2, ROWS_DEV), jnp.int32).at[:, order].set(chosen)
    blocks = jax.vmap(one_block)(jnp.arange(block_count, dtype=jnp.int32))
    return blocks.transpose(1, 0, 2).reshape(2, SEQUENCE_TOKENS)


def block_scale(key, extent, split, low, largest):
    gain = 1.0
    for position, shards_of in split:
        steps = jax.random.uniform(jax.random.fold_in(jax.random.fold_in(key, 6), position), (shards_of,), jnp.float32, low / len(split), largest / len(split))
        gain = gain * jnp.repeat(jnp.exp(steps), extent[position] // shards_of).reshape((-1,) + (1,) * (len(extent) - 1 - position))
    return gain


def noise(rng, dims, deviation, limit, split=(), kind=jnp.bfloat16):
    array = jax.random.normal(rng, dims, jnp.float32) * deviation
    if len(split) > 0:
        array = block_scale(rng, dims, split, -0.22, 0.18) * array
    return jnp.clip(array, min=-limit, max=limit).astype(kind)


def setup_inputs(seed: int = 0) -> dict:
    streams_of = jax.random.split(jax.random.key(seed), 18)
    return {
        "queries_small": draw_queries_small(jax.random.fold_in(streams_of[17], 71), 0),
        "queries_large": draw_queries_large(jax.random.fold_in(streams_of[17], 71), 0),
        "kv_small": draw_kv_small(jax.random.fold_in(streams_of[17], 71), 0),
        "kv_large": draw_kv_large(jax.random.fold_in(streams_of[17], 71), 0),
        "cum_small": draw_cum_small(jax.random.fold_in(streams_of[17], 71), 0),
        "cum_large": draw_cum_large(jax.random.fold_in(streams_of[17], 71), 0),
        "residual": noise(streams_of[6], (SEQUENCE_TOKENS, D), 1.0, 6.0, ((0, 32),)),
        "out_small": noise(streams_of[7], (HA * DA, D), D ** -0.5, 0.125),
        "out_large": noise(streams_of[8], (HB * DB, D), D ** -0.5, 0.125),
        "gain_mix": jnp.clip(1.0 + 0.18 * jax.random.normal(streams_of[9], (D,), jnp.float32), 0.1, 1.9),
        "gain_route": jnp.clip(1.0 + 0.18 * jax.random.normal(streams_of[10], (D,), jnp.float32), 0.1, 1.9),
        "gain_blend": jnp.clip(1.0 + 0.18 * jax.random.normal(streams_of[11], (D,), jnp.float32), 0.1, 1.9),
        "w_gate": noise(streams_of[12], (EXPERTS, D, FF), D ** -0.5, 0.125, ((0, 32),)),
        "w_up": noise(streams_of[13], (EXPERTS, D, FF), D ** -0.5, 0.125, ((0, 32),)),
        "w_down": noise(streams_of[14], (EXPERTS, FF, D), FF ** -0.5, 0.1875, ((0, 32),)),
        "route": draw_route(jax.random.fold_in(streams_of[17], 71), 0),
        "route_bias": noise(streams_of[16], (SEQUENCE_TOKENS,), 1.5, 6.0, ((0, 32),), jnp.float32),
    }


norm_eps = 1e-06

def rms_scale(values, gain_row):
    return values * lax.rsqrt(lax.optimization_barrier(jnp.mean(values * values, axis=-1, keepdims=True)) + norm_eps) * gain_row.astype(jnp.float32)

def attend_group(queries, keys_values, cumulative, head_count, head_size):
    key_rows = keys_values[:, :head_size].astype(jnp.float32)
    value_rows = keys_values[:, head_size:].astype(jnp.float32)
    block_rows = min(256, SEQUENCE_TOKENS)
    block_count = SEQUENCE_TOKENS // block_rows
    query_blocks = queries.reshape(block_count, block_rows, head_count, head_size)
    cum_blocks = cumulative.reshape(head_count, block_count, block_rows).transpose(1, 0, 2)
    key_pos = jnp.arange(SEQUENCE_TOKENS, dtype=jnp.int32)

    def one_block(inputs):
        query_block, cum_block, block_index = inputs
        scores = jnp.einsum('qhd,kd->hqk', query_block.astype(jnp.float32), key_rows) * head_size ** (-0.5)
        scores = scores + cum_block[:, :, None] - cumulative[:, None, :]
        query_pos = block_index * block_rows + jnp.arange(block_rows, dtype=jnp.int32)
        allowed = key_pos[None, None, :] <= query_pos[None, :, None]
        scores = jnp.where(allowed, scores, -jnp.inf)
        row_max = lax.optimization_barrier(jnp.max(scores, axis=-1, keepdims=True))
        weights = jnp.where(allowed, jnp.exp(scores - row_max), 0.0)
        rounded = lax.optimization_barrier(weights.astype(jnp.bfloat16)).astype(jnp.float32)
        numerator = jnp.einsum('hqk,kd->qhd', rounded, value_rows)
        denominator = lax.optimization_barrier(jnp.sum(weights, axis=-1)).T
        return (numerator / denominator[:, :, None]).astype(jnp.bfloat16)
    outputs = lax.map(one_block, (query_blocks, cum_blocks, jnp.arange(block_count, dtype=jnp.int32)))
    return outputs.reshape(SEQUENCE_TOKENS, head_count * head_size)

def reference(queries_small, queries_large, kv_small, kv_large, cum_small, cum_large, residual, out_small, out_large, gain_mix, gain_route, gain_blend, w_gate, w_up, w_down, route, route_bias):
    attn_small = attend_group(queries_small, kv_small, cum_small, HA, DA)
    attn_large = attend_group(queries_large, kv_large, cum_large, HB, DB)
    mixer_out = jnp.dot(attn_small, out_small, preferred_element_type=jnp.float32) + jnp.dot(attn_large, out_large, preferred_element_type=jnp.float32)
    mixed = (residual.astype(jnp.float32) + rms_scale(mixer_out, gain_mix)).astype(jnp.bfloat16)
    routed = rms_scale(mixed.astype(jnp.float32), gain_route).astype(jnp.bfloat16)
    flat_ids = route.reshape(-1)
    most_rows = N_SP * N_TP * CAP

    def one_expert(carried, inputs):
        expert_id, gate_w, up_w, down_w = inputs
        matches = flat_ids == expert_id
        picked = jnp.nonzero(matches, size=most_rows, fill_value=0)[0].astype(jnp.int32)
        valid_rows = jnp.arange(most_rows, dtype=jnp.int32) < jnp.sum(matches.astype(jnp.int32))
        expert_rows = routed[picked % SEQUENCE_TOKENS]
        gate_pre = jnp.dot(expert_rows, gate_w, preferred_element_type=jnp.float32)
        up_pre = jnp.dot(expert_rows, up_w, preferred_element_type=jnp.float32)
        hidden = (jax.nn.silu(gate_pre) * up_pre).astype(jnp.bfloat16)
        expert_out = jnp.dot(hidden, down_w, preferred_element_type=jnp.float32).astype(jnp.bfloat16)
        masked = jnp.where(valid_rows[:, None], expert_out.astype(jnp.float32), 0.0)
        return (carried.at[picked].add(masked), None)
    outputs, _ = lax.scan(one_expert, jnp.zeros((2 * SEQUENCE_TOKENS, D), jnp.float32), (jnp.arange(EXPERTS, dtype=jnp.int32), w_gate, w_up, w_down))
    blended = jax.nn.sigmoid(route_bias)[:, None] * outputs[:SEQUENCE_TOKENS] + jax.nn.sigmoid(-route_bias)[:, None] * outputs[SEQUENCE_TOKENS:]
    return (mixed.astype(jnp.float32) + rms_scale(blended, gain_blend)).astype(jnp.bfloat16)
```

```python
import functools
import math

import jax
import jax.numpy as jnp
from jax import lax
from jax.experimental import pallas as pl
from jax.experimental.pallas import tpu as pltpu
from jax.sharding import PartitionSpec as P

norm_eps = 1e-06
far_score = -1e30
log2e = math.log2(math.e)
MESH = pl.DeviceIdType.MESH


def rms_scale(values, gain_row):
    return (
        values * lax.rsqrt(jnp.mean(values * values, axis=-1, keepdims=True) + norm_eps) * gain_row
    )


def mesh_shape(mesh):
    coords = [tuple(device.coords) for device in mesh.devices.reshape(-1)]
    return tuple(1 + max(c[axis] for c in coords) - min(c[axis] for c in coords) for axis in (2, 1, 0))


def bf16_pieces(values):
    high = values.astype(jnp.bfloat16)
    rest = values - high.astype(jnp.float32)
    middle = rest.astype(jnp.bfloat16)
    low = (rest - middle.astype(jnp.float32)).astype(jnp.bfloat16)
    return [high.astype(jnp.float32), middle.astype(jnp.float32), low.astype(jnp.float32)]


def round_up(value, unit):
    return -(-value // unit) * unit


def mix_kernel(
    dims, head_shape,
    q_small, q_large, kv_small, kv_large, cum_small, cum_large, residual, gain_mix, gain_route, out_small, out_large,
    mixed_ref, routed_ref,
    table, cums, qs, ql, top, total, acc_s, acc_l, stage, whole, weights, mixer,
    send_far, send_near, send_core, recv_kv, recv_cum, recv_core, swap_send, swap_recv, load_sem,
):
    heads_small, heads_large, size_small, size_large = head_shape
    depth, rows_y, rows_x = dims
    plane = rows_y * rows_x
    me = lax.axis_index("sp")
    core = lax.axis_index("tp")
    mine_z = me // plane
    mine_y = me % plane // rows_x
    mine_x = me % rows_x
    tokens = q_small.shape[0]
    heads = heads_small + heads_large
    extra_s = round_up(3 * heads_small, 32)
    extra_l = round_up(3 * heads_large, 16)
    wire = 2 * size_small + 2 * size_large
    half = wire // 2
    small_v = extra_s + size_small
    large_v = small_v + size_small
    large_k = large_v + size_large
    gate_l = extra_s + wire

    loads = (
        pltpu.make_async_copy(out_small, weights.at[pl.ds(0, out_small.shape[0])], load_sem.at[0]),
        pltpu.make_async_copy(
            out_large, weights.at[pl.ds(out_small.shape[0], out_large.shape[0])], load_sem.at[1]),
    )
    for load in loads:
        load.start()
    barrier = pltpu.get_barrier_semaphore()
    for step in range(1, depth):
        target = (mine_z + step) % depth * plane + me % plane
        pl.semaphore_signal(barrier, inc=1, device_id=(target, core), device_id_type=MESH)
    for step in range(1, rows_y):
        target = mine_z * plane + (mine_y + step) % rows_y * rows_x + mine_x
        pl.semaphore_signal(barrier, inc=1, device_id=(target, core), device_id_type=MESH)
    for step in range(1, rows_x):
        target = mine_z * plane + mine_y * rows_x + (mine_x + step) % rows_x
        pl.semaphore_signal(barrier, inc=1, device_id=(target, core), device_id_type=MESH)
    pl.semaphore_signal(barrier, inc=1, device_id=(me, 1 - core), device_id_type=MESH)

    def turned(block):
        width = block.shape[1]
        eye = jnp.where(
            lax.broadcasted_iota(jnp.int32, (width, width), 0) == lax.broadcasted_iota(jnp.int32, (width, width), 1),
            1.0, 0.0).astype(jnp.bfloat16)
        return lax.dot_general(
            eye, block, (((1,), (1,)), ((), ())), preferred_element_type=jnp.float32).astype(jnp.bfloat16)

    table[me, extra_s:large_v, :] = turned(kv_small[...])
    table[me, large_k:gate_l, :] = turned(kv_large[:, :size_large])
    table[me, large_v:large_k, :] = turned(kv_large[:, size_large:])
    cums[me, :heads_small] = cum_small[...]
    cums[me, heads_small:heads] = cum_large[...]

    lanes_s = lax.broadcasted_iota(jnp.int32, (tokens, extra_s), 1)
    lanes_l = lax.broadcasted_iota(jnp.int32, (tokens, extra_l), 1)
    for h in range(heads_small):
        picks = jnp.where((lanes_s % heads_small == h) & (lanes_s < 3 * heads_small), 1.0, 0.0)
        qs[h] = jnp.concatenate(
            [picks.astype(jnp.bfloat16), q_small[:, h * size_small:(h + 1) * size_small]], axis=1)
    for h in range(heads_large):
        picks = jnp.where((lanes_l % heads_large == h) & (lanes_l < 3 * heads_large), 1.0, 0.0)
        ql[h] = jnp.concatenate(
            [q_large[:, h * size_large:(h + 1) * size_large], picks.astype(jnp.bfloat16)], axis=1)
    pl.semaphore_wait(barrier, depth - 1 + rows_y - 1 + rows_x - 1 + 1)

    def place(behind, off_y, off_x):
        return (mine_z - behind) * plane + (mine_y + off_y) % rows_y * rows_x + (mine_x + off_x) % rows_x

    def copies(shard, target, sems):
        part = table.at[shard, pl.ds(extra_s + core * half, half)]
        return (
            pltpu.make_async_remote_copy(
                src_ref=part, dst_ref=part, send_sem=sems.at[0], recv_sem=recv_kv.at[shard],
                device_id=(target, core), device_id_type=MESH),
            pltpu.make_async_remote_copy(
                src_ref=cums.at[shard], dst_ref=cums.at[shard], send_sem=sems.at[1],
                recv_sem=recv_cum.at[shard], device_id=(target, core), device_id_type=MESH),
        )

    def start(shard, target, sems):
        for copy in copies(shard, target, sems):
            copy.start()

    def across(shard, which):
        part = table.at[shard, pl.ds(extra_s + which * half, half)]
        return pltpu.make_async_remote_copy(
            src_ref=part, dst_ref=part, send_sem=send_core.at[shard], recv_sem=recv_core.at[shard],
            device_id=(me, 1 - core), device_id_type=MESH)

    def arrived(shard):
        for copy in copies(shard, me, send_far.at[0]):
            copy.wait_recv()
        across(shard, core).start()

    near_y = rows_y - 1
    near_x = rows_x - 1
    near = near_y + near_x

    def both_ways(behind):
        shard = place(behind, 0, 0)
        for step in range(1, rows_x):
            yield shard, place(0, 0, step), near_y + step - 1
        for step in range(1, rows_y):
            yield shard, place(0, step, 0), step - 1

    def onward(behind, first_axis):
        if first_axis == "y":
            for step_a in range(1, rows_y):
                for step_b in range(1, rows_x):
                    yield place(behind, step_a, 0), place(0, 0, step_b), near + (step_a - 1) * near_x + step_b - 1
        else:
            for step_a in range(1, rows_x):
                for step_b in range(1, rows_y):
                    yield place(behind, 0, step_a), place(0, step_b, 0), near + (step_a - 1) * near_y + step_b - 1

    def column(behind):
        if not isinstance(behind, int):
            arrived(place(behind, 0, 0))
        for shard, target, slot in both_ways(behind):
            start(shard, target, send_near.at[behind, slot])

    def neighbours(behind):
        def along(first_axis):
            waited = []
            for shard, target, slot in onward(behind, first_axis):
                key = slot
                inner = (rows_x if first_axis == "y" else rows_y) - 1
                if (slot - near) % inner == 0:
                    arrived(shard)
                start(shard, target, send_near.at[behind, slot])
            if first_axis == "y":
                if near_x == 0:
                    for step in range(1, rows_y):
                        arrived(place(behind, step, 0))
                for step in range(1, rows_x):
                    arrived(place(behind, 0, step))
            else:
                if near_y == 0:
                    for step in range(1, rows_x):
                        arrived(place(behind, 0, step))
                for step in range(1, rows_y):
                    arrived(place(behind, step, 0))

        pl.when(core == 0)(functools.partial(along, "y"))
        pl.when(core == 1)(functools.partial(along, "x"))

    def corners(behind):
        for off_y in range(1, rows_y):
            for off_x in range(1, rows_x):
                arrived(place(behind, off_y, off_x))

    def far(step):
        return copies(me, (mine_z + step) * plane + me % plane, send_far.at[step])

    column(0)
    for step in range(1, depth):

        def send_up(step=step):
            for copy in far(step):
                copy.start()

        pl.when(mine_z + step < depth)(send_up)

    def attend(shard, own):
        gates = cums[shard]
        picked = bf16_pieces(gates[:heads_small] * (-math.sqrt(size_small)))
        if extra_s > 3 * heads_small:
            picked.append(jnp.zeros((extra_s - 3 * heads_small, tokens), jnp.float32))
        table[shard, :extra_s, :] = jnp.concatenate(picked, axis=0).astype(jnp.bfloat16)
        picked = bf16_pieces(gates[heads_small:heads] * (-math.sqrt(size_large)))
        if extra_l > 3 * heads_large:
            picked.append(jnp.zeros((extra_l - 3 * heads_large, tokens), jnp.float32))
        table[shard, gate_l:, :] = jnp.concatenate(picked, axis=0).astype(jnp.bfloat16)
        for h in range(heads):
            small = h < heads_small
            size = size_small if small else size_large
            scale = size ** (-0.5) * log2e
            query = qs[h] if small else ql[h - heads_small]
            keys = table[shard, :small_v, :] if small else table[shard, large_k:, :]
            values = table[shard, small_v:large_v, :] if small else table[shard, large_v:large_k, :]
            acc_ref, number = (acc_s, h) if small else (acc_l, h - heads_small)
            scores = jnp.dot(query, keys, preferred_element_type=jnp.float32)
            if own:
                key_pos = lax.broadcasted_iota(jnp.int32, (tokens, tokens), 1)
                query_pos = lax.broadcasted_iota(jnp.int32, (tokens, tokens), 0)
                scores = jnp.where(key_pos <= query_pos, scores, far_score)
            parts = [scores[:, j * 128:(j + 1) * 128] for j in range(tokens // 128)]
            newest = jnp.max(functools.reduce(jnp.maximum, parts), axis=-1, keepdims=True)
            if own:
                newest = jnp.broadcast_to(newest, (tokens, 128))
            else:
                before = top[h]
                newest = jnp.maximum(before, newest)
                factor = jnp.exp2((before - newest) * scale)
            scaled = newest * scale
            found = [jnp.exp2(part * scale - scaled) for part in parts]
            partial_sum = functools.reduce(jnp.add, found)
            product = lax.dot_general(
                jnp.concatenate(found, axis=1).astype(jnp.bfloat16), values,
                (((1,), (1,)), ((), ())), preferred_element_type=jnp.float32)
            top[h] = newest
            if own:
                total[h] = partial_sum
                acc_ref[number] = product
            else:
                total[h] = total[h] * factor + partial_sum
                acc_ref[number] = acc_ref[number] * factor[:, :size] + product

    attend(me, True)
    pl.when(mine_z >= 1)(lambda: column(jnp.int32(1)))
    neighbours(0)
    order = [(0, 0)] + [(step, 0) for step in range(1, rows_y)] + [(0, step) for step in range(1, rows_x)]
    order += [(a, b) for a in range(1, rows_y) for b in range(1, rows_x)]

    def step_of(number, _):
        behind = number // plane
        turn = number % plane
        pl.when((turn == 0) & (behind + 1 <= mine_z))(lambda: column(behind + 1))
        pl.when(turn == min(2, plane - 1))(lambda: corners(behind))
        pl.when((turn == plane - 1) & (behind + 1 <= mine_z))(lambda: neighbours(behind + 1))
        off_y = jnp.int32(0)
        off_x = jnp.int32(0)
        for index, (a, b) in enumerate(order):
            off_y = jnp.where(turn == index, a, off_y)
            off_x = jnp.where(turn == index, b, off_x)
        shard = place(behind, off_y, off_x)
        across(shard, 1 - core).wait_recv()
        pl.when(shard < me)(lambda: attend(shard, False))
        return 0

    lax.fori_loop(1, (mine_z + 1) * plane, step_of, 0)

    keep = tokens // 2
    width_s = heads_small * size_small
    width_l = heads_large * size_large
    for mine in (False, True):
        rows = pl.ds(pl.multiple_of((core if mine else 1 - core) * keep, keep), keep)
        columns = []
        for h in range(heads):
            small = h < heads_small
            sums = jnp.sum(total[h, rows, :], axis=-1, keepdims=True)
            values = acc_s[h, rows, :] if small else acc_l[h - heads_small, rows, :]
            columns.append((values / sums).astype(jnp.bfloat16))
        joined_s = jnp.concatenate(columns[:heads_small], axis=1)
        joined_l = jnp.concatenate(columns[heads_small:], axis=1)
        if mine:
            whole[:, pl.ds(pl.multiple_of(core * width_s, 128), width_s)] = joined_s
            whole[:, pl.ds(pl.multiple_of(2 * width_s + core * width_l, 128), width_l)] = joined_l
        else:
            stage[:, :width_s] = joined_s
            stage[:, width_s:] = joined_l

    def swap(which):
        return (
            pltpu.make_async_remote_copy(
                src_ref=stage.at[:, pl.ds(0, width_s)],
                dst_ref=whole.at[:, pl.ds(pl.multiple_of(which * width_s, 128), width_s)],
                send_sem=swap_send.at[0], recv_sem=swap_recv.at[0],
                device_id=(me, 1 - core), device_id_type=MESH),
            pltpu.make_async_remote_copy(
                src_ref=stage.at[:, pl.ds(width_s, width_l)],
                dst_ref=whole.at[:, pl.ds(pl.multiple_of(2 * width_s + which * width_l, 128), width_l)],
                send_sem=swap_send.at[1], recv_sem=swap_recv.at[1],
                device_id=(me, 1 - core), device_id_type=MESH),
        )

    for copy in swap(core):
        copy.start()
    for load in loads:
        load.wait()
    for step in range(1, depth):

        def sent_up(step=step):
            for copy in far(step):
                copy.wait_send()

        pl.when(mine_z + step < depth)(sent_up)

    def sent(behind, _):
        for shard, target, slot in both_ways(behind):
            for copy in copies(shard, target, send_near.at[behind, slot]):
                copy.wait_send()
        for slot in range(near, near + near_y * near_x):
            for copy in copies(me, me, send_near.at[behind, slot]):
                copy.wait_send()

        def crossed(number, _):
            shard = (mine_z - behind) * plane + number
            pl.when(shard != me)(lambda: across(shard, core).wait_send())
            return 0

        lax.fori_loop(0, plane, crossed, 0)
        return 0

    lax.fori_loop(0, mine_z + 1, sent, 0)
    for copy in swap(1 - core):
        copy.wait_recv()
    columns = weights.shape[1]
    tile = 512

    def project(number, squares):
        span = pl.ds(pl.multiple_of(number * tile, tile), tile)
        part = jnp.dot(whole[...], weights[:, span], preferred_element_type=jnp.float32)
        mixer[:, span] = part
        square = part * part
        return squares + functools.reduce(jnp.add, [square[:, j * 128:(j + 1) * 128] for j in range(tile // 128)])

    squares = lax.fori_loop(0, columns // tile, project, jnp.zeros((keep, 128), jnp.float32))
    mean = jnp.sum(squares, axis=-1, keepdims=True) * (1.0 / columns)
    mixed = (
        residual[...].astype(jnp.float32) + mixer[...] * lax.rsqrt(mean + norm_eps) * gain_mix[...]
    ).astype(jnp.bfloat16)
    mixed_ref[...] = mixed
    routed_ref[...] = rms_scale(mixed.astype(jnp.float32), gain_route[...]).astype(jnp.bfloat16)
    for copy in swap(core):
        copy.wait_send()


def mix(dims, queries_small, queries_large, kv_small, kv_large, cum_small, cum_large, residual, gain_mix, gain_route, out_small, out_large):
    shards = lax.axis_size("sp")
    depth, rows_y, rows_x = dims
    tokens = queries_small.shape[0]
    heads_small = cum_small.shape[0]
    heads_large = cum_large.shape[0]
    size_small = kv_small.shape[1] // 2
    size_large = kv_large.shape[1] // 2
    heads = heads_small + heads_large
    extra_s = round_up(3 * heads_small, 32)
    extra_l = round_up(3 * heads_large, 16)
    rows = extra_s + 2 * size_small + 2 * size_large + extra_l
    near = rows_y + rows_x - 2 + (rows_y - 1) * (rows_x - 1)
    keep, columns = residual.shape
    dma = pltpu.SemaphoreType.DMA
    vmem = pl.BlockSpec(memory_space=pltpu.VMEM)
    hbm = pl.BlockSpec(memory_space=pl.ANY)
    bf16, f32 = jnp.bfloat16, jnp.float32
    return pl.pallas_call(
        functools.partial(mix_kernel, dims, (heads_small, heads_large, size_small, size_large)),
        out_shape=(
            jax.ShapeDtypeStruct(residual.shape, bf16),
            jax.ShapeDtypeStruct(residual.shape, bf16),
        ),
        in_specs=[vmem] * 9 + [hbm] * 2,
        out_specs=(vmem,) * 2,
        scratch_shapes=[
            pltpu.VMEM((shards, rows, tokens), bf16),
            pltpu.VMEM((shards, heads, tokens), f32),
            pltpu.VMEM((heads_small, tokens, extra_s + size_small), bf16),
            pltpu.VMEM((heads_large, tokens, size_large + extra_l), bf16),
            pltpu.VMEM((heads, tokens, 128), f32),
            pltpu.VMEM((heads, tokens, 128), f32),
            pltpu.VMEM((heads_small, tokens, size_small), f32),
            pltpu.VMEM((heads_large, tokens, size_large), f32),
            pltpu.VMEM((keep, heads_small * size_small + heads_large * size_large), bf16),
            pltpu.VMEM((keep, out_small.shape[0] + out_large.shape[0]), bf16),
            pltpu.VMEM((out_small.shape[0] + out_large.shape[0], columns), bf16),
            pltpu.VMEM((keep, columns), f32),
            dma((depth, 2)), dma((depth, near, 2)), dma((shards,)), dma((shards,)), dma((shards,)), dma((shards,)),
            dma((2,)), dma((2,)), dma((2,)),
        ],
        compiler_params=pltpu.CompilerParams(
            collective_id=0, has_side_effects=True, vmem_limit_bytes=56 * 1024 * 1024),
        name="mix",
    )(queries_small, queries_large, kv_small, kv_large, cum_small, cum_large, residual,
      gain_mix.reshape(1, columns), gain_route.reshape(1, columns), out_small, out_large)


def greet(depth, plane, cores, me, core):
    barrier = pltpu.get_barrier_semaphore()
    lanes = plane * cores
    here = me % plane * cores + core
    for step in range(1, depth):
        target = (me // plane + step) % depth * plane + me % plane
        pl.semaphore_signal(barrier, inc=1, device_id=(target, core), device_id_type=MESH)
    for step in range(1, lanes):
        other = (here + step) % lanes
        target = me // plane * plane + other // cores
        pl.semaphore_signal(barrier, inc=1, device_id=(target, other % cores), device_id_type=MESH)
    pl.semaphore_wait(barrier, depth - 1 + lanes - 1)


def distances(depth):
    found = [0]
    for step in range(1, depth):
        found += [step, -step]
    return found


def dispatch_kernel(depth, cores, rows_ref, meta_ref, received, metas, in_rows, stage, send_rows, send_meta, recv_rows, recv_meta, send_block, recv_block, own_sem):
    me = lax.axis_index("sp")
    core = lax.axis_index("tp")
    _, lanes, capacity, columns = stage.shape
    plane = lanes // cores
    slots = rows_ref.shape[1]
    mine = me // plane
    here = me % plane * cores + core
    own_rows = pltpu.make_async_copy(rows_ref.at[mine], in_rows.at[mine], own_sem.at[0, 0])
    own_meta = pltpu.make_async_copy(meta_ref.at[mine], metas.at[mine], own_sem.at[0, 1])
    own_rows.start()
    own_meta.start()
    greet(depth, plane, cores, me, core)

    def along(other):
        target = (other * plane + me % plane, core)
        return (
            pltpu.make_async_remote_copy(
                src_ref=rows_ref.at[other], dst_ref=in_rows.at[mine], send_sem=send_rows.at[other],
                recv_sem=recv_rows.at[mine], device_id=target, device_id_type=MESH),
            pltpu.make_async_remote_copy(
                src_ref=meta_ref.at[other], dst_ref=metas.at[mine], send_sem=send_meta.at[other],
                recv_sem=recv_meta.at[mine], device_id=target, device_id_type=MESH),
        )

    def incoming(other):
        target = (other * plane + me % plane, core)
        return (
            pltpu.make_async_remote_copy(
                src_ref=rows_ref.at[other], dst_ref=in_rows.at[other], send_sem=send_rows.at[other],
                recv_sem=recv_rows.at[other], device_id=target, device_id_type=MESH),
            pltpu.make_async_remote_copy(
                src_ref=meta_ref.at[other], dst_ref=metas.at[other], send_sem=send_meta.at[other],
                recv_sem=recv_meta.at[other], device_id=target, device_id_type=MESH),
        )

    def block(source, other, slot_of):
        return pltpu.make_async_remote_copy(
            src_ref=stage.at[source, other], dst_ref=received.at[source * lanes + slot_of],
            send_sem=send_block.at[source, other], recv_sem=recv_block.at[source, slot_of],
            device_id=(mine * plane + other // cores, other % cores), device_id_type=MESH)

    def keep(source):
        return pltpu.make_async_copy(
            stage.at[source, here], received.at[source * lanes + here], own_sem.at[1, source])

    steps = distances(depth)
    for step in steps[1:]:
        other = mine + step

        def launch(other=other):
            for copy in along(other):
                copy.start()

        pl.when((other >= 0) & (other < depth))(launch)
    own_rows.wait()
    own_meta.wait()
    for step in steps:
        other = mine + step

        def expand(other=other, step=step):
            if step:
                for copy in incoming(other):
                    copy.wait_recv()
            wanted = lax.broadcasted_iota(jnp.int32, (lanes * capacity, slots), 0).astype(jnp.float32) + 1.0
            first = metas[other, 0:1, :slots]
            second = metas[other, 1:2, :slots]
            table = jnp.where((wanted == first) | (wanted == second), 1.0, 0.0).astype(jnp.bfloat16)
            spread = jnp.dot(table, in_rows[other], preferred_element_type=jnp.float32)
            for lane in range(lanes):
                stage[other, lane] = spread[lane * capacity:(lane + 1) * capacity].astype(jnp.bfloat16)
            for move in range(1, lanes):
                block(other, (here + move) % lanes, here).start()
            keep(other).start()

        pl.when((other >= 0) & (other < depth))(expand)
    for source in range(depth):
        keep(source).wait()
        for move in range(1, lanes):
            block(source, (here + move) % lanes, (here + move) % lanes).wait_recv()
            block(source, (here + move) % lanes, here).wait_send()
    for step in steps[1:]:
        other = mine + step

        def sent(other=other):
            for copy in along(other):
                copy.wait_send()

        pl.when((other >= 0) & (other < depth))(sent)


def dispatch(rows, meta, lanes, cores, capacity):
    depth, slots, columns = rows.shape
    dma = pltpu.SemaphoreType.DMA
    vmem = pl.BlockSpec(memory_space=pltpu.VMEM)
    return pl.pallas_call(
        functools.partial(dispatch_kernel, depth, cores),
        out_shape=(
            jax.ShapeDtypeStruct((depth * lanes, capacity, columns), rows.dtype),
            jax.ShapeDtypeStruct(meta.shape, meta.dtype),
        ),
        in_specs=[vmem] * 2,
        out_specs=(vmem,) * 2,
        scratch_shapes=[
            pltpu.VMEM(rows.shape, rows.dtype),
            pltpu.VMEM((depth, lanes, capacity, columns), rows.dtype),
            dma((depth,)), dma((depth,)), dma((depth,)), dma((depth,)),
            dma((depth, lanes)), dma((depth, lanes)), dma((2, max(depth, 2))),
        ],
        compiler_params=pltpu.CompilerParams(
            collective_id=1, has_side_effects=True, vmem_limit_bytes=48 * 1024 * 1024),
        name="dispatch_rows",
    )(rows, meta)


def return_kernel(depth, cores, outs, metas, final, back, stage, send_block, recv_block, send_rows, recv_rows, own_sem):
    me = lax.axis_index("sp")
    core = lax.axis_index("tp")
    _, lanes, capacity, columns = back.shape
    plane = lanes // cores
    slots = final.shape[1]
    mine = me // plane
    here = me % plane * cores + core
    greet(depth, plane, cores, me, core)

    def block(source, other, slot_of):
        return pltpu.make_async_remote_copy(
            src_ref=outs.at[source * lanes + other], dst_ref=back.at[source, slot_of],
            send_sem=send_block.at[source, other], recv_sem=recv_block.at[source, slot_of],
            device_id=(mine * plane + other // cores, other % cores), device_id_type=MESH)

    def keep(source):
        return pltpu.make_async_copy(
            outs.at[source * lanes + here], back.at[source, here], own_sem.at[source])

    def along(other, slot_of):
        return pltpu.make_async_remote_copy(
            src_ref=stage.at[other], dst_ref=final.at[slot_of], send_sem=send_rows.at[other],
            recv_sem=recv_rows.at[slot_of], device_id=(other * plane + me % plane, core), device_id_type=MESH)

    steps = distances(depth)[::-1]
    for step in steps:
        other = mine + step

        def launch(other=other):
            for move in range(1, lanes):
                block(other, (here + move) % lanes, here).start()
            keep(other).start()

        pl.when((other >= 0) & (other < depth))(launch)
    for step in steps:
        other = mine + step

        def combine(other=other, step=step):
            keep(other).wait()
            for move in range(1, lanes):
                block(other, (here + move) % lanes, (here + move) % lanes).wait_recv()
            count = lanes * capacity
            width = metas.shape[2]
            wanted = lax.broadcasted_iota(jnp.int32, (count, width), 0).astype(jnp.float32) + 1.0
            weights = jnp.where(wanted == metas[other, 0:1, :], metas[other, 2:3, :], 0.0)
            weights = weights + jnp.where(wanted == metas[other, 1:2, :], metas[other, 3:4, :], 0.0)
            weights = weights.T[:slots]
            high = weights.astype(jnp.bfloat16)
            low = (weights - high.astype(jnp.float32)).astype(jnp.bfloat16)
            if capacity % 16:
                picked = jnp.concatenate(
                    [back[other, lane].astype(jnp.float32) for lane in range(lanes)], axis=0
                ).astype(jnp.bfloat16)
            else:
                picked = back[other].reshape(count, columns)
            mixed = jnp.dot(high, picked, preferred_element_type=jnp.float32) + jnp.dot(
                low, picked, preferred_element_type=jnp.float32)
            if step:
                stage[other] = mixed.astype(stage.dtype)
                along(other, mine).start()
            else:
                final[other] = mixed.astype(final.dtype)

        pl.when((other >= 0) & (other < depth))(combine)
    for step in steps:
        other = mine + step

        def settle(other=other, step=step):
            for move in range(1, lanes):
                block(other, (here + move) % lanes, here).wait_send()
            if step:
                along(other, other).wait_recv()
                along(other, mine).wait_send()

        pl.when((other >= 0) & (other < depth))(settle)


def give_back(outs, metas, lanes, cores, slots):
    depth = metas.shape[0]
    _, capacity, columns = outs.shape
    dma = pltpu.SemaphoreType.DMA
    vmem = pl.BlockSpec(memory_space=pltpu.VMEM)
    return pl.pallas_call(
        functools.partial(return_kernel, depth, cores),
        out_shape=jax.ShapeDtypeStruct((depth, slots, columns), outs.dtype),
        in_specs=[vmem] * 2,
        out_specs=vmem,
        scratch_shapes=[
            pltpu.VMEM((depth, lanes, capacity, columns), outs.dtype),
            pltpu.VMEM((depth, slots, columns), outs.dtype),
            dma((depth, lanes)), dma((depth, lanes)), dma((depth,)), dma((depth,)), dma((depth,)),
        ],
        compiler_params=pltpu.CompilerParams(
            collective_id=2, has_side_effects=True, vmem_limit_bytes=48 * 1024 * 1024),
        name="return_rows",
    )(outs, metas)


def earlier_same(ids):
    order = jnp.arange(ids.shape[0], dtype=jnp.int32)
    same = (ids[:, None] == ids[None, :]) & (order[None, :] < order[:, None])
    return jnp.sum(same.astype(jnp.int32), axis=1)


def on_device(
    dims,
    queries_small,
    queries_large,
    kv_small,
    kv_large,
    cum_small,
    cum_large,
    residual,
    out_small,
    out_large,
    gain_mix,
    gain_route,
    gain_blend,
    w_gate,
    w_up,
    w_down,
    route,
    route_bias,
):
    row_count = residual.shape[0]
    mixed, routed = mix(
        dims, queries_small, queries_large, kv_small, kv_large, cum_small, cum_large, residual,
        gain_mix, gain_route, out_small, out_large,
    )
    experts = lax.axis_size(("sp", "tp"))
    cores = lax.axis_size("tp")
    depth = dims[0]
    lanes = experts // depth
    capacity = 4 * row_count // experts
    slots = capacity * lanes // 2
    group_ids = route[0] // lanes
    row_slots = group_ids * slots + earlier_same(group_ids)
    row_table = row_slots[None, :] == jnp.arange(depth * slots, dtype=jnp.int32)[:, None]
    flat_ids = route.reshape(2 * row_count)
    places = (flat_ids % lanes * capacity + earlier_same(flat_ids) + 1).astype(jnp.float32)
    facts = jnp.stack(
        [places[:row_count], places[row_count:], jax.nn.sigmoid(route_bias), jax.nn.sigmoid(-route_bias)]
    )
    meta = jnp.sum(jnp.where(row_table[None], facts[:, None, :], 0.0), axis=2)
    meta = meta.reshape(4, depth, slots).transpose(1, 0, 2)
    meta = jnp.pad(meta, ((0, 0), (0, 4), (0, -slots % 128)))
    outgoing = jnp.dot(
        row_table.astype(jnp.bfloat16), routed, preferred_element_type=jnp.float32
    ).astype(jnp.bfloat16)
    received, metas = dispatch(
        outgoing.reshape(depth, slots, routed.shape[1]), meta, lanes, cores, capacity
    )
    row_total = received.shape[0] * received.shape[1]
    expert_rows = received.reshape(row_total, received.shape[2])
    gate_pre = jnp.dot(expert_rows, w_gate[0], preferred_element_type=jnp.float32)
    up_pre = jnp.dot(expert_rows, w_up[0], preferred_element_type=jnp.float32)
    hidden = (jax.nn.silu(gate_pre) * up_pre).astype(jnp.bfloat16)
    expert_out = jnp.dot(hidden, w_down[0], preferred_element_type=jnp.float32).astype(jnp.bfloat16)
    returned = give_back(expert_out.reshape(received.shape), metas, lanes, cores, slots)
    blended = lax.dot_general(
        row_table.astype(jnp.bfloat16),
        returned.reshape(depth * slots, routed.shape[1]),
        (((0,), (0,)), ((), ())),
        preferred_element_type=jnp.float32,
    )
    return (mixed.astype(jnp.float32) + rms_scale(blended, gain_blend)).astype(jnp.bfloat16)


def solution(mesh):
    in_specs = (
        P("sp", "tp"),
        P("sp", "tp"),
        P("sp", None),
        P("sp", None),
        P("tp", "sp"),
        P("tp", "sp"),
        P(("sp", "tp"), None),
        P(),
        P(),
        P(),
        P(),
        P(),
        P(("sp", "tp"), None, None),
        P(("sp", "tp"), None, None),
        P(("sp", "tp"), None, None),
        P(None, ("sp", "tp")),
        P(("sp", "tp")),
    )
    out_specs = P(("sp", "tp"), None)
    return jax.shard_map(
        functools.partial(on_device, mesh_shape(mesh)), mesh=mesh, in_specs=in_specs, out_specs=out_specs, check_vma=False
    )
```

```python
import functools
import math

import jax
import jax.numpy as jnp
from jax import lax
from jax.experimental import pallas as pl
from jax.experimental.pallas import tpu as pltpu
from jax.sharding import PartitionSpec as P

norm_eps = 1e-06
far_score = -1e30
log2e = math.log2(math.e)
MESH = pl.DeviceIdType.MESH


def rms_scale(values, gain_row):
    return (
        values * lax.rsqrt(jnp.mean(values * values, axis=-1, keepdims=True) + norm_eps) * gain_row
    )


def mesh_shape(mesh):
    coords = [tuple(device.coords) for device in mesh.devices.reshape(-1)]
    return tuple(1 + max(c[axis] for c in coords) - min(c[axis] for c in coords) for axis in (2, 1, 0))


def bf16_pieces(values):
    high = values.astype(jnp.bfloat16)
    rest = values - high.astype(jnp.float32)
    middle = rest.astype(jnp.bfloat16)
    low = (rest - middle.astype(jnp.float32)).astype(jnp.bfloat16)
    return [high.astype(jnp.float32), middle.astype(jnp.float32), low.astype(jnp.float32)]


def round_up(value, unit):
    return -(-value // unit) * unit


def mix_kernel(
    dims, head_shape,
    q_small, q_large, kv_small, kv_large, cum_small, cum_large, residual, gain_mix, gain_route, out_small, out_large,
    mixed_ref, routed_ref,
    table, cums, qs, ql, top, total, acc_s, acc_l, stage, whole, weights, mixer,
    send_far, send_near, send_core, recv_kv, recv_cum, recv_core, swap_send, swap_recv, load_sem,
):
    heads_small, heads_large, size_small, size_large = head_shape
    depth, rows_y, rows_x = dims
    plane = rows_y * rows_x
    me = lax.axis_index("sp")
    core = lax.axis_index("tp")
    mine_z = me // plane
    mine_y = me % plane // rows_x
    mine_x = me % rows_x
    tokens = q_small.shape[0]
    heads = heads_small + heads_large
    extra_s = round_up(3 * heads_small, 32)
    extra_l = round_up(3 * heads_large, 16)
    wire = 2 * size_small + 2 * size_large
    half = wire // 2
    small_v = extra_s + size_small
    large_v = small_v + size_small
    large_k = large_v + size_large
    gate_l = extra_s + wire

    loads = (
        pltpu.make_async_copy(out_small, weights.at[pl.ds(0, out_small.shape[0])], load_sem.at[0]),
        pltpu.make_async_copy(
            out_large, weights.at[pl.ds(out_small.shape[0], out_large.shape[0])], load_sem.at[1]),
    )
    for load in loads:
        load.start()
    barrier = pltpu.get_barrier_semaphore()
    for step in range(1, depth):
        target = (mine_z + step) % depth * plane + me % plane
        pl.semaphore_signal(barrier, inc=1, device_id=(target, core), device_id_type=MESH)
    for step in range(1, rows_y):
        target = mine_z * plane + (mine_y + step) % rows_y * rows_x + mine_x
        pl.semaphore_signal(barrier, inc=1, device_id=(target, core), device_id_type=MESH)
    for step in range(1, rows_x):
        target = mine_z * plane + mine_y * rows_x + (mine_x + step) % rows_x
        pl.semaphore_signal(barrier, inc=1, device_id=(target, core), device_id_type=MESH)
    pl.semaphore_signal(barrier, inc=1, device_id=(me, 1 - core), device_id_type=MESH)

    def turned(block):
        width = block.shape[1]
        eye = jnp.where(
            lax.broadcasted_iota(jnp.int32, (width, width), 0) == lax.broadcasted_iota(jnp.int32, (width, width), 1),
            1.0, 0.0).astype(jnp.bfloat16)
        return lax.dot_general(
            eye, block, (((1,), (1,)), ((), ())), preferred_element_type=jnp.float32).astype(jnp.bfloat16)

    table[me, extra_s:large_v, :] = turned(kv_small[...])
    table[me, large_k:gate_l, :] = turned(kv_large[:, :size_large])
    table[me, large_v:large_k, :] = turned(kv_large[:, size_large:])
    cums[me, :heads_small] = cum_small[...]
    cums[me, heads_small:heads] = cum_large[...]

    lanes_s = lax.broadcasted_iota(jnp.int32, (tokens, extra_s), 1)
    lanes_l = lax.broadcasted_iota(jnp.int32, (tokens, extra_l), 1)
    for h in range(heads_small):
        picks = jnp.where((lanes_s % heads_small == h) & (lanes_s < 3 * heads_small), 1.0, 0.0)
        qs[h] = jnp.concatenate(
            [picks.astype(jnp.bfloat16), q_small[:, h * size_small:(h + 1) * size_small]], axis=1)
    for h in range(heads_large):
        picks = jnp.where((lanes_l % heads_large == h) & (lanes_l < 3 * heads_large), 1.0, 0.0)
        ql[h] = jnp.concatenate(
            [q_large[:, h * size_large:(h + 1) * size_large], picks.astype(jnp.bfloat16)], axis=1)
    pl.semaphore_wait(barrier, depth - 1 + rows_y - 1 + rows_x - 1 + 1)

    def place(behind, off_y, off_x):
        return (mine_z - behind) * plane + (mine_y + off_y) % rows_y * rows_x + (mine_x + off_x) % rows_x

    def copies(shard, target, sems):
        part = table.at[shard, pl.ds(extra_s + core * half, half)]
        return (
            pltpu.make_async_remote_copy(
                src_ref=part, dst_ref=part, send_sem=sems.at[0], recv_sem=recv_kv.at[shard],
                device_id=(target, core), device_id_type=MESH),
            pltpu.make_async_remote_copy(
                src_ref=cums.at[shard], dst_ref=cums.at[shard], send_sem=sems.at[1],
                recv_sem=recv_cum.at[shard], device_id=(target, core), device_id_type=MESH),
        )

    def start(shard, target, sems):
        for copy in copies(shard, target, sems):
            copy.start()

    def across(shard, which):
        part = table.at[shard, pl.ds(extra_s + which * half, half)]
        return pltpu.make_async_remote_copy(
            src_ref=part, dst_ref=part, send_sem=send_core.at[shard], recv_sem=recv_core.at[shard],
            device_id=(me, 1 - core), device_id_type=MESH)

    def arrived(shard):
        for copy in copies(shard, me, send_far.at[0]):
            copy.wait_recv()
        across(shard, core).start()

    near_y = rows_y - 1
    near_x = rows_x - 1
    near = near_y + near_x

    def both_ways(behind):
        shard = place(behind, 0, 0)
        for step in range(1, rows_x):
            yield shard, place(0, 0, step), near_y + step - 1
        for step in range(1, rows_y):
            yield shard, place(0, step, 0), step - 1

    def onward(behind, first_axis):
        if first_axis == "y":
            for step_a in range(1, rows_y):
                for step_b in range(1, rows_x):
                    yield place(behind, step_a, 0), place(0, 0, step_b), near + (step_a - 1) * near_x + step_b - 1
        else:
            for step_a in range(1, rows_x):
                for step_b in range(1, rows_y):
                    yield place(behind, 0, step_a), place(0, step_b, 0), near + (step_a - 1) * near_y + step_b - 1

    def column(behind):
        if not isinstance(behind, int):
            arrived(place(behind, 0, 0))
        for shard, target, slot in both_ways(behind):
            start(shard, target, send_near.at[behind, slot])

    def neighbours(behind):
        def along(first_axis):
            waited = []
            for shard, target, slot in onward(behind, first_axis):
                key = slot
                inner = (rows_x if first_axis == "y" else rows_y) - 1
                if (slot - near) % inner == 0:
                    arrived(shard)
                start(shard, target, send_near.at[behind, slot])
            if first_axis == "y":
                if near_x == 0:
                    for step in range(1, rows_y):
                        arrived(place(behind, step, 0))
                for step in range(1, rows_x):
                    arrived(place(behind, 0, step))
            else:
                if near_y == 0:
                    for step in range(1, rows_x):
                        arrived(place(behind, 0, step))
                for step in range(1, rows_y):
                    arrived(place(behind, step, 0))

        pl.when(core == 0)(functools.partial(along, "y"))
        pl.when(core == 1)(functools.partial(along, "x"))

    def corners(behind):
        for off_y in range(1, rows_y):
            for off_x in range(1, rows_x):
                arrived(place(behind, off_y, off_x))

    def far(step):
        return copies(me, (mine_z + step) * plane + me % plane, send_far.at[step])

    column(0)
    for step in range(1, depth):

        def send_up(step=step):
            for copy in far(step):
                copy.start()

        pl.when(mine_z + step < depth)(send_up)

    def attend(shard, own):
        gates = cums[shard]
        picked = bf16_pieces(gates[:heads_small] * (-math.sqrt(size_small)))
        if extra_s > 3 * heads_small:
            picked.append(jnp.zeros((extra_s - 3 * heads_small, tokens), jnp.float32))
        table[shard, :extra_s, :] = jnp.concatenate(picked, axis=0).astype(jnp.bfloat16)
        picked = bf16_pieces(gates[heads_small:heads] * (-math.sqrt(size_large)))
        if extra_l > 3 * heads_large:
            picked.append(jnp.zeros((extra_l - 3 * heads_large, tokens), jnp.float32))
        table[shard, gate_l:, :] = jnp.concatenate(picked, axis=0).astype(jnp.bfloat16)
        for h in range(heads):
            small = h < heads_small
            size = size_small if small else size_large
            scale = size ** (-0.5) * log2e
            query = qs[h] if small else ql[h - heads_small]
            keys = table[shard, :small_v, :] if small else table[shard, large_k:, :]
            values = table[shard, small_v:large_v, :] if small else table[shard, large_v:large_k, :]
            acc_ref, number = (acc_s, h) if small else (acc_l, h - heads_small)
            scores = jnp.dot(query, keys, preferred_element_type=jnp.float32)
            if own:
                key_pos = lax.broadcasted_iota(jnp.int32, (tokens, tokens), 1)
                query_pos = lax.broadcasted_iota(jnp.int32, (tokens, tokens), 0)
                scores = jnp.where(key_pos <= query_pos, scores, far_score)
            parts = [scores[:, j * 128:(j + 1) * 128] for j in range(tokens // 128)]
            newest = jnp.max(functools.reduce(jnp.maximum, parts), axis=-1, keepdims=True)
            if own:
                newest = jnp.broadcast_to(newest, (tokens, 128))
            else:
                before = top[h]
                newest = jnp.maximum(before, newest)
                factor = jnp.exp2((before - newest) * scale)
            scaled = newest * scale
            found = [jnp.exp2(part * scale - scaled) for part in parts]
            partial_sum = functools.reduce(jnp.add, found)
            product = lax.dot_general(
                jnp.concatenate(found, axis=1).astype(jnp.bfloat16), values,
                (((1,), (1,)), ((), ())), preferred_element_type=jnp.float32)
            top[h] = newest
            if own:
                total[h] = partial_sum
                acc_ref[number] = product
            else:
                total[h] = total[h] * factor + partial_sum
                acc_ref[number] = acc_ref[number] * factor[:, :size] + product

    attend(me, True)
    pl.when(mine_z >= 1)(lambda: column(jnp.int32(1)))
    neighbours(0)
    order = [(0, 0)] + [(step, 0) for step in range(1, rows_y)] + [(0, step) for step in range(1, rows_x)]
    order += [(a, b) for a in range(1, rows_y) for b in range(1, rows_x)]

    def step_of(number, _):
        behind = number // plane
        turn = number % plane
        pl.when((turn == 0) & (behind + 1 <= mine_z))(lambda: column(behind + 1))
        pl.when(turn == min(2, plane - 1))(lambda: corners(behind))
        pl.when((turn == plane - 1) & (behind + 1 <= mine_z))(lambda: neighbours(behind + 1))
        off_y = jnp.int32(0)
        off_x = jnp.int32(0)
        for index, (a, b) in enumerate(order):
            off_y = jnp.where(turn == index, a, off_y)
            off_x = jnp.where(turn == index, b, off_x)
        shard = place(behind, off_y, off_x)
        across(shard, 1 - core).wait_recv()
        pl.when(shard < me)(lambda: attend(shard, False))
        return 0

    lax.fori_loop(1, (mine_z + 1) * plane, step_of, 0)

    keep = tokens // 2
    width_s = heads_small * size_small
    width_l = heads_large * size_large
    for mine in (False, True):
        rows = pl.ds(pl.multiple_of((core if mine else 1 - core) * keep, keep), keep)
        columns = []
        for h in range(heads):
            small = h < heads_small
            sums = jnp.sum(total[h, rows, :], axis=-1, keepdims=True)
            values = acc_s[h, rows, :] if small else acc_l[h - heads_small, rows, :]
            columns.append((values / sums).astype(jnp.bfloat16))
        joined_s = jnp.concatenate(columns[:heads_small], axis=1)
        joined_l = jnp.concatenate(columns[heads_small:], axis=1)
        if mine:
            whole[:, pl.ds(pl.multiple_of(core * width_s, 128), width_s)] = joined_s
            whole[:, pl.ds(pl.multiple_of(2 * width_s + core * width_l, 128), width_l)] = joined_l
        else:
            stage[:, :width_s] = joined_s
            stage[:, width_s:] = joined_l

    def swap(which):
        return (
            pltpu.make_async_remote_copy(
                src_ref=stage.at[:, pl.ds(0, width_s)],
                dst_ref=whole.at[:, pl.ds(pl.multiple_of(which * width_s, 128), width_s)],
                send_sem=swap_send.at[0], recv_sem=swap_recv.at[0],
                device_id=(me, 1 - core), device_id_type=MESH),
            pltpu.make_async_remote_copy(
                src_ref=stage.at[:, pl.ds(width_s, width_l)],
                dst_ref=whole.at[:, pl.ds(pl.multiple_of(2 * width_s + which * width_l, 128), width_l)],
                send_sem=swap_send.at[1], recv_sem=swap_recv.at[1],
                device_id=(me, 1 - core), device_id_type=MESH),
        )

    for copy in swap(core):
        copy.start()
    for load in loads:
        load.wait()
    for step in range(1, depth):

        def sent_up(step=step):
            for copy in far(step):
                copy.wait_send()

        pl.when(mine_z + step < depth)(sent_up)

    def sent(behind, _):
        for shard, target, slot in both_ways(behind):
            for copy in copies(shard, target, send_near.at[behind, slot]):
                copy.wait_send()
        for slot in range(near, near + near_y * near_x):
            for copy in copies(me, me, send_near.at[behind, slot]):
                copy.wait_send()

        def crossed(number, _):
            shard = (mine_z - behind) * plane + number
            pl.when(shard != me)(lambda: across(shard, core).wait_send())
            return 0

        lax.fori_loop(0, plane, crossed, 0)
        return 0

    lax.fori_loop(0, mine_z + 1, sent, 0)
    for copy in swap(1 - core):
        copy.wait_recv()
    columns = weights.shape[1]
    tile = 512

    def project(number, squares):
        span = pl.ds(pl.multiple_of(number * tile, tile), tile)
        part = jnp.dot(whole[...], weights[:, span], preferred_element_type=jnp.float32)
        mixer[:, span] = part
        square = part * part
        return squares + functools.reduce(jnp.add, [square[:, j * 128:(j + 1) * 128] for j in range(tile // 128)])

    squares = lax.fori_loop(0, columns // tile, project, jnp.zeros((keep, 128), jnp.float32))
    mean = jnp.sum(squares, axis=-1, keepdims=True) * (1.0 / columns)
    mixed = (
        residual[...].astype(jnp.float32) + mixer[...] * lax.rsqrt(mean + norm_eps) * gain_mix[...]
    ).astype(jnp.bfloat16)
    mixed_ref[...] = mixed
    routed_ref[...] = rms_scale(mixed.astype(jnp.float32), gain_route[...]).astype(jnp.bfloat16)
    for copy in swap(core):
        copy.wait_send()


def mix(dims, queries_small, queries_large, kv_small, kv_large, cum_small, cum_large, residual, gain_mix, gain_route, out_small, out_large):
    shards = lax.axis_size("sp")
    depth, rows_y, rows_x = dims
    tokens = queries_small.shape[0]
    heads_small = cum_small.shape[0]
    heads_large = cum_large.shape[0]
    size_small = kv_small.shape[1] // 2
    size_large = kv_large.shape[1] // 2
    heads = heads_small + heads_large
    extra_s = round_up(3 * heads_small, 32)
    extra_l = round_up(3 * heads_large, 16)
    rows = extra_s + 2 * size_small + 2 * size_large + extra_l
    near = rows_y + rows_x - 2 + (rows_y - 1) * (rows_x - 1)
    keep, columns = residual.shape
    dma = pltpu.SemaphoreType.DMA
    vmem = pl.BlockSpec(memory_space=pltpu.VMEM)
    hbm = pl.BlockSpec(memory_space=pl.ANY)
    bf16, f32 = jnp.bfloat16, jnp.float32
    return pl.pallas_call(
        functools.partial(mix_kernel, dims, (heads_small, heads_large, size_small, size_large)),
        out_shape=(
            jax.ShapeDtypeStruct(residual.shape, bf16),
            jax.ShapeDtypeStruct(residual.shape, bf16),
        ),
        in_specs=[vmem] * 9 + [hbm] * 2,
        out_specs=(vmem,) * 2,
        scratch_shapes=[
            pltpu.VMEM((shards, rows, tokens), bf16),
            pltpu.VMEM((shards, heads, tokens), f32),
            pltpu.VMEM((heads_small, tokens, extra_s + size_small), bf16),
            pltpu.VMEM((heads_large, tokens, size_large + extra_l), bf16),
            pltpu.VMEM((heads, tokens, 128), f32),
            pltpu.VMEM((heads, tokens, 128), f32),
            pltpu.VMEM((heads_small, tokens, size_small), f32),
            pltpu.VMEM((heads_large, tokens, size_large), f32),
            pltpu.VMEM((keep, heads_small * size_small + heads_large * size_large), bf16),
            pltpu.VMEM((keep, out_small.shape[0] + out_large.shape[0]), bf16),
            pltpu.VMEM((out_small.shape[0] + out_large.shape[0], columns), bf16),
            pltpu.VMEM((keep, columns), f32),
            dma((depth, 2)), dma((depth, near, 2)), dma((shards,)), dma((shards,)), dma((shards,)), dma((shards,)),
            dma((2,)), dma((2,)), dma((2,)),
        ],
        compiler_params=pltpu.CompilerParams(
            collective_id=0, has_side_effects=True, vmem_limit_bytes=56 * 1024 * 1024),
        name="mix",
    )(queries_small, queries_large, kv_small, kv_large, cum_small, cum_large, residual,
      gain_mix.reshape(1, columns), gain_route.reshape(1, columns), out_small, out_large)


def greet(depth, plane, cores, me, core):
    barrier = pltpu.get_barrier_semaphore()
    lanes = plane * cores
    here = me % plane * cores + core
    for step in range(1, depth):
        target = (me // plane + step) % depth * plane + me % plane
        pl.semaphore_signal(barrier, inc=1, device_id=(target, core), device_id_type=MESH)
    for step in range(1, lanes):
        other = (here + step) % lanes
        target = me // plane * plane + other // cores
        pl.semaphore_signal(barrier, inc=1, device_id=(target, other % cores), device_id_type=MESH)
    return depth - 1 + lanes - 1


def distances(depth):
    found = [0]
    for step in range(1, depth):
        found += [step, -step]
    return found


def as_column(row, eye):
    return jnp.sum(jnp.where(eye, row, 0.0), axis=1, keepdims=True)


def expert_kernel(
    depth, cores,
    routed_ref, mixed_ref, route_ref, bias_ref, gain_ref, w_gate, w_up, w_down,
    result_ref,
    out_rows, in_rows, out_meta, metas, spread, received, outs, back, combined, final, hidden, gate_w, up_w, down_w,
    send_rows, recv_rows, send_meta, recv_meta, send_block, recv_block, send_back, recv_back, send_home, recv_home, load_sem,
):
    me = lax.axis_index("sp")
    core = lax.axis_index("tp")
    _, lanes, capacity, columns = spread.shape
    slots = in_rows.shape[1]
    width = metas.shape[2]
    tokens = routed_ref.shape[0]
    plane = lanes // cores
    count = lanes * capacity
    mine = me // plane
    here = me % plane * cores + core
    loads = (
        pltpu.make_async_copy(w_gate.at[0], gate_w, load_sem.at[0]),
        pltpu.make_async_copy(w_up.at[0], up_w, load_sem.at[1]),
        pltpu.make_async_copy(w_down.at[0], down_w, load_sem.at[2]),
    )
    for load in loads:
        load.start()
    greeted = greet(depth, plane, cores, me, core)

    row_of = lax.broadcasted_iota(jnp.int32, (tokens, tokens), 0)
    lane_of = lax.broadcasted_iota(jnp.int32, (tokens, tokens), 1)
    eye = row_of == lane_of
    before = row_of < lane_of
    ids = route_ref[...].astype(jnp.float32)
    first, second = ids[0:1], ids[1:2]
    groups = jnp.floor((first + 0.5) * (1.0 / lanes))
    groups_col = as_column(groups, eye)
    first_col = as_column(first, eye)
    second_col = as_column(second, eye)

    def total_rows(mask):
        return jnp.sum(jnp.where(mask, 1.0, 0.0), axis=0, keepdims=True)

    ranks = total_rows((groups_col == groups) & before)
    places_first = (first - groups * lanes) * capacity + total_rows((first_col == first) & before) + 1.0
    places_second = (
        (second - groups * lanes) * capacity
        + total_rows(first_col == second) + total_rows((second_col == second) & before) + 1.0
    )
    bias = bias_ref[...]
    facts = [as_column(fact, eye) for fact in (places_first, places_second, jax.nn.sigmoid(bias), jax.nn.sigmoid(-bias))]
    ranks_col = as_column(ranks, eye)
    slot_rows = lax.broadcasted_iota(jnp.int32, (slots, tokens), 0).astype(jnp.float32)
    slot_lanes = lax.broadcasted_iota(jnp.int32, (tokens, width), 1).astype(jnp.float32)
    for group in range(depth):
        table = jnp.where((slot_rows == ranks) & (groups == group), 1.0, 0.0).astype(jnp.bfloat16)
        out_rows[group] = jnp.dot(table, routed_ref[...], preferred_element_type=jnp.float32).astype(jnp.bfloat16)
        chosen = (slot_lanes == ranks_col) & (groups_col == group)
        rows = [jnp.sum(jnp.where(chosen, fact, 0.0), axis=0, keepdims=True) for fact in facts]
        out_meta[group] = jnp.concatenate(rows + [jnp.zeros((4, width), jnp.float32)], axis=0)
    in_rows[mine] = out_rows[mine]
    metas[mine] = out_meta[mine]
    pl.semaphore_wait(pltpu.get_barrier_semaphore(), greeted)

    def along(other, slot):
        target = (other * plane + me % plane, core)
        return (
            pltpu.make_async_remote_copy(
                src_ref=out_rows.at[other], dst_ref=in_rows.at[slot], send_sem=send_rows.at[other],
                recv_sem=recv_rows.at[slot], device_id=target, device_id_type=MESH),
            pltpu.make_async_remote_copy(
                src_ref=out_meta.at[other], dst_ref=metas.at[slot], send_sem=send_meta.at[other],
                recv_sem=recv_meta.at[slot], device_id=target, device_id_type=MESH),
        )

    def outward(source, other, slot):
        return pltpu.make_async_remote_copy(
            src_ref=spread.at[source, other], dst_ref=received.at[source, slot],
            send_sem=send_block.at[source, other], recv_sem=recv_block.at[source, slot],
            device_id=(mine * plane + other // cores, other % cores), device_id_type=MESH)

    def inward(source, other, slot):
        return pltpu.make_async_remote_copy(
            src_ref=outs.at[source, other], dst_ref=back.at[source, slot],
            send_sem=send_back.at[source, other], recv_sem=recv_back.at[source, slot],
            device_id=(mine * plane + other // cores, other % cores), device_id_type=MESH)

    def homeward(other, slot):
        return pltpu.make_async_remote_copy(
            src_ref=combined.at[other], dst_ref=final.at[slot], send_sem=send_home.at[other],
            recv_sem=recv_home.at[slot], device_id=(other * plane + me % plane, core), device_id_type=MESH)

    steps = distances(depth)
    for step in steps[1:]:
        other = mine + step

        def launch(other=other):
            for copy in along(other, mine):
                copy.start()

        pl.when((other >= 0) & (other < depth))(launch)

    orders = [[z + step for step in steps if 0 <= z + step < depth] for z in range(depth)]

    def source_of(turn):
        found = jnp.int32(0)
        for z in range(depth):
            for index in range(depth):
                found = jnp.where((mine == z) & (turn == index), orders[z][index], found)
        return found

    def flat(ref, source):
        if capacity % 16:
            return jnp.concatenate(
                [ref[source, lane].astype(jnp.float32) for lane in range(lanes)], axis=0).astype(jnp.bfloat16)
        return ref[source].reshape(count, columns)

    def split(ref, source, values, span):
        for lane in range(lanes):
            ref[source, lane, :, span] = values[lane * capacity:(lane + 1) * capacity].astype(jnp.bfloat16)

    def expand(source):
        def landed():
            for copy in along(source, source):
                copy.wait_recv()

        pl.when(source != mine)(landed)
        wanted = lax.broadcasted_iota(jnp.int32, (count, slots), 0).astype(jnp.float32) + 1.0
        table = jnp.where(
            (wanted == metas[source, 0:1, :slots]) | (wanted == metas[source, 1:2, :slots]), 1.0, 0.0
        ).astype(jnp.bfloat16)
        split(spread, source, jnp.dot(table, in_rows[source], preferred_element_type=jnp.float32), slice(None))
        received[source, here] = spread[source, here]
        for move in range(1, lanes):
            outward(source, (here + move) % lanes, here).start()

    tile = 256

    def compute(source):
        for move in range(1, lanes):
            outward(source, (here + move) % lanes, (here + move) % lanes).wait_recv()
        rows = flat(received, source)

        def enter(number, _):
            span = pl.ds(pl.multiple_of(number * tile, tile), tile)
            gate = jnp.dot(rows, gate_w[:, span], preferred_element_type=jnp.float32)
            up = jnp.dot(rows, up_w[:, span], preferred_element_type=jnp.float32)
            hidden[:, span] = (jax.nn.silu(gate) * up).astype(jnp.bfloat16)
            return 0

        lax.fori_loop(0, gate_w.shape[1] // tile, enter, 0)

        def leave(number, _):
            span = pl.ds(pl.multiple_of(number * 2 * tile, 2 * tile), 2 * tile)
            split(outs, source, jnp.dot(hidden[...], down_w[:, span], preferred_element_type=jnp.float32), span)
            return 0

        lax.fori_loop(0, columns // (2 * tile), leave, 0)
        back[source, here] = outs[source, here]
        for move in range(1, lanes):
            inward(source, (here + move) % lanes, here).start()

    def combine(source):
        for move in range(1, lanes):
            inward(source, (here + move) % lanes, (here + move) % lanes).wait_recv()
        wanted = lax.broadcasted_iota(jnp.int32, (count, width), 0).astype(jnp.float32) + 1.0
        shares = jnp.where(wanted == metas[source, 0:1, :], metas[source, 2:3, :], 0.0)
        shares = shares + jnp.where(wanted == metas[source, 1:2, :], metas[source, 3:4, :], 0.0)
        shares = shares.T[:slots]
        high = shares.astype(jnp.bfloat16)
        low = (shares - high.astype(jnp.float32)).astype(jnp.bfloat16)
        picked = flat(back, source)
        mixed = jnp.dot(high, picked, preferred_element_type=jnp.float32) + jnp.dot(
            low, picked, preferred_element_type=jnp.float32)

        def away():
            combined[source] = mixed.astype(jnp.bfloat16)
            homeward(source, mine).start()

        def stay():
            final[source] = mixed.astype(jnp.bfloat16)

        pl.when(source != mine)(away)
        pl.when(source == mine)(stay)

    def turn_of(turn, _):
        pl.when(turn < depth)(lambda: expand(source_of(turn)))

        @pl.when(turn == 1)
        def _():
            for load in loads:
                load.wait()

        pl.when((turn >= 1) & (turn <= depth))(lambda: compute(source_of(turn - 1)))
        pl.when(turn >= 2)(lambda: combine(source_of(turn - 2)))
        return 0

    lax.fori_loop(0, depth + 2, turn_of, 0)
    for step in steps[1:]:
        other = mine + step

        def settle(other=other):
            homeward(other, other).wait_recv()
            homeward(other, mine).wait_send()
            for copy in along(other, mine):
                copy.wait_send()

        pl.when((other >= 0) & (other < depth))(settle)
    for source in range(depth):
        for move in range(1, lanes):
            outward(source, (here + move) % lanes, here).wait_send()
            inward(source, (here + move) % lanes, here).wait_send()
    slot_all = lax.broadcasted_iota(jnp.int32, (tokens, depth * slots), 1).astype(jnp.float32)
    table = jnp.where(slot_all == groups_col * slots + ranks_col, 1.0, 0.0).astype(jnp.bfloat16)
    blended = jnp.dot(table, final[...].reshape(depth * slots, columns), preferred_element_type=jnp.float32)
    result_ref[...] = (
        mixed_ref[...].astype(jnp.float32) + rms_scale(blended, gain_ref[...])
    ).astype(jnp.bfloat16)


def experts_of(dims, routed, mixed, route, bias, gain, w_gate, w_up, w_down):
    depth = dims[0]
    cores = lax.axis_size("tp")
    lanes = lax.axis_size(("sp", "tp")) // depth
    tokens, columns = routed.shape
    capacity = 4 * tokens // (depth * lanes)
    slots = capacity * lanes // 2
    width = round_up(slots, 128)
    inner = w_gate.shape[2]
    dma = pltpu.SemaphoreType.DMA
    vmem = pl.BlockSpec(memory_space=pltpu.VMEM)
    hbm = pl.BlockSpec(memory_space=pl.ANY)
    bf16, f32 = jnp.bfloat16, jnp.float32
    rows = pltpu.VMEM((depth, slots, columns), bf16)
    blocks = pltpu.VMEM((depth, lanes, capacity, columns), bf16)
    meta = pltpu.VMEM((depth, 8, width), f32)
    return pl.pallas_call(
        functools.partial(expert_kernel, depth, cores),
        out_shape=jax.ShapeDtypeStruct(mixed.shape, bf16),
        in_specs=[vmem] * 5 + [hbm] * 3,
        out_specs=vmem,
        scratch_shapes=[
            rows, rows, meta, meta, blocks, blocks, blocks, blocks, rows, rows,
            pltpu.VMEM((lanes * capacity, inner), bf16),
            pltpu.VMEM((columns, inner), bf16),
            pltpu.VMEM((columns, inner), bf16),
            pltpu.VMEM((inner, columns), bf16),
            dma((depth,)), dma((depth,)), dma((depth,)), dma((depth,)),
            dma((depth, lanes)), dma((depth, lanes)), dma((depth, lanes)), dma((depth, lanes)),
            dma((depth,)), dma((depth,)), dma((3,)),
        ],
        compiler_params=pltpu.CompilerParams(
            collective_id=1, has_side_effects=True, vmem_limit_bytes=60 * 1024 * 1024),
        name="experts",
    )(routed, mixed, route, bias.reshape(1, tokens), gain.reshape(1, columns), w_gate, w_up, w_down)


def on_device(
    dims,
    queries_small,
    queries_large,
    kv_small,
    kv_large,
    cum_small,
    cum_large,
    residual,
    out_small,
    out_large,
    gain_mix,
    gain_route,
    gain_blend,
    w_gate,
    w_up,
    w_down,
    route,
    route_bias,
):
    mixed, routed = mix(
        dims, queries_small, queries_large, kv_small, kv_large, cum_small, cum_large, residual,
        gain_mix, gain_route, out_small, out_large,
    )
    return experts_of(dims, routed, mixed, route, route_bias, gain_blend, w_gate, w_up, w_down)


def solution(mesh):
    in_specs = (
        P("sp", "tp"),
        P("sp", "tp"),
        P("sp", None),
        P("sp", None),
        P("tp", "sp"),
        P("tp", "sp"),
        P(("sp", "tp"), None),
        P(),
        P(),
        P(),
        P(),
        P(),
        P(("sp", "tp"), None, None),
        P(("sp", "tp"), None, None),
        P(("sp", "tp"), None, None),
        P(None, ("sp", "tp")),
        P(("sp", "tp")),
    )
    out_specs = P(("sp", "tp"), None)
    return jax.shard_map(
        functools.partial(on_device, mesh_shape(mesh)), mesh=mesh, in_specs=in_specs, out_specs=out_specs, check_vma=False
    )
```

```python
import functools
import math

import jax
import jax.numpy as jnp
from jax import lax
from jax.experimental import pallas as pl
from jax.experimental.pallas import tpu as pltpu
from jax.sharding import PartitionSpec as P

norm_eps = 1e-06
far_score = -1e30
log2e = math.log2(math.e)
MESH = pl.DeviceIdType.MESH


def rms_scale(values, gain_row):
    return (
        values * lax.rsqrt(jnp.mean(values * values, axis=-1, keepdims=True) + norm_eps) * gain_row
    )


def mesh_shape(mesh):
    coords = [tuple(device.coords) for device in mesh.devices.reshape(-1)]
    return tuple(1 + max(c[axis] for c in coords) - min(c[axis] for c in coords) for axis in (2, 1, 0))


def bf16_pieces(values):
    high = values.astype(jnp.bfloat16)
    rest = values - high.astype(jnp.float32)
    middle = rest.astype(jnp.bfloat16)
    low = (rest - middle.astype(jnp.float32)).astype(jnp.bfloat16)
    return [high.astype(jnp.float32), middle.astype(jnp.float32), low.astype(jnp.float32)]


def round_up(value, unit):
    return -(-value // unit) * unit


def greet(depth, plane, cores, me, core):
    barrier = pltpu.get_barrier_semaphore()
    lanes = plane * cores
    here = me % plane * cores + core
    for step in range(1, depth):
        target = (me // plane + step) % depth * plane + me % plane
        pl.semaphore_signal(barrier, inc=1, device_id=(target, core), device_id_type=MESH)
    for step in range(1, lanes):
        other = (here + step) % lanes
        target = me // plane * plane + other // cores
        pl.semaphore_signal(barrier, inc=1, device_id=(target, other % cores), device_id_type=MESH)
    return depth - 1 + lanes - 1


def distances(depth):
    found = [0]
    for step in range(1, depth):
        found += [step, -step]
    return found


def as_column(row, eye):
    return jnp.sum(jnp.where(eye, row, 0.0), axis=1, keepdims=True)


def plan_of(depth):
    if depth == 4:
        texts = (
            "E0 E1 F0 F1 E3 E2 F3 F2 C3 C2 C1 C0",
            "E1 E0 E2 F1 F2 C2 C1 E3 F3 F0 C3 C0",
            "E0 E2 E1 E3 F0 F2 F1 C0 F3 C1 C3 C2",
            "E3 E1 E0 E2 F1 F3 C3 C1 F0 F2 C0 C2",
        )
        return [[("EFC".index(word[0]), int(word[1])) for word in text.split()] for text in texts]
    plans = []
    for z in range(depth):
        order = [z + step for step in distances(depth) if 0 <= z + step < depth]
        plan = []
        for turn in range(depth + 2):
            plan += [(0, order[turn])] if turn < depth else []
            plan += [(1, order[turn - 1])] if 1 <= turn <= depth else []
            plan += [(2, order[turn - 2])] if turn >= 2 else []
        plans.append(plan)
    return plans


def layer_kernel(
    dims, head_shape,
    q_small, q_large, kv_small, kv_large, cum_small, cum_large, residual, gain_mix, gain_route, route_ref, bias_ref, gain_ref,
    out_small, out_large, w_gate, w_up, w_down,
    result_ref,
    table, cums, qs, ql, top, total, acc_s, acc_l, stage, whole, weights, mixer, mixed_ref, routing,
    out_rows, in_rows, out_meta, metas, spread, received, outs, back, combined, final, hidden, gate_w, up_w, down_w,
    send_far, send_near, send_core, recv_kv, recv_cum, recv_core, swap_send, swap_recv, load_sem,
    send_rows, recv_rows, send_meta, recv_meta, send_block, recv_block, send_back, recv_back, send_home, recv_home,
):
    heads_small, heads_large, size_small, size_large = head_shape
    depth, rows_y, rows_x = dims
    plane = rows_y * rows_x
    me = lax.axis_index("sp")
    core = lax.axis_index("tp")
    mine_z = me // plane
    mine_y = me % plane // rows_x
    mine_x = me % rows_x
    tokens = q_small.shape[0]
    _, lanes, capacity, columns = spread.shape
    cores = lanes // (dims[1] * dims[2])
    slots = in_rows.shape[1]
    width = metas.shape[2]
    keep = residual.shape[0]
    count = lanes * capacity
    here = me % plane * cores + core
    heads = heads_small + heads_large
    extra_s = round_up(3 * heads_small, 32)
    extra_l = round_up(3 * heads_large, 16)
    wire = 2 * size_small + 2 * size_large
    half = wire // 2
    small_v = extra_s + size_small
    large_v = small_v + size_small
    large_k = large_v + size_large
    gate_l = extra_s + wire

    loads = (
        pltpu.make_async_copy(out_small, weights.at[pl.ds(0, out_small.shape[0])], load_sem.at[0]),
        pltpu.make_async_copy(
            out_large, weights.at[pl.ds(out_small.shape[0], out_large.shape[0])], load_sem.at[1]),
    )
    expert_loads = (
        pltpu.make_async_copy(w_gate.at[0], gate_w, load_sem.at[2]),
        pltpu.make_async_copy(w_up.at[0], up_w, load_sem.at[3]),
        pltpu.make_async_copy(w_down.at[0], down_w, load_sem.at[4]),
    )
    for load in loads + expert_loads:
        load.start()
    greeted = greet(depth, plane, cores, me, core)
    def turned(block):
        width = block.shape[1]
        eye = jnp.where(
            lax.broadcasted_iota(jnp.int32, (width, width), 0) == lax.broadcasted_iota(jnp.int32, (width, width), 1),
            1.0, 0.0).astype(jnp.bfloat16)
        return lax.dot_general(
            eye, block, (((1,), (1,)), ((), ())), preferred_element_type=jnp.float32).astype(jnp.bfloat16)

    table[me, extra_s:large_v, :] = turned(kv_small[...])
    table[me, large_k:gate_l, :] = turned(kv_large[:, :size_large])
    table[me, large_v:large_k, :] = turned(kv_large[:, size_large:])
    cums[me, :heads_small] = cum_small[...]
    cums[me, heads_small:heads] = cum_large[...]

    lanes_s = lax.broadcasted_iota(jnp.int32, (tokens, extra_s), 1)
    lanes_l = lax.broadcasted_iota(jnp.int32, (tokens, extra_l), 1)
    for h in range(heads_small):
        picks = jnp.where((lanes_s % heads_small == h) & (lanes_s < 3 * heads_small), 1.0, 0.0)
        qs[h] = jnp.concatenate(
            [picks.astype(jnp.bfloat16), q_small[:, h * size_small:(h + 1) * size_small]], axis=1)
    for h in range(heads_large):
        picks = jnp.where((lanes_l % heads_large == h) & (lanes_l < 3 * heads_large), 1.0, 0.0)
        ql[h] = jnp.concatenate(
            [q_large[:, h * size_large:(h + 1) * size_large], picks.astype(jnp.bfloat16)], axis=1)
    row_of = lax.broadcasted_iota(jnp.int32, (keep, keep), 0)
    lane_of = lax.broadcasted_iota(jnp.int32, (keep, keep), 1)
    eye = row_of == lane_of
    before = row_of < lane_of
    ids = route_ref[...].astype(jnp.float32)
    first, second = ids[0:1], ids[1:2]
    groups = jnp.floor((first + 0.5) * (1.0 / lanes))
    groups_col = as_column(groups, eye)
    first_col = as_column(first, eye)
    second_col = as_column(second, eye)

    def total_rows(mask):
        return jnp.sum(jnp.where(mask, 1.0, 0.0), axis=0, keepdims=True)

    ranks = total_rows((groups_col == groups) & before)
    places_first = (first - groups * lanes) * capacity + total_rows((first_col == first) & before) + 1.0
    places_second = (
        (second - groups * lanes) * capacity
        + total_rows(first_col == second) + total_rows((second_col == second) & before) + 1.0
    )
    bias = bias_ref[...]
    facts = [as_column(fact, eye) for fact in (places_first, places_second, jax.nn.sigmoid(bias), jax.nn.sigmoid(-bias))]
    ranks_col = as_column(ranks, eye)
    slot_lanes = lax.broadcasted_iota(jnp.int32, (keep, width), 1).astype(jnp.float32)
    for group in range(depth):
        chosen = (slot_lanes == ranks_col) & (groups_col == group)
        rows = [jnp.sum(jnp.where(chosen, fact, 0.0), axis=0, keepdims=True) for fact in facts]
        out_meta[group] = jnp.concatenate(rows + [jnp.zeros((4, width), jnp.float32)], axis=0)
    routing[0:1] = groups
    routing[1:2] = ranks
    pl.semaphore_wait(pltpu.get_barrier_semaphore(), greeted)

    def place(behind, off_y, off_x):
        return (mine_z - behind) * plane + (mine_y + off_y) % rows_y * rows_x + (mine_x + off_x) % rows_x

    def copies(shard, target, sems):
        part = table.at[shard, pl.ds(extra_s + core * half, half)]
        return (
            pltpu.make_async_remote_copy(
                src_ref=part, dst_ref=part, send_sem=sems.at[0], recv_sem=recv_kv.at[shard],
                device_id=(target, core), device_id_type=MESH),
            pltpu.make_async_remote_copy(
                src_ref=cums.at[shard], dst_ref=cums.at[shard], send_sem=sems.at[1],
                recv_sem=recv_cum.at[shard], device_id=(target, core), device_id_type=MESH),
        )

    def start(shard, target, sems):
        for copy in copies(shard, target, sems):
            copy.start()

    def across(shard, which):
        part = table.at[shard, pl.ds(extra_s + which * half, half)]
        return pltpu.make_async_remote_copy(
            src_ref=part, dst_ref=part, send_sem=send_core.at[shard], recv_sem=recv_core.at[shard],
            device_id=(me, 1 - core), device_id_type=MESH)

    def arrived(shard):
        for copy in copies(shard, me, send_far.at[0]):
            copy.wait_recv()
        across(shard, core).start()

    near_y = rows_y - 1
    near_x = rows_x - 1
    near = near_y + near_x

    def both_ways(behind):
        shard = place(behind, 0, 0)
        for step in range(1, rows_x):
            yield shard, place(0, 0, step), near_y + step - 1
        for step in range(1, rows_y):
            yield shard, place(0, step, 0), step - 1

    def onward(behind, first_axis):
        if first_axis == "y":
            for step_a in range(1, rows_y):
                for step_b in range(1, rows_x):
                    yield place(behind, step_a, 0), place(0, 0, step_b), near + (step_a - 1) * near_x + step_b - 1
        else:
            for step_a in range(1, rows_x):
                for step_b in range(1, rows_y):
                    yield place(behind, 0, step_a), place(0, step_b, 0), near + (step_a - 1) * near_y + step_b - 1

    def column(behind):
        if not isinstance(behind, int):
            arrived(place(behind, 0, 0))
        for shard, target, slot in both_ways(behind):
            start(shard, target, send_near.at[behind, slot])

    def neighbours(behind):
        def along(first_axis):
            for shard, target, slot in onward(behind, first_axis):
                inner = (rows_x if first_axis == "y" else rows_y) - 1
                if (slot - near) % inner == 0:
                    arrived(shard)
                start(shard, target, send_near.at[behind, slot])
            if first_axis == "y":
                if near_x == 0:
                    for step in range(1, rows_y):
                        arrived(place(behind, step, 0))
                for step in range(1, rows_x):
                    arrived(place(behind, 0, step))
            else:
                if near_y == 0:
                    for step in range(1, rows_x):
                        arrived(place(behind, 0, step))
                for step in range(1, rows_y):
                    arrived(place(behind, step, 0))

        pl.when(core == 0)(functools.partial(along, "y"))
        pl.when(core == 1)(functools.partial(along, "x"))

    def corners(behind):
        for off_y in range(1, rows_y):
            for off_x in range(1, rows_x):
                arrived(place(behind, off_y, off_x))

    def far(step):
        return copies(me, (mine_z + step) * plane + me % plane, send_far.at[step])

    column(0)
    for step in reversed(range(1, depth)):

        def send_up(step=step):
            for copy in far(step):
                copy.start()

        pl.when(mine_z + step < depth)(send_up)

    def attend(shard, own):
        gates = cums[shard]
        picked = bf16_pieces(gates[:heads_small] * (-math.sqrt(size_small)))
        if extra_s > 3 * heads_small:
            picked.append(jnp.zeros((extra_s - 3 * heads_small, tokens), jnp.float32))
        table[shard, :extra_s, :] = jnp.concatenate(picked, axis=0).astype(jnp.bfloat16)
        picked = bf16_pieces(gates[heads_small:heads] * (-math.sqrt(size_large)))
        if extra_l > 3 * heads_large:
            picked.append(jnp.zeros((extra_l - 3 * heads_large, tokens), jnp.float32))
        table[shard, gate_l:, :] = jnp.concatenate(picked, axis=0).astype(jnp.bfloat16)
        for h in range(heads):
            small = h < heads_small
            size = size_small if small else size_large
            scale = size ** (-0.5) * log2e
            query = qs[h] if small else ql[h - heads_small]
            keys = table[shard, :small_v, :] if small else table[shard, large_k:, :]
            values = table[shard, small_v:large_v, :] if small else table[shard, large_v:large_k, :]
            acc_ref, number = (acc_s, h) if small else (acc_l, h - heads_small)
            scores = jnp.dot(query, keys, preferred_element_type=jnp.float32)
            if own:
                key_pos = lax.broadcasted_iota(jnp.int32, (tokens, tokens), 1)
                query_pos = lax.broadcasted_iota(jnp.int32, (tokens, tokens), 0)
                scores = jnp.where(key_pos <= query_pos, scores, far_score)
            parts = [scores[:, j * 128:(j + 1) * 128] for j in range(tokens // 128)]
            newest = jnp.max(functools.reduce(jnp.maximum, parts), axis=-1, keepdims=True)
            if own:
                newest = jnp.broadcast_to(newest, (tokens, 128))
            else:
                before = top[h]
                newest = jnp.maximum(before, newest)
                factor = jnp.exp2((before - newest) * scale)
            scaled = newest * scale
            found = [jnp.exp2(part * scale - scaled) for part in parts]
            partial_sum = functools.reduce(jnp.add, found)
            product = lax.dot_general(
                jnp.concatenate(found, axis=1).astype(jnp.bfloat16), values,
                (((1,), (1,)), ((), ())), preferred_element_type=jnp.float32)
            top[h] = newest
            if own:
                total[h] = partial_sum
                acc_ref[number] = product
            else:
                total[h] = total[h] * factor + partial_sum
                acc_ref[number] = acc_ref[number] * factor[:, :size] + product

    attend(me, True)
    pl.when(mine_z >= 1)(lambda: column(jnp.int32(1)))
    neighbours(0)
    order = [(0, 0)] + [(step, 0) for step in range(1, rows_y)] + [(0, step) for step in range(1, rows_x)]
    order += [(a, b) for a in range(1, rows_y) for b in range(1, rows_x)]

    def step_of(number, _):
        behind = number // plane
        turn = number % plane
        pl.when((turn == 0) & (behind + 1 <= mine_z))(lambda: column(behind + 1))
        pl.when(turn == min(2, plane - 1))(lambda: corners(behind))
        pl.when((turn == plane - 1) & (behind + 1 <= mine_z))(lambda: neighbours(behind + 1))
        off_y = jnp.int32(0)
        off_x = jnp.int32(0)
        for index, (a, b) in enumerate(order):
            off_y = jnp.where(turn == index, a, off_y)
            off_x = jnp.where(turn == index, b, off_x)
        shard = place(behind, off_y, off_x)
        across(shard, 1 - core).wait_recv()
        pl.when(shard < me)(lambda: attend(shard, False))
        return 0

    lax.fori_loop(1, (mine_z + 1) * plane, step_of, 0)

    width_s = heads_small * size_small
    width_l = heads_large * size_large
    for mine in (False, True):
        rows = pl.ds(pl.multiple_of((core if mine else 1 - core) * keep, keep), keep)
        shown = []
        for h in range(heads):
            small = h < heads_small
            sums = jnp.sum(total[h, rows, :], axis=-1, keepdims=True)
            values = acc_s[h, rows, :] if small else acc_l[h - heads_small, rows, :]
            shown.append((values / sums).astype(jnp.bfloat16))
        joined_s = jnp.concatenate(shown[:heads_small], axis=1)
        joined_l = jnp.concatenate(shown[heads_small:], axis=1)
        if mine:
            whole[:, pl.ds(pl.multiple_of(core * width_s, 128), width_s)] = joined_s
            whole[:, pl.ds(pl.multiple_of(2 * width_s + core * width_l, 128), width_l)] = joined_l
        else:
            stage[:, :width_s] = joined_s
            stage[:, width_s:] = joined_l

    def swap(which):
        return (
            pltpu.make_async_remote_copy(
                src_ref=stage.at[:, pl.ds(0, width_s)],
                dst_ref=whole.at[:, pl.ds(pl.multiple_of(which * width_s, 128), width_s)],
                send_sem=swap_send.at[0], recv_sem=swap_recv.at[0],
                device_id=(me, 1 - core), device_id_type=MESH),
            pltpu.make_async_remote_copy(
                src_ref=stage.at[:, pl.ds(width_s, width_l)],
                dst_ref=whole.at[:, pl.ds(pl.multiple_of(2 * width_s + which * width_l, 128), width_l)],
                send_sem=swap_send.at[1], recv_sem=swap_recv.at[1],
                device_id=(me, 1 - core), device_id_type=MESH),
        )

    for copy in swap(core):
        copy.start()
    for load in loads:
        load.wait()
    for copy in swap(1 - core):
        copy.wait_recv()
    span_w = 512

    def project(number, squares):
        span = pl.ds(pl.multiple_of(number * span_w, span_w), span_w)
        part = jnp.dot(whole[...], weights[:, span], preferred_element_type=jnp.float32)
        mixer[:, span] = part
        square = part * part
        return squares + functools.reduce(jnp.add, [square[:, j * 128:(j + 1) * 128] for j in range(span_w // 128)])

    squares = lax.fori_loop(0, columns // span_w, project, jnp.zeros((keep, 128), jnp.float32))
    mean = jnp.sum(squares, axis=-1, keepdims=True) * (1.0 / columns)
    mixed = (
        residual[...].astype(jnp.float32) + mixer[...] * lax.rsqrt(mean + norm_eps) * gain_mix[...]
    ).astype(jnp.bfloat16)
    mixed_ref[...] = mixed
    routed = rms_scale(mixed.astype(jnp.float32), gain_route[...])


    routed = routed.astype(jnp.bfloat16)
    slot_rows = lax.broadcasted_iota(jnp.int32, (slots, keep), 0).astype(jnp.float32)
    for group in range(depth):
        table_of = jnp.where((slot_rows == routing[1:2]) & (routing[0:1] == group), 1.0, 0.0).astype(jnp.bfloat16)
        out_rows[group] = jnp.dot(table_of, routed, preferred_element_type=jnp.float32).astype(jnp.bfloat16)
    in_rows[mine_z] = out_rows[mine_z]
    metas[mine_z] = out_meta[mine_z]

    def along(other, slot):
        target = (other * plane + me % plane, core)
        return (
            pltpu.make_async_remote_copy(
                src_ref=out_rows.at[other], dst_ref=in_rows.at[slot], send_sem=send_rows.at[other],
                recv_sem=recv_rows.at[slot], device_id=target, device_id_type=MESH),
            pltpu.make_async_remote_copy(
                src_ref=out_meta.at[other], dst_ref=metas.at[slot], send_sem=send_meta.at[other],
                recv_sem=recv_meta.at[slot], device_id=target, device_id_type=MESH),
        )

    def outward(source, other, slot):
        return pltpu.make_async_remote_copy(
            src_ref=spread.at[source, other], dst_ref=received.at[source, slot],
            send_sem=send_block.at[source, other], recv_sem=recv_block.at[source, slot],
            device_id=(mine_z * plane + other // cores, other % cores), device_id_type=MESH)

    def inward(source, other, slot):
        return pltpu.make_async_remote_copy(
            src_ref=outs.at[source, other], dst_ref=back.at[source, slot],
            send_sem=send_back.at[source, other], recv_sem=recv_back.at[source, slot],
            device_id=(mine_z * plane + other // cores, other % cores), device_id_type=MESH)

    def homeward(other, slot):
        return pltpu.make_async_remote_copy(
            src_ref=combined.at[other], dst_ref=final.at[slot], send_sem=send_home.at[other],
            recv_sem=recv_home.at[slot], device_id=(other * plane + me % plane, core), device_id_type=MESH)

    steps = distances(depth)
    for step in steps[1:]:
        other = mine_z + step

        def launch(other=other):
            for copy in along(other, mine_z):
                copy.start()

        pl.when((other >= 0) & (other < depth))(launch)

    def flat(ref, source):
        if capacity % 16:
            return jnp.concatenate(
                [ref[source, lane].astype(jnp.float32) for lane in range(lanes)], axis=0).astype(jnp.bfloat16)
        return ref[source].reshape(count, columns)

    def split(ref, source, values, span):
        for lane in range(lanes):
            ref[source, lane, :, span] = values[lane * capacity:(lane + 1) * capacity].astype(jnp.bfloat16)

    def expand(source):
        def landed():
            for copy in along(source, source):
                copy.wait_recv()

        pl.when(source != mine_z)(landed)
        wanted = lax.broadcasted_iota(jnp.int32, (count, slots), 0).astype(jnp.float32) + 1.0
        spots = jnp.where(
            (wanted == metas[source, 0:1, :slots]) | (wanted == metas[source, 1:2, :slots]), 1.0, 0.0
        ).astype(jnp.bfloat16)
        split(spread, source, jnp.dot(spots, in_rows[source], preferred_element_type=jnp.float32), slice(None))
        received[source, here] = spread[source, here]
        for move in range(1, lanes):
            outward(source, (here + move) % lanes, here).start()

    tile = 256

    def compute(source):
        for move in range(1, lanes):
            outward(source, (here + move) % lanes, (here + move) % lanes).wait_recv()
        rows = flat(received, source)

        def enter(number, _):
            span = pl.ds(pl.multiple_of(number * tile, tile), tile)
            gate = jnp.dot(rows, gate_w[:, span], preferred_element_type=jnp.float32)
            up = jnp.dot(rows, up_w[:, span], preferred_element_type=jnp.float32)
            hidden[:, span] = (jax.nn.silu(gate) * up).astype(jnp.bfloat16)
            return 0

        lax.fori_loop(0, gate_w.shape[1] // tile, enter, 0)

        def leave(number, _):
            span = pl.ds(pl.multiple_of(number * 2 * tile, 2 * tile), 2 * tile)
            split(outs, source, jnp.dot(hidden[...], down_w[:, span], preferred_element_type=jnp.float32), span)
            return 0

        lax.fori_loop(0, columns // (2 * tile), leave, 0)
        back[source, here] = outs[source, here]
        for move in range(1, lanes):
            inward(source, (here + move) % lanes, here).start()

    def combine(source):
        for move in range(1, lanes):
            inward(source, (here + move) % lanes, (here + move) % lanes).wait_recv()
        wanted = lax.broadcasted_iota(jnp.int32, (count, width), 0).astype(jnp.float32) + 1.0
        shares = jnp.where(wanted == metas[source, 0:1, :], metas[source, 2:3, :], 0.0)
        shares = shares + jnp.where(wanted == metas[source, 1:2, :], metas[source, 3:4, :], 0.0)
        shares = shares.T[:slots]
        high = shares.astype(jnp.bfloat16)
        low = (shares - high.astype(jnp.float32)).astype(jnp.bfloat16)
        picked = flat(back, source)
        mixed = jnp.dot(high, picked, preferred_element_type=jnp.float32) + jnp.dot(
            low, picked, preferred_element_type=jnp.float32)

        def away():
            combined[source] = mixed.astype(jnp.bfloat16)
            homeward(source, mine_z).start()

        def stay():
            final[source] = mixed.astype(jnp.bfloat16)

        pl.when(source != mine_z)(away)
        pl.when(source == mine_z)(stay)

    plans = plan_of(depth)

    def turn_of(turn, _):
        found = jnp.int32(0)
        for z in range(depth):
            for index, (kind, source) in enumerate(plans[z]):
                found = jnp.where((mine_z == z) & (turn == index), kind * depth + source, found)
        kind = found // depth
        source = found % depth
        pl.when(kind == 0)(lambda: expand(source))
        pl.when(kind == 1)(lambda: compute(source))
        pl.when(kind == 2)(lambda: combine(source))
        return 0

    for load in expert_loads:
        load.wait()
    lax.fori_loop(0, 3 * depth, turn_of, 0)
    for step in steps[1:]:
        other = mine_z + step

        def settle(other=other):
            homeward(other, other).wait_recv()
            homeward(other, mine_z).wait_send()
            for copy in along(other, mine_z):
                copy.wait_send()

        pl.when((other >= 0) & (other < depth))(settle)
    for source in range(depth):
        for move in range(1, lanes):
            outward(source, (here + move) % lanes, here).wait_send()
            inward(source, (here + move) % lanes, here).wait_send()
    for step in range(1, depth):

        def sent_up(step=step):
            for copy in far(step):
                copy.wait_send()

        pl.when(mine_z + step < depth)(sent_up)

    def sent(behind, _):
        for shard, target, slot in both_ways(behind):
            for copy in copies(shard, target, send_near.at[behind, slot]):
                copy.wait_send()
        for slot in range(near, near + near_y * near_x):
            for copy in copies(me, me, send_near.at[behind, slot]):
                copy.wait_send()

        def crossed(number, _):
            shard = (mine_z - behind) * plane + number
            pl.when(shard != me)(lambda: across(shard, core).wait_send())
            return 0

        lax.fori_loop(0, plane, crossed, 0)
        return 0

    lax.fori_loop(0, mine_z + 1, sent, 0)
    for copy in swap(core):
        copy.wait_send()
    eye = lax.broadcasted_iota(jnp.int32, (keep, keep), 0) == lax.broadcasted_iota(jnp.int32, (keep, keep), 1)
    slot_all = lax.broadcasted_iota(jnp.int32, (keep, depth * slots), 1).astype(jnp.float32)
    places = jnp.where(slot_all == as_column(routing[0:1] * slots + routing[1:2], eye), 1.0, 0.0).astype(jnp.bfloat16)
    blended = jnp.dot(places, final[...].reshape(depth * slots, columns), preferred_element_type=jnp.float32)
    result_ref[...] = (
        mixed_ref[...].astype(jnp.float32) + rms_scale(blended, gain_ref[...])
    ).astype(jnp.bfloat16)


def layer(dims, queries_small, queries_large, kv_small, kv_large, cum_small, cum_large, residual, gain_mix, gain_route, route, bias, gain_blend, out_small, out_large, w_gate, w_up, w_down):
    shards = lax.axis_size("sp")
    depth, rows_y, rows_x = dims
    tokens = queries_small.shape[0]
    heads_small = cum_small.shape[0]
    heads_large = cum_large.shape[0]
    size_small = kv_small.shape[1] // 2
    size_large = kv_large.shape[1] // 2
    heads = heads_small + heads_large
    extra_s = round_up(3 * heads_small, 32)
    extra_l = round_up(3 * heads_large, 16)
    table_rows = extra_s + 2 * size_small + 2 * size_large + extra_l
    near = rows_y + rows_x - 2 + (rows_y - 1) * (rows_x - 1)
    keep, columns = residual.shape
    lanes = lax.axis_size(("sp", "tp")) // depth
    capacity = 4 * keep // (depth * lanes)
    slots = capacity * lanes // 2
    width = round_up(slots, 128)
    inner = w_gate.shape[2]
    joined = out_small.shape[0] + out_large.shape[0]
    dma = pltpu.SemaphoreType.DMA
    vmem = pl.BlockSpec(memory_space=pltpu.VMEM)
    hbm = pl.BlockSpec(memory_space=pl.ANY)
    bf16, f32 = jnp.bfloat16, jnp.float32
    rows = pltpu.VMEM((depth, slots, columns), bf16)
    blocks = pltpu.VMEM((depth, lanes, capacity, columns), bf16)
    meta = pltpu.VMEM((depth, 8, width), f32)
    return pl.pallas_call(
        functools.partial(layer_kernel, dims, (heads_small, heads_large, size_small, size_large)),
        out_shape=jax.ShapeDtypeStruct(residual.shape, bf16),
        in_specs=[vmem] * 12 + [hbm] * 5,
        out_specs=vmem,
        scratch_shapes=[
            pltpu.VMEM((shards, table_rows, tokens), bf16),
            pltpu.VMEM((shards, heads, tokens), f32),
            pltpu.VMEM((heads_small, tokens, extra_s + size_small), bf16),
            pltpu.VMEM((heads_large, tokens, size_large + extra_l), bf16),
            pltpu.VMEM((heads, tokens, 128), f32),
            pltpu.VMEM((heads, tokens, 128), f32),
            pltpu.VMEM((heads_small, tokens, size_small), f32),
            pltpu.VMEM((heads_large, tokens, size_large), f32),
            pltpu.VMEM((keep, heads_small * size_small + heads_large * size_large), bf16),
            pltpu.VMEM((keep, joined), bf16),
            pltpu.VMEM((joined, columns), bf16),
            pltpu.VMEM((keep, columns), f32),
            pltpu.VMEM((keep, columns), bf16),
            pltpu.VMEM((8, keep), f32),
            rows, rows, meta, meta, blocks, blocks, blocks, blocks, rows, rows,
            pltpu.VMEM((lanes * capacity, inner), bf16),
            pltpu.VMEM((columns, inner), bf16),
            pltpu.VMEM((columns, inner), bf16),
            pltpu.VMEM((inner, columns), bf16),
            dma((depth, 2)), dma((depth, near, 2)), dma((shards,)), dma((shards,)), dma((shards,)), dma((shards,)),
            dma((2,)), dma((2,)), dma((5,)),
            dma((depth,)), dma((depth,)), dma((depth,)), dma((depth,)),
            dma((depth, lanes)), dma((depth, lanes)), dma((depth, lanes)), dma((depth, lanes)),
            dma((depth,)), dma((depth,)),
        ],
        compiler_params=pltpu.CompilerParams(
            collective_id=0, has_side_effects=True, vmem_limit_bytes=66 * 1000 * 1000),
        name="layer",
    )(queries_small, queries_large, kv_small, kv_large, cum_small, cum_large, residual,
      gain_mix.reshape(1, columns), gain_route.reshape(1, columns), route, bias.reshape(1, keep),
      gain_blend.reshape(1, columns), out_small, out_large, w_gate, w_up, w_down)


def on_device(
    dims,
    queries_small,
    queries_large,
    kv_small,
    kv_large,
    cum_small,
    cum_large,
    residual,
    out_small,
    out_large,
    gain_mix,
    gain_route,
    gain_blend,
    w_gate,
    w_up,
    w_down,
    route,
    route_bias,
):
    return layer(
        dims, queries_small, queries_large, kv_small, kv_large, cum_small, cum_large, residual,
        gain_mix, gain_route, route, route_bias, gain_blend, out_small, out_large, w_gate, w_up, w_down,
    )


def solution(mesh):
    in_specs = (
        P("sp", "tp"),
        P("sp", "tp"),
        P("sp", None),
        P("sp", None),
        P("tp", "sp"),
        P("tp", "sp"),
        P(("sp", "tp"), None),
        P(),
        P(),
        P(),
        P(),
        P(),
        P(("sp", "tp"), None, None),
        P(("sp", "tp"), None, None),
        P(("sp", "tp"), None, None),
        P(None, ("sp", "tp")),
        P(("sp", "tp")),
    )
    out_specs = P(("sp", "tp"), None)
    return jax.shard_map(
        functools.partial(on_device, mesh_shape(mesh)), mesh=mesh, in_specs=in_specs, out_specs=out_specs, check_vma=False
    )
```

```python
import functools
import math

import jax
import jax.numpy as jnp
from jax import lax
from jax.experimental import pallas as pl
from jax.experimental.pallas import tpu as pltpu
from jax.sharding import PartitionSpec as P

norm_eps = 1e-06
far_score = -1e30
log2e = math.log2(math.e)
MESH = pl.DeviceIdType.MESH


def rms_scale(values, gain_row):
    return (
        values * lax.rsqrt(jnp.mean(values * values, axis=-1, keepdims=True) + norm_eps) * gain_row
    )


def mesh_shape(mesh):
    coords = [tuple(device.coords) for device in mesh.devices.reshape(-1)]
    return tuple(1 + max(c[axis] for c in coords) - min(c[axis] for c in coords) for axis in (2, 1, 0))


def bf16_pieces(values):
    high = values.astype(jnp.bfloat16)
    rest = values - high.astype(jnp.float32)
    middle = rest.astype(jnp.bfloat16)
    low = (rest - middle.astype(jnp.float32)).astype(jnp.bfloat16)
    return [high.astype(jnp.float32), middle.astype(jnp.float32), low.astype(jnp.float32)]


def round_up(value, unit):
    return -(-value // unit) * unit


def greet(depth, plane, cores, me, core):
    barrier = pltpu.get_barrier_semaphore()
    lanes = plane * cores
    here = me % plane * cores + core
    for step in range(1, depth):
        target = (me // plane + step) % depth * plane + me % plane
        pl.semaphore_signal(barrier, inc=1, device_id=(target, core), device_id_type=MESH)
    for step in range(1, lanes):
        other = (here + step) % lanes
        target = me // plane * plane + other // cores
        pl.semaphore_signal(barrier, inc=1, device_id=(target, other % cores), device_id_type=MESH)
    return depth - 1 + lanes - 1


def distances(depth):
    found = [0]
    for step in range(1, depth):
        found += [step, -step]
    return found


def as_column(row, eye):
    return jnp.sum(jnp.where(eye, row, 0.0), axis=1, keepdims=True)


def plan_of(depth, parts):
    if depth == 4 and parts == 2:
        texts = (
            ("E00 E01 E10 E11 F0 F1 E20 E30 E21 E31 C10 F2 C11 F3 C20 C00 C01 C21 C30 C31", (3, 1, 2)),
            ("E00 E01 E10 E20 E21 E11 F0 F2 C00 C20 E30 E31 C21 C01 F3 F1 C30 C10 C31 C11", (3, 2, 0)),
            ("E20 E30 E10 E31 E11 E00 F3 C30 E01 F1 C31 E21 C10 F0 C11 F2 C00 C01 C20 C21", (1, 0, 3)),
            ("E10 E11 E00 E01 F1 F0 E30 C00 C10 E20 C01 E21 E31 C11 F2 F3 C20 C21 C30 C31", (2, 0, 1)),
        )
        kinds = {"F": 0, "E0": 1, "E1": 2, "C0": 3, "C1": 4}
        plans = [[(kinds[word[0] + word[2:]], int(word[1])) for word in text.split()] for text, _ in texts]
        return plans, [sends for _, sends in texts]
    plans, sends = [], []
    for z in range(depth):
        order = [z + step for step in distances(depth) if 0 <= z + step < depth]
        plan = []
        for turn in range(depth + 2):
            if turn < depth:
                plan += [(1 + part, order[turn]) for part in range(parts)]
            if 1 <= turn <= depth:
                plan += [(0, order[turn - 1])]
            if turn >= 2:
                plan += [(1 + parts + part, order[turn - 2]) for part in range(parts)]
        plans.append(plan)
        sends.append(order[1:])
    return plans, sends


def layer_kernel(
    dims, head_shape,
    q_small, q_large, kv_small, kv_large, cum_small, cum_large, residual, gain_mix, gain_route, route_ref, bias_ref, gain_ref,
    out_small, out_large, w_gate, w_up, w_down,
    result_ref,
    table, cums, qs, ql, top, total, acc_s, acc_l, stage, whole, weights, mixer, mixed_ref, routing,
    out_rows, in_rows, out_meta, metas, spread, received, outs, back, combined, final, hidden, gate_w, up_w, down_w,
    send_far, send_near, send_core, recv_kv, recv_cum, recv_core, swap_send, swap_recv, load_sem,
    send_rows, recv_rows, send_meta, recv_meta, send_block, recv_block, send_back, recv_back, send_home, recv_home,
):
    heads_small, heads_large, size_small, size_large = head_shape
    depth, rows_y, rows_x = dims
    plane = rows_y * rows_x
    me = lax.axis_index("sp")
    core = lax.axis_index("tp")
    mine_z = me // plane
    mine_y = me % plane // rows_x
    mine_x = me % rows_x
    tokens = q_small.shape[0]
    _, lanes, capacity, columns = spread.shape
    cores = lanes // (dims[1] * dims[2])
    slots = in_rows.shape[1]
    width = metas.shape[2]
    keep = residual.shape[0]
    count = lanes * capacity
    here = me % plane * cores + core
    heads = heads_small + heads_large
    extra_s = round_up(3 * heads_small, 32)
    extra_l = round_up(3 * heads_large, 16)
    wire = 2 * size_small + 2 * size_large
    half = wire // 2
    small_v = extra_s + size_small
    large_v = small_v + size_small
    large_k = large_v + size_large
    gate_l = extra_s + wire

    loads = (
        pltpu.make_async_copy(out_small, weights.at[pl.ds(0, out_small.shape[0])], load_sem.at[0]),
        pltpu.make_async_copy(
            out_large, weights.at[pl.ds(out_small.shape[0], out_large.shape[0])], load_sem.at[1]),
    )
    expert_loads = (
        pltpu.make_async_copy(w_gate.at[0], gate_w, load_sem.at[2]),
        pltpu.make_async_copy(w_up.at[0], up_w, load_sem.at[3]),
        pltpu.make_async_copy(w_down.at[0], down_w, load_sem.at[4]),
    )
    for load in loads + expert_loads:
        load.start()
    greeted = greet(depth, plane, cores, me, core)
    def turned(block):
        width = block.shape[1]
        eye = jnp.where(
            lax.broadcasted_iota(jnp.int32, (width, width), 0) == lax.broadcasted_iota(jnp.int32, (width, width), 1),
            1.0, 0.0).astype(jnp.bfloat16)
        return lax.dot_general(
            eye, block, (((1,), (1,)), ((), ())), preferred_element_type=jnp.float32).astype(jnp.bfloat16)

    table[me, extra_s:large_v, :] = turned(kv_small[...])
    table[me, large_k:gate_l, :] = turned(kv_large[:, :size_large])
    table[me, large_v:large_k, :] = turned(kv_large[:, size_large:])
    cums[me, :heads_small] = cum_small[...]
    cums[me, heads_small:heads] = cum_large[...]

    lanes_s = lax.broadcasted_iota(jnp.int32, (tokens, extra_s), 1)
    lanes_l = lax.broadcasted_iota(jnp.int32, (tokens, extra_l), 1)
    for h in range(heads_small):
        picks = jnp.where((lanes_s % heads_small == h) & (lanes_s < 3 * heads_small), 1.0, 0.0)
        qs[h] = jnp.concatenate(
            [picks.astype(jnp.bfloat16), q_small[:, h * size_small:(h + 1) * size_small]], axis=1)
    for h in range(heads_large):
        picks = jnp.where((lanes_l % heads_large == h) & (lanes_l < 3 * heads_large), 1.0, 0.0)
        ql[h] = jnp.concatenate(
            [q_large[:, h * size_large:(h + 1) * size_large], picks.astype(jnp.bfloat16)], axis=1)
    row_of = lax.broadcasted_iota(jnp.int32, (keep, keep), 0)
    lane_of = lax.broadcasted_iota(jnp.int32, (keep, keep), 1)
    eye = row_of == lane_of
    before = row_of < lane_of
    ids = route_ref[...].astype(jnp.float32)
    first, second = ids[0:1], ids[1:2]
    groups = jnp.floor((first + 0.5) * (1.0 / lanes))
    groups_col = as_column(groups, eye)
    first_col = as_column(first, eye)
    second_col = as_column(second, eye)

    def total_rows(mask):
        return jnp.sum(jnp.where(mask, 1.0, 0.0), axis=0, keepdims=True)

    ranks = total_rows((groups_col == groups) & before)
    places_first = (first - groups * lanes) * capacity + total_rows((first_col == first) & before) + 1.0
    places_second = (
        (second - groups * lanes) * capacity
        + total_rows(first_col == second) + total_rows((second_col == second) & before) + 1.0
    )
    bias = bias_ref[...]
    facts = [as_column(fact, eye) for fact in (places_first, places_second, jax.nn.sigmoid(bias), jax.nn.sigmoid(-bias))]
    ranks_col = as_column(ranks, eye)
    slot_lanes = lax.broadcasted_iota(jnp.int32, (keep, width), 1).astype(jnp.float32)
    for group in range(depth):
        chosen = (slot_lanes == ranks_col) & (groups_col == group)
        rows = [jnp.sum(jnp.where(chosen, fact, 0.0), axis=0, keepdims=True) for fact in facts]
        out_meta[group] = jnp.concatenate(rows + [jnp.zeros((4, width), jnp.float32)], axis=0)
    routing[0:1] = groups
    routing[1:2] = ranks
    pl.semaphore_wait(pltpu.get_barrier_semaphore(), greeted)

    def place(behind, off_y, off_x):
        return (mine_z - behind) * plane + (mine_y + off_y) % rows_y * rows_x + (mine_x + off_x) % rows_x

    def copies(shard, target, sems):
        part = table.at[shard, pl.ds(extra_s + core * half, half)]
        return (
            pltpu.make_async_remote_copy(
                src_ref=part, dst_ref=part, send_sem=sems.at[0], recv_sem=recv_kv.at[shard],
                device_id=(target, core), device_id_type=MESH),
            pltpu.make_async_remote_copy(
                src_ref=cums.at[shard], dst_ref=cums.at[shard], send_sem=sems.at[1],
                recv_sem=recv_cum.at[shard], device_id=(target, core), device_id_type=MESH),
        )

    def start(shard, target, sems):
        for copy in copies(shard, target, sems):
            copy.start()

    def across(shard, which):
        part = table.at[shard, pl.ds(extra_s + which * half, half)]
        return pltpu.make_async_remote_copy(
            src_ref=part, dst_ref=part, send_sem=send_core.at[shard], recv_sem=recv_core.at[shard],
            device_id=(me, 1 - core), device_id_type=MESH)

    def arrived(shard):
        for copy in copies(shard, me, send_far.at[0]):
            copy.wait_recv()
        across(shard, core).start()

    near_y = rows_y - 1
    near_x = rows_x - 1
    near = near_y + near_x

    def both_ways(behind):
        shard = place(behind, 0, 0)
        for step in range(1, rows_x):
            yield shard, place(0, 0, step), near_y + step - 1
        for step in range(1, rows_y):
            yield shard, place(0, step, 0), step - 1

    def onward(behind, first_axis):
        if first_axis == "y":
            for step_a in range(1, rows_y):
                for step_b in range(1, rows_x):
                    yield place(behind, step_a, 0), place(0, 0, step_b), near + (step_a - 1) * near_x + step_b - 1
        else:
            for step_a in range(1, rows_x):
                for step_b in range(1, rows_y):
                    yield place(behind, 0, step_a), place(0, step_b, 0), near + (step_a - 1) * near_y + step_b - 1

    def column(behind):
        if not isinstance(behind, int):
            arrived(place(behind, 0, 0))
        for shard, target, slot in both_ways(behind):
            start(shard, target, send_near.at[behind, slot])

    def neighbours(behind):
        def along(first_axis):
            for shard, target, slot in onward(behind, first_axis):
                inner = (rows_x if first_axis == "y" else rows_y) - 1
                if (slot - near) % inner == 0:
                    arrived(shard)
                start(shard, target, send_near.at[behind, slot])
            if first_axis == "y":
                if near_x == 0:
                    for step in range(1, rows_y):
                        arrived(place(behind, step, 0))
                for step in range(1, rows_x):
                    arrived(place(behind, 0, step))
            else:
                if near_y == 0:
                    for step in range(1, rows_x):
                        arrived(place(behind, 0, step))
                for step in range(1, rows_y):
                    arrived(place(behind, step, 0))

        pl.when(core == 0)(functools.partial(along, "y"))
        pl.when(core == 1)(functools.partial(along, "x"))

    def corners(behind):
        for off_y in range(1, rows_y):
            for off_x in range(1, rows_x):
                arrived(place(behind, off_y, off_x))

    def far(step):
        return copies(me, (mine_z + step) * plane + me % plane, send_far.at[step])

    column(0)
    for step in range(1, depth):

        def send_up(step=step):
            for copy in far(step):
                copy.start()

        pl.when(mine_z + step < depth)(send_up)

    def attend(shard, own):
        gates = cums[shard]
        picked = bf16_pieces(gates[:heads_small] * (-math.sqrt(size_small)))
        if extra_s > 3 * heads_small:
            picked.append(jnp.zeros((extra_s - 3 * heads_small, tokens), jnp.float32))
        table[shard, :extra_s, :] = jnp.concatenate(picked, axis=0).astype(jnp.bfloat16)
        picked = bf16_pieces(gates[heads_small:heads] * (-math.sqrt(size_large)))
        if extra_l > 3 * heads_large:
            picked.append(jnp.zeros((extra_l - 3 * heads_large, tokens), jnp.float32))
        table[shard, gate_l:, :] = jnp.concatenate(picked, axis=0).astype(jnp.bfloat16)
        for h in range(heads):
            small = h < heads_small
            size = size_small if small else size_large
            scale = size ** (-0.5) * log2e
            query = qs[h] if small else ql[h - heads_small]
            keys = table[shard, :small_v, :] if small else table[shard, large_k:, :]
            values = table[shard, small_v:large_v, :] if small else table[shard, large_v:large_k, :]
            acc_ref, number = (acc_s, h) if small else (acc_l, h - heads_small)
            scores = jnp.dot(query, keys, preferred_element_type=jnp.float32)
            if own:
                key_pos = lax.broadcasted_iota(jnp.int32, (tokens, tokens), 1)
                query_pos = lax.broadcasted_iota(jnp.int32, (tokens, tokens), 0)
                scores = jnp.where(key_pos <= query_pos, scores, far_score)
            parts = [scores[:, j * 128:(j + 1) * 128] for j in range(tokens // 128)]
            newest = jnp.max(functools.reduce(jnp.maximum, parts), axis=-1, keepdims=True)
            if own:
                newest = jnp.broadcast_to(newest, (tokens, 128))
            else:
                before = top[h]
                newest = jnp.maximum(before, newest)
                factor = jnp.exp2((before - newest) * scale)
            scaled = newest * scale
            found = [jnp.exp2(part * scale - scaled) for part in parts]
            partial_sum = functools.reduce(jnp.add, found)
            product = lax.dot_general(
                jnp.concatenate(found, axis=1).astype(jnp.bfloat16), values,
                (((1,), (1,)), ((), ())), preferred_element_type=jnp.float32)
            top[h] = newest
            if own:
                total[h] = partial_sum
                acc_ref[number] = product
            else:
                total[h] = total[h] * factor + partial_sum
                acc_ref[number] = acc_ref[number] * factor[:, :size] + product

    attend(me, True)
    neighbours(0)
    order = [(0, 0)] + [(step, 0) for step in range(1, rows_y)] + [(0, step) for step in range(1, rows_x)]
    order += [(a, b) for a in range(1, rows_y) for b in range(1, rows_x)]

    def step_of(number, _):
        behind = number // plane
        turn = number % plane
        pl.when((turn == jnp.where(behind == 0, min(1, plane - 1), 0)) & (behind + 1 <= mine_z))(lambda: column(behind + 1))
        pl.when(turn == min(2, plane - 1))(lambda: corners(behind))
        pl.when((turn == plane - 1) & (behind + 1 <= mine_z))(lambda: neighbours(behind + 1))
        off_y = jnp.int32(0)
        off_x = jnp.int32(0)
        for index, (a, b) in enumerate(order):
            off_y = jnp.where(turn == index, a, off_y)
            off_x = jnp.where(turn == index, b, off_x)
        shard = place(behind, off_y, off_x)
        across(shard, 1 - core).wait_recv()
        pl.when(shard < me)(lambda: attend(shard, False))
        return 0

    lax.fori_loop(1, (mine_z + 1) * plane, step_of, 0)

    width_s = heads_small * size_small
    width_l = heads_large * size_large
    for mine in (False, True):
        rows = pl.ds(pl.multiple_of((core if mine else 1 - core) * keep, keep), keep)
        shown = []
        for h in range(heads):
            small = h < heads_small
            sums = jnp.sum(total[h, rows, :], axis=-1, keepdims=True)
            values = acc_s[h, rows, :] if small else acc_l[h - heads_small, rows, :]
            shown.append((values / sums).astype(jnp.bfloat16))
        joined_s = jnp.concatenate(shown[:heads_small], axis=1)
        joined_l = jnp.concatenate(shown[heads_small:], axis=1)
        if mine:
            whole[:, pl.ds(pl.multiple_of(core * width_s, 128), width_s)] = joined_s
            whole[:, pl.ds(pl.multiple_of(2 * width_s + core * width_l, 128), width_l)] = joined_l
        else:
            stage[:, :width_s] = joined_s
            stage[:, width_s:] = joined_l

    def swap(which):
        return (
            pltpu.make_async_remote_copy(
                src_ref=stage.at[:, pl.ds(0, width_s)],
                dst_ref=whole.at[:, pl.ds(pl.multiple_of(which * width_s, 128), width_s)],
                send_sem=swap_send.at[0], recv_sem=swap_recv.at[0],
                device_id=(me, 1 - core), device_id_type=MESH),
            pltpu.make_async_remote_copy(
                src_ref=stage.at[:, pl.ds(width_s, width_l)],
                dst_ref=whole.at[:, pl.ds(pl.multiple_of(2 * width_s + which * width_l, 128), width_l)],
                send_sem=swap_send.at[1], recv_sem=swap_recv.at[1],
                device_id=(me, 1 - core), device_id_type=MESH),
        )

    for copy in swap(core):
        copy.start()
    for load in loads:
        load.wait()
    span_w = 512

    def half_product(which, span):
        cols_s = pl.ds(pl.multiple_of(which * width_s, 128), width_s)
        cols_l = pl.ds(pl.multiple_of(2 * width_s + which * width_l, 128), width_l)
        return jnp.dot(whole[:, cols_s], weights[cols_s, span], preferred_element_type=jnp.float32) + jnp.dot(
            whole[:, cols_l], weights[cols_l, span], preferred_element_type=jnp.float32)

    def project_own(number, _):
        span = pl.ds(pl.multiple_of(number * span_w, span_w), span_w)
        mixer[:, span] = half_product(core, span)
        return 0

    lax.fori_loop(0, columns // span_w, project_own, 0)
    for copy in swap(1 - core):
        copy.wait_recv()

    def project(number, squares):
        span = pl.ds(pl.multiple_of(number * span_w, span_w), span_w)
        part = mixer[:, span] + half_product(1 - core, span)
        mixer[:, span] = part
        square = part * part
        return squares + functools.reduce(jnp.add, [square[:, j * 128:(j + 1) * 128] for j in range(span_w // 128)])

    squares = lax.fori_loop(0, columns // span_w, project, jnp.zeros((keep, 128), jnp.float32))
    mean = jnp.sum(squares, axis=-1, keepdims=True) * (1.0 / columns)
    mixed = (
        residual[...].astype(jnp.float32) + mixer[...] * lax.rsqrt(mean + norm_eps) * gain_mix[...]
    ).astype(jnp.bfloat16)
    mixed_ref[...] = mixed
    routed = rms_scale(mixed.astype(jnp.float32), gain_route[...])


    routed = routed.astype(jnp.bfloat16)
    slot_rows = lax.broadcasted_iota(jnp.int32, (slots, keep), 0).astype(jnp.float32)
    for group in range(depth):
        table_of = jnp.where((slot_rows == routing[1:2]) & (routing[0:1] == group), 1.0, 0.0).astype(jnp.bfloat16)
        out_rows[group] = jnp.dot(table_of, routed, preferred_element_type=jnp.float32).astype(jnp.bfloat16)
    in_rows[mine_z] = out_rows[mine_z]
    metas[mine_z] = out_meta[mine_z]

    parts = recv_rows.shape[1]
    plans, sends = plan_of(depth, parts)
    extent = columns // parts

    def columns_of(part):
        return pl.ds(part * extent, extent)

    def along_rows(other, slot, part):
        return pltpu.make_async_remote_copy(
            src_ref=out_rows.at[other, :, columns_of(part)], dst_ref=in_rows.at[slot, :, columns_of(part)],
            send_sem=send_rows.at[other, part], recv_sem=recv_rows.at[slot, part],
            device_id=(other * plane + me % plane, core), device_id_type=MESH)

    def along_meta(other, slot):
        return pltpu.make_async_remote_copy(
            src_ref=out_meta.at[other], dst_ref=metas.at[slot], send_sem=send_meta.at[other],
            recv_sem=recv_meta.at[slot], device_id=(other * plane + me % plane, core), device_id_type=MESH)

    def outward(source, other, slot, part):
        return pltpu.make_async_remote_copy(
            src_ref=spread.at[source, other, :, columns_of(part)],
            dst_ref=received.at[source, slot, :, columns_of(part)],
            send_sem=send_block.at[source, other, part], recv_sem=recv_block.at[source, slot, part],
            device_id=(mine_z * plane + other // cores, other % cores), device_id_type=MESH)

    def inward(source, other, slot, part):
        return pltpu.make_async_remote_copy(
            src_ref=outs.at[source, other, :, columns_of(part)],
            dst_ref=back.at[source, slot, :, columns_of(part)],
            send_sem=send_back.at[source, other, part], recv_sem=recv_back.at[source, slot, part],
            device_id=(mine_z * plane + other // cores, other % cores), device_id_type=MESH)

    def homeward(other, slot, part):
        return pltpu.make_async_remote_copy(
            src_ref=combined.at[other, :, columns_of(part)], dst_ref=final.at[slot, :, columns_of(part)],
            send_sem=send_home.at[other, part], recv_sem=recv_home.at[slot, part],
            device_id=(other * plane + me % plane, core), device_id_type=MESH)

    steps = distances(depth)
    for index in range(depth - 1):
        other = jnp.int32(0)
        for z in range(depth):
            other = jnp.where(mine_z == z, sends[z][index], other)
        along_meta(other, mine_z).start()
        for part in range(parts):
            along_rows(other, mine_z, part).start()

    def flat(ref, source, span):
        if capacity % 16:
            return jnp.concatenate(
                [ref[source, lane, :, span].astype(jnp.float32) for lane in range(lanes)], axis=0).astype(jnp.bfloat16)
        found = ref[source, :, :, span]
        return found.reshape(count, found.shape[2])

    def split(ref, source, values, span):
        for lane in range(lanes):
            ref[source, lane, :, span] = values[lane * capacity:(lane + 1) * capacity].astype(jnp.bfloat16)

    def expand(source, part):
        span = columns_of(part)

        def landed():
            if part == 0:
                along_meta(source, source).wait_recv()
            along_rows(source, source, part).wait_recv()

        pl.when(source != mine_z)(landed)
        wanted = lax.broadcasted_iota(jnp.int32, (count, slots), 0).astype(jnp.float32) + 1.0
        spots = jnp.where(
            (wanted == metas[source, 0:1, :slots]) | (wanted == metas[source, 1:2, :slots]), 1.0, 0.0
        ).astype(jnp.bfloat16)
        split(spread, source, jnp.dot(spots, in_rows[source, :, span], preferred_element_type=jnp.float32), span)
        received[source, here, :, span] = spread[source, here, :, span]
        for move in range(1, lanes):
            outward(source, (here + move) % lanes, here, part).start()

    tile = 256

    def compute(source):
        for part in range(parts):
            for move in range(1, lanes):
                outward(source, (here + move) % lanes, (here + move) % lanes, part).wait_recv()
        rows = flat(received, source, slice(None))

        def enter(number, _):
            span = pl.ds(pl.multiple_of(number * tile, tile), tile)
            gate = jnp.dot(rows, gate_w[:, span], preferred_element_type=jnp.float32)
            up = jnp.dot(rows, up_w[:, span], preferred_element_type=jnp.float32)
            hidden[:, span] = (jax.nn.silu(gate) * up).astype(jnp.bfloat16)
            return 0

        lax.fori_loop(0, gate_w.shape[1] // tile, enter, 0)
        for part in range(parts):

            def leave(number, _):
                span = pl.ds(pl.multiple_of(part * extent + number * 2 * tile, 2 * tile), 2 * tile)
                split(outs, source, jnp.dot(hidden[...], down_w[:, span], preferred_element_type=jnp.float32), span)
                return 0

            lax.fori_loop(0, extent // (2 * tile), leave, 0)
            span = columns_of(part)
            back[source, here, :, span] = outs[source, here, :, span]
            for move in range(1, lanes):
                inward(source, (here + move) % lanes, here, part).start()

    def combine(source, part):
        span = columns_of(part)
        for move in range(1, lanes):
            inward(source, (here + move) % lanes, (here + move) % lanes, part).wait_recv()
        wanted = lax.broadcasted_iota(jnp.int32, (count, width), 0).astype(jnp.float32) + 1.0
        shares = jnp.where(wanted == metas[source, 0:1, :], metas[source, 2:3, :], 0.0)
        shares = shares + jnp.where(wanted == metas[source, 1:2, :], metas[source, 3:4, :], 0.0)
        shares = shares.T[:slots]
        high = shares.astype(jnp.bfloat16)
        low = (shares - high.astype(jnp.float32)).astype(jnp.bfloat16)
        picked = flat(back, source, span)
        mixed = jnp.dot(high, picked, preferred_element_type=jnp.float32) + jnp.dot(
            low, picked, preferred_element_type=jnp.float32)

        def away():
            combined[source, :, span] = mixed.astype(jnp.bfloat16)
            homeward(source, mine_z, part).start()

        def stay():
            final[source, :, span] = mixed.astype(jnp.bfloat16)

        pl.when(source != mine_z)(away)
        pl.when(source == mine_z)(stay)


    def turn_of(turn, _):
        found = jnp.int32(0)
        for z in range(depth):
            for index, (kind, source) in enumerate(plans[z]):
                found = jnp.where((mine_z == z) & (turn == index), kind * depth + source, found)
        kind = found // depth
        source = found % depth
        pl.when(kind == 0)(lambda: compute(source))
        for part in range(parts):
            pl.when(kind == 1 + part)(functools.partial(expand, source, part))
            pl.when(kind == 1 + parts + part)(functools.partial(combine, source, part))
        return 0

    for load in expert_loads:
        load.wait()
    lax.fori_loop(0, (1 + 2 * parts) * depth, turn_of, 0)
    for step in steps[1:]:
        other = mine_z + step

        def settle(other=other):
            along_meta(other, mine_z).wait_send()
            for part in range(parts):
                homeward(other, other, part).wait_recv()
                homeward(other, mine_z, part).wait_send()
                along_rows(other, mine_z, part).wait_send()

        pl.when((other >= 0) & (other < depth))(settle)
    for source in range(depth):
        for move in range(1, lanes):
            for part in range(parts):
                outward(source, (here + move) % lanes, here, part).wait_send()
                inward(source, (here + move) % lanes, here, part).wait_send()
    for step in range(1, depth):

        def sent_up(step=step):
            for copy in far(step):
                copy.wait_send()

        pl.when(mine_z + step < depth)(sent_up)

    def sent(behind, _):
        for shard, target, slot in both_ways(behind):
            for copy in copies(shard, target, send_near.at[behind, slot]):
                copy.wait_send()
        for slot in range(near, near + near_y * near_x):
            for copy in copies(me, me, send_near.at[behind, slot]):
                copy.wait_send()

        def crossed(number, _):
            shard = (mine_z - behind) * plane + number
            pl.when(shard != me)(lambda: across(shard, core).wait_send())
            return 0

        lax.fori_loop(0, plane, crossed, 0)
        return 0

    lax.fori_loop(0, mine_z + 1, sent, 0)
    for copy in swap(core):
        copy.wait_send()
    eye = lax.broadcasted_iota(jnp.int32, (keep, keep), 0) == lax.broadcasted_iota(jnp.int32, (keep, keep), 1)
    slot_all = lax.broadcasted_iota(jnp.int32, (keep, depth * slots), 1).astype(jnp.float32)
    places = jnp.where(slot_all == as_column(routing[0:1] * slots + routing[1:2], eye), 1.0, 0.0).astype(jnp.bfloat16)
    blended = jnp.dot(places, final[...].reshape(depth * slots, columns), preferred_element_type=jnp.float32)
    result_ref[...] = (
        mixed_ref[...].astype(jnp.float32) + rms_scale(blended, gain_ref[...])
    ).astype(jnp.bfloat16)


def padded_bytes(item):
    size = jnp.dtype(item.dtype).itemsize if jnp.issubdtype(item.dtype, jnp.floating) else 0
    lead = math.prod(item.shape[:-2]) if len(item.shape) > 1 else 0
    return size * lead * round_up(item.shape[-2], 32 // max(size, 1)) * round_up(item.shape[-1], 128) if lead else 0


def layer(dims, queries_small, queries_large, kv_small, kv_large, cum_small, cum_large, residual, gain_mix, gain_route, route, bias, gain_blend, out_small, out_large, w_gate, w_up, w_down):
    shards = lax.axis_size("sp")
    depth, rows_y, rows_x = dims
    tokens = queries_small.shape[0]
    heads_small = cum_small.shape[0]
    heads_large = cum_large.shape[0]
    size_small = kv_small.shape[1] // 2
    size_large = kv_large.shape[1] // 2
    heads = heads_small + heads_large
    extra_s = round_up(3 * heads_small, 32)
    extra_l = round_up(3 * heads_large, 16)
    table_rows = extra_s + 2 * size_small + 2 * size_large + extra_l
    near = rows_y + rows_x - 2 + (rows_y - 1) * (rows_x - 1)
    keep, columns = residual.shape
    lanes = lax.axis_size(("sp", "tp")) // depth
    capacity = 4 * keep // (depth * lanes)
    slots = capacity * lanes // 2
    width = round_up(slots, 128)
    parts = 2
    inner = w_gate.shape[2]
    joined = out_small.shape[0] + out_large.shape[0]
    dma = pltpu.SemaphoreType.DMA
    vmem = pl.BlockSpec(memory_space=pltpu.VMEM)
    hbm = pl.BlockSpec(memory_space=pl.ANY)
    bf16, f32 = jnp.bfloat16, jnp.float32
    rows = pltpu.VMEM((depth, slots, columns), bf16)
    blocks = pltpu.VMEM((depth, lanes, capacity, columns), bf16)
    meta = pltpu.VMEM((depth, 8, width), f32)
    scratch = [
        pltpu.VMEM((shards, table_rows, tokens), bf16),
        pltpu.VMEM((shards, heads, tokens), f32),
        pltpu.VMEM((heads_small, tokens, extra_s + size_small), bf16),
        pltpu.VMEM((heads_large, tokens, size_large + extra_l), bf16),
        pltpu.VMEM((heads, tokens, 128), f32),
        pltpu.VMEM((heads, tokens, 128), f32),
        pltpu.VMEM((heads_small, tokens, size_small), f32),
        pltpu.VMEM((heads_large, tokens, size_large), f32),
        pltpu.VMEM((keep, heads_small * size_small + heads_large * size_large), bf16),
        pltpu.VMEM((keep, joined), bf16),
        pltpu.VMEM((joined, columns), bf16),
        pltpu.VMEM((keep, columns), f32),
        pltpu.VMEM((keep, columns), bf16),
        pltpu.VMEM((8, keep), f32),
        rows, rows, meta, meta, blocks, blocks, blocks, blocks, rows, rows,
        pltpu.VMEM((lanes * capacity, inner), bf16),
        pltpu.VMEM((columns, inner), bf16),
        pltpu.VMEM((columns, inner), bf16),
        pltpu.VMEM((inner, columns), bf16),
        dma((depth, 2)), dma((depth, near, 2)), dma((shards,)), dma((shards,)), dma((shards,)), dma((shards,)),
        dma((2,)), dma((2,)), dma((5,)),
        dma((depth, parts)), dma((depth, parts)), dma((depth,)), dma((depth,)),
        dma((depth, lanes, parts)), dma((depth, lanes, parts)), dma((depth, lanes, parts)), dma((depth, lanes, parts)),
        dma((depth, parts)), dma((depth, parts)),
    ]
    needed = sum(padded_bytes(item) for item in scratch if isinstance(item, type(rows)))
    return pl.pallas_call(
        functools.partial(layer_kernel, dims, (heads_small, heads_large, size_small, size_large)),
        out_shape=jax.ShapeDtypeStruct(residual.shape, bf16),
        in_specs=[vmem] * 12 + [hbm] * 5,
        out_specs=vmem,
        scratch_shapes=scratch,
        compiler_params=pltpu.CompilerParams(
            collective_id=0, has_side_effects=True, vmem_limit_bytes=min(needed + 4 * 1024 * 1024, 66 * 1000 * 1000)),
        name="layer",
    )(queries_small, queries_large, kv_small, kv_large, cum_small, cum_large, residual,
      gain_mix.reshape(1, columns), gain_route.reshape(1, columns), route, bias.reshape(1, keep),
      gain_blend.reshape(1, columns), out_small, out_large, w_gate, w_up, w_down)


def on_device(
    dims,
    queries_small,
    queries_large,
    kv_small,
    kv_large,
    cum_small,
    cum_large,
    residual,
    out_small,
    out_large,
    gain_mix,
    gain_route,
    gain_blend,
    w_gate,
    w_up,
    w_down,
    route,
    route_bias,
):
    return layer(
        dims, queries_small, queries_large, kv_small, kv_large, cum_small, cum_large, residual,
        gain_mix, gain_route, route, route_bias, gain_blend, out_small, out_large, w_gate, w_up, w_down,
    )


def solution(mesh):
    in_specs = (
        P("sp", "tp"),
        P("sp", "tp"),
        P("sp", None),
        P("sp", None),
        P("tp", "sp"),
        P("tp", "sp"),
        P(("sp", "tp"), None),
        P(),
        P(),
        P(),
        P(),
        P(),
        P(("sp", "tp"), None, None),
        P(("sp", "tp"), None, None),
        P(("sp", "tp"), None, None),
        P(None, ("sp", "tp")),
        P(("sp", "tp")),
    )
    out_specs = P(("sp", "tp"), None)
    return jax.shard_map(
        functools.partial(on_device, mesh_shape(mesh)), mesh=mesh, in_specs=in_specs, out_specs=out_specs, check_vma=False
    )
```

```python
import functools
import math

import jax
import jax.numpy as jnp
from jax import lax
from jax.experimental import pallas as pl
from jax.experimental.pallas import tpu as pltpu
from jax.sharding import PartitionSpec as P

norm_eps = 1e-06
far_score = -1e30
log2e = math.log2(math.e)
MESH = pl.DeviceIdType.MESH


def rms_scale(values, gain_row):
    return (
        values * lax.rsqrt(jnp.mean(values * values, axis=-1, keepdims=True) + norm_eps) * gain_row
    )


def mesh_shape(mesh):
    coords = [tuple(device.coords) for device in mesh.devices.reshape(-1)]
    return tuple(1 + max(c[axis] for c in coords) - min(c[axis] for c in coords) for axis in (2, 1, 0))


def bf16_pieces(values):
    high = values.astype(jnp.bfloat16)
    rest = values - high.astype(jnp.float32)
    middle = rest.astype(jnp.bfloat16)
    low = (rest - middle.astype(jnp.float32)).astype(jnp.bfloat16)
    return [high.astype(jnp.float32), middle.astype(jnp.float32), low.astype(jnp.float32)]


def round_up(value, unit):
    return -(-value // unit) * unit


def greet(depth, plane, cores, me, core):
    barrier = pltpu.get_barrier_semaphore()
    lanes = plane * cores
    here = me % plane * cores + core
    for step in range(1, depth):
        target = (me // plane + step) % depth * plane + me % plane
        pl.semaphore_signal(barrier, inc=1, device_id=(target, core), device_id_type=MESH)
    for step in range(1, lanes):
        other = (here + step) % lanes
        target = me // plane * plane + other // cores
        pl.semaphore_signal(barrier, inc=1, device_id=(target, other % cores), device_id_type=MESH)
    return depth - 1 + lanes - 1


def distances(depth):
    found = [0]
    for step in range(1, depth):
        found += [step, -step]
    return found


def as_column(row, eye):
    return jnp.sum(jnp.where(eye, row, 0.0), axis=1, keepdims=True)


def plan_of(depth, parts):
    if depth == 4 and parts == 2:
        texts = (
            ("E00 E01 E10 E11 F0 F1 E20 E30 E21 E31 C10 F2 C11 F3 C20 C00 C01 C21 C30 C31", (3, 1, 2)),
            ("E00 E01 E10 E20 E21 E11 F0 F2 C00 C20 E30 E31 C21 C01 F3 F1 C30 C10 C31 C11", (3, 2, 0)),
            ("E20 E30 E10 E31 E11 E00 F3 C30 E01 F1 C31 E21 C10 F0 C11 F2 C00 C01 C20 C21", (1, 0, 3)),
            ("E10 E11 E00 E01 F1 F0 E30 C00 C10 E20 C01 E21 E31 C11 F2 F3 C20 C21 C30 C31", (2, 0, 1)),
        )
        kinds = {"F": 0, "E0": 1, "E1": 2, "C0": 3, "C1": 4}
        plans = [[(kinds[word[0] + word[2:]], int(word[1])) for word in text.split()] for text, _ in texts]
        return plans, [sends for _, sends in texts]
    plans, sends = [], []
    for z in range(depth):
        order = [z + step for step in distances(depth) if 0 <= z + step < depth]
        plan = []
        for turn in range(depth + 2):
            if turn < depth:
                plan += [(1 + part, order[turn]) for part in range(parts)]
            if 1 <= turn <= depth:
                plan += [(0, order[turn - 1])]
            if turn >= 2:
                plan += [(1 + parts + part, order[turn - 2]) for part in range(parts)]
        plans.append(plan)
        sends.append(order[1:])
    return plans, sends


def layer_kernel(
    dims, head_shape,
    q_small_in, q_large_in, kv_small_in, kv_large_in, cum_small_in, cum_large_in, residual_in, gain_mix_in, gain_route_in, route_ref_in, bias_ref_in, gain_ref_in,
    out_small, out_large, w_gate, w_up, w_down,
    result_ref,
    q_small, q_large, kv_small, kv_large, cum_small, cum_large, residual, gain_mix, gain_route, route_ref, bias_ref, gain_ref,
    table, cums, qs, ql, top, total, acc_s, acc_l, stage, whole, weights, mixer, mixed_ref, routing,
    out_rows, in_rows, out_meta, metas, spread, received, outs, back, combined, final, hidden, gate_w, up_w, down_w,
    send_far, send_near, send_core, recv_kv, recv_cum, recv_core, swap_send, swap_recv, load_sem,
    operand_sem, send_rows, recv_rows, send_meta, recv_meta, send_block, recv_block, send_back, recv_back, send_home, recv_home,
):
    heads_small, heads_large, size_small, size_large = head_shape
    depth, rows_y, rows_x = dims
    plane = rows_y * rows_x
    me = lax.axis_index("sp")
    core = lax.axis_index("tp")
    mine_z = me // plane
    mine_y = me % plane // rows_x
    mine_x = me % rows_x
    tokens = q_small.shape[0]
    _, lanes, capacity, columns = spread.shape
    cores = lanes // (dims[1] * dims[2])
    slots = in_rows.shape[1]
    width = metas.shape[2]
    keep = residual.shape[0]
    count = lanes * capacity
    here = me % plane * cores + core
    heads = heads_small + heads_large
    extra_s = round_up(3 * heads_small, 32)
    extra_l = round_up(3 * heads_large, 16)
    wire = 2 * size_small + 2 * size_large
    half = wire // 2
    small_v = extra_s + size_small
    large_v = small_v + size_small
    large_k = large_v + size_large
    gate_l = extra_s + wire

    loads = (
        pltpu.make_async_copy(out_small, weights.at[pl.ds(0, out_small.shape[0])], load_sem.at[0]),
        pltpu.make_async_copy(
            out_large, weights.at[pl.ds(out_small.shape[0], out_large.shape[0])], load_sem.at[1]),
    )
    expert_loads = (
        pltpu.make_async_copy(w_gate.at[0], gate_w, load_sem.at[2]),
        pltpu.make_async_copy(w_up.at[0], up_w, load_sem.at[3]),
        pltpu.make_async_copy(w_down.at[0], down_w, load_sem.at[4]),
    )
    moved = (
        (kv_small_in, kv_small), (kv_large_in, kv_large), (cum_small_in, cum_small), (cum_large_in, cum_large),
        (route_ref_in, route_ref), (bias_ref_in, bias_ref), (q_small_in, q_small), (q_large_in, q_large),
        (residual_in, residual), (gain_mix_in, gain_mix), (gain_route_in, gain_route), (gain_ref_in, gain_ref),
    )
    moves = [pltpu.make_async_copy(source, target, operand_sem.at[n]) for n, (source, target) in enumerate(moved)]
    for move in moves:
        move.start()
    greeted = greet(depth, plane, cores, me, core)
    for move in moves[:4]:
        move.wait()
    def turned(block):
        width = block.shape[1]
        eye = jnp.where(
            lax.broadcasted_iota(jnp.int32, (width, width), 0) == lax.broadcasted_iota(jnp.int32, (width, width), 1),
            1.0, 0.0).astype(jnp.bfloat16)
        return lax.dot_general(
            eye, block, (((1,), (1,)), ((), ())), preferred_element_type=jnp.float32).astype(jnp.bfloat16)

    table[me, extra_s:large_v, :] = turned(kv_small[...])
    table[me, large_k:gate_l, :] = turned(kv_large[:, :size_large])
    table[me, large_v:large_k, :] = turned(kv_large[:, size_large:])
    cums[me, :heads_small] = cum_small[...]
    cums[me, heads_small:heads] = cum_large[...]

    for move in moves[4:]:
        move.wait()
    for load in loads + expert_loads:
        load.start()
    lanes_s = lax.broadcasted_iota(jnp.int32, (tokens, extra_s), 1)
    lanes_l = lax.broadcasted_iota(jnp.int32, (tokens, extra_l), 1)
    for h in range(heads_small):
        picks = jnp.where((lanes_s % heads_small == h) & (lanes_s < 3 * heads_small), 1.0, 0.0)
        qs[h] = jnp.concatenate(
            [picks.astype(jnp.bfloat16), q_small[:, h * size_small:(h + 1) * size_small]], axis=1)
    for h in range(heads_large):
        picks = jnp.where((lanes_l % heads_large == h) & (lanes_l < 3 * heads_large), 1.0, 0.0)
        ql[h] = jnp.concatenate(
            [q_large[:, h * size_large:(h + 1) * size_large], picks.astype(jnp.bfloat16)], axis=1)
    row_of = lax.broadcasted_iota(jnp.int32, (keep, keep), 0)
    lane_of = lax.broadcasted_iota(jnp.int32, (keep, keep), 1)
    eye = row_of == lane_of
    before = row_of < lane_of
    ids = route_ref[...].astype(jnp.float32)
    first, second = ids[0:1], ids[1:2]
    groups = jnp.floor((first + 0.5) * (1.0 / lanes))
    groups_col = as_column(groups, eye)
    first_col = as_column(first, eye)
    second_col = as_column(second, eye)

    def total_rows(mask):
        return jnp.sum(jnp.where(mask, 1.0, 0.0), axis=0, keepdims=True)

    ranks = total_rows((groups_col == groups) & before)
    places_first = (first - groups * lanes) * capacity + total_rows((first_col == first) & before) + 1.0
    places_second = (
        (second - groups * lanes) * capacity
        + total_rows(first_col == second) + total_rows((second_col == second) & before) + 1.0
    )
    bias = bias_ref[...]
    facts = [as_column(fact, eye) for fact in (places_first, places_second, jax.nn.sigmoid(bias), jax.nn.sigmoid(-bias))]
    ranks_col = as_column(ranks, eye)
    slot_lanes = lax.broadcasted_iota(jnp.int32, (keep, width), 1).astype(jnp.float32)
    for group in range(depth):
        chosen = (slot_lanes == ranks_col) & (groups_col == group)
        rows = [jnp.sum(jnp.where(chosen, fact, 0.0), axis=0, keepdims=True) for fact in facts]
        out_meta[group] = jnp.concatenate(rows + [jnp.zeros((4, width), jnp.float32)], axis=0)
    routing[0:1] = groups
    routing[1:2] = ranks
    pl.semaphore_wait(pltpu.get_barrier_semaphore(), greeted)

    def place(behind, off_y, off_x):
        return (mine_z - behind) * plane + (mine_y + off_y) % rows_y * rows_x + (mine_x + off_x) % rows_x

    def copies(shard, target, sems):
        part = table.at[shard, pl.ds(extra_s + core * half, half)]
        return (
            pltpu.make_async_remote_copy(
                src_ref=part, dst_ref=part, send_sem=sems.at[0], recv_sem=recv_kv.at[shard],
                device_id=(target, core), device_id_type=MESH),
            pltpu.make_async_remote_copy(
                src_ref=cums.at[shard], dst_ref=cums.at[shard], send_sem=sems.at[1],
                recv_sem=recv_cum.at[shard], device_id=(target, core), device_id_type=MESH),
        )

    def start(shard, target, sems):
        for copy in copies(shard, target, sems):
            copy.start()

    def across(shard, which):
        part = table.at[shard, pl.ds(extra_s + which * half, half)]
        return pltpu.make_async_remote_copy(
            src_ref=part, dst_ref=part, send_sem=send_core.at[shard], recv_sem=recv_core.at[shard],
            device_id=(me, 1 - core), device_id_type=MESH)

    def arrived(shard):
        for copy in copies(shard, me, send_far.at[0]):
            copy.wait_recv()
        across(shard, core).start()

    near_y = rows_y - 1
    near_x = rows_x - 1
    near = near_y + near_x

    def both_ways(behind):
        shard = place(behind, 0, 0)
        for step in range(1, rows_x):
            yield shard, place(0, 0, step), near_y + step - 1
        for step in range(1, rows_y):
            yield shard, place(0, step, 0), step - 1

    def onward(behind, first_axis):
        if first_axis == "y":
            for step_a in range(1, rows_y):
                for step_b in range(1, rows_x):
                    yield place(behind, step_a, 0), place(0, 0, step_b), near + (step_a - 1) * near_x + step_b - 1
        else:
            for step_a in range(1, rows_x):
                for step_b in range(1, rows_y):
                    yield place(behind, 0, step_a), place(0, step_b, 0), near + (step_a - 1) * near_y + step_b - 1

    def column(behind):
        if not isinstance(behind, int):
            arrived(place(behind, 0, 0))
        for shard, target, slot in both_ways(behind):
            start(shard, target, send_near.at[behind, slot])

    def neighbours(behind):
        def along(first_axis):
            for shard, target, slot in onward(behind, first_axis):
                inner = (rows_x if first_axis == "y" else rows_y) - 1
                if (slot - near) % inner == 0:
                    arrived(shard)
                start(shard, target, send_near.at[behind, slot])
            if first_axis == "y":
                if near_x == 0:
                    for step in range(1, rows_y):
                        arrived(place(behind, step, 0))
                for step in range(1, rows_x):
                    arrived(place(behind, 0, step))
            else:
                if near_y == 0:
                    for step in range(1, rows_x):
                        arrived(place(behind, 0, step))
                for step in range(1, rows_y):
                    arrived(place(behind, step, 0))

        pl.when(core == 0)(functools.partial(along, "y"))
        pl.when(core == 1)(functools.partial(along, "x"))

    def corners(behind):
        for off_y in range(1, rows_y):
            for off_x in range(1, rows_x):
                arrived(place(behind, off_y, off_x))

    def far(step):
        return copies(me, (mine_z + step) * plane + me % plane, send_far.at[step])

    column(0)
    for step in range(1, depth):

        def send_up(step=step):
            for copy in far(step):
                copy.start()

        pl.when(mine_z + step < depth)(send_up)

    def attend(shard, own):
        gates = cums[shard]
        picked = bf16_pieces(gates[:heads_small] * (-math.sqrt(size_small)))
        if extra_s > 3 * heads_small:
            picked.append(jnp.zeros((extra_s - 3 * heads_small, tokens), jnp.float32))
        table[shard, :extra_s, :] = jnp.concatenate(picked, axis=0).astype(jnp.bfloat16)
        picked = bf16_pieces(gates[heads_small:heads] * (-math.sqrt(size_large)))
        if extra_l > 3 * heads_large:
            picked.append(jnp.zeros((extra_l - 3 * heads_large, tokens), jnp.float32))
        table[shard, gate_l:, :] = jnp.concatenate(picked, axis=0).astype(jnp.bfloat16)
        for h in range(heads):
            small = h < heads_small
            size = size_small if small else size_large
            scale = size ** (-0.5) * log2e
            query = qs[h] if small else ql[h - heads_small]
            keys = table[shard, :small_v, :] if small else table[shard, large_k:, :]
            values = table[shard, small_v:large_v, :] if small else table[shard, large_v:large_k, :]
            acc_ref, number = (acc_s, h) if small else (acc_l, h - heads_small)
            scores = jnp.dot(query, keys, preferred_element_type=jnp.float32)
            if own:
                key_pos = lax.broadcasted_iota(jnp.int32, (tokens, tokens), 1)
                query_pos = lax.broadcasted_iota(jnp.int32, (tokens, tokens), 0)
                scores = jnp.where(key_pos <= query_pos, scores, far_score)
            parts = [scores[:, j * 128:(j + 1) * 128] for j in range(tokens // 128)]
            newest = jnp.max(functools.reduce(jnp.maximum, parts), axis=-1, keepdims=True)
            if own:
                newest = jnp.broadcast_to(newest, (tokens, 128))
            else:
                before = top[h]
                newest = jnp.maximum(before, newest)
                factor = jnp.exp2((before - newest) * scale)
            scaled = newest * scale
            found = [jnp.exp2(part * scale - scaled) for part in parts]
            partial_sum = functools.reduce(jnp.add, found)
            product = lax.dot_general(
                jnp.concatenate(found, axis=1).astype(jnp.bfloat16), values,
                (((1,), (1,)), ((), ())), preferred_element_type=jnp.float32)
            top[h] = newest
            if own:
                total[h] = partial_sum
                acc_ref[number] = product
            else:
                total[h] = total[h] * factor + partial_sum
                acc_ref[number] = acc_ref[number] * factor[:, :size] + product

    attend(me, True)
    neighbours(0)
    order = [(0, 0)] + [(step, 0) for step in range(1, rows_y)] + [(0, step) for step in range(1, rows_x)]
    order += [(a, b) for a in range(1, rows_y) for b in range(1, rows_x)]

    def step_of(number, _):
        behind = number // plane
        turn = number % plane
        pl.when((turn == jnp.where(behind == 0, min(1, plane - 1), 0)) & (behind + 1 <= mine_z))(lambda: column(behind + 1))
        pl.when(turn == min(2, plane - 1))(lambda: corners(behind))
        pl.when((turn == plane - 1) & (behind + 1 <= mine_z))(lambda: neighbours(behind + 1))
        off_y = jnp.int32(0)
        off_x = jnp.int32(0)
        for index, (a, b) in enumerate(order):
            off_y = jnp.where(turn == index, a, off_y)
            off_x = jnp.where(turn == index, b, off_x)
        shard = place(behind, off_y, off_x)
        across(shard, 1 - core).wait_recv()
        pl.when(shard < me)(lambda: attend(shard, False))
        return 0

    lax.fori_loop(1, (mine_z + 1) * plane, step_of, 0)

    width_s = heads_small * size_small
    width_l = heads_large * size_large
    for mine in (False, True):
        rows = pl.ds(pl.multiple_of((core if mine else 1 - core) * keep, keep), keep)
        shown = []
        for h in range(heads):
            small = h < heads_small
            sums = jnp.sum(total[h, rows, :], axis=-1, keepdims=True)
            values = acc_s[h, rows, :] if small else acc_l[h - heads_small, rows, :]
            shown.append((values / sums).astype(jnp.bfloat16))
        joined_s = jnp.concatenate(shown[:heads_small], axis=1)
        joined_l = jnp.concatenate(shown[heads_small:], axis=1)
        if mine:
            whole[:, pl.ds(pl.multiple_of(core * width_s, 128), width_s)] = joined_s
            whole[:, pl.ds(pl.multiple_of(2 * width_s + core * width_l, 128), width_l)] = joined_l
        else:
            stage[:, :width_s] = joined_s
            stage[:, width_s:] = joined_l

    def swap(which):
        return (
            pltpu.make_async_remote_copy(
                src_ref=stage.at[:, pl.ds(0, width_s)],
                dst_ref=whole.at[:, pl.ds(pl.multiple_of(which * width_s, 128), width_s)],
                send_sem=swap_send.at[0], recv_sem=swap_recv.at[0],
                device_id=(me, 1 - core), device_id_type=MESH),
            pltpu.make_async_remote_copy(
                src_ref=stage.at[:, pl.ds(width_s, width_l)],
                dst_ref=whole.at[:, pl.ds(pl.multiple_of(2 * width_s + which * width_l, 128), width_l)],
                send_sem=swap_send.at[1], recv_sem=swap_recv.at[1],
                device_id=(me, 1 - core), device_id_type=MESH),
        )

    for copy in swap(core):
        copy.start()
    for load in loads:
        load.wait()
    span_w = 512

    def half_product(which, span):
        cols_s = pl.ds(pl.multiple_of(which * width_s, 128), width_s)
        cols_l = pl.ds(pl.multiple_of(2 * width_s + which * width_l, 128), width_l)
        return jnp.dot(whole[:, cols_s], weights[cols_s, span], preferred_element_type=jnp.float32) + jnp.dot(
            whole[:, cols_l], weights[cols_l, span], preferred_element_type=jnp.float32)

    def project_own(number, _):
        span = pl.ds(pl.multiple_of(number * span_w, span_w), span_w)
        mixer[:, span] = half_product(core, span)
        return 0

    lax.fori_loop(0, columns // span_w, project_own, 0)
    for copy in swap(1 - core):
        copy.wait_recv()

    def project(number, squares):
        span = pl.ds(pl.multiple_of(number * span_w, span_w), span_w)
        part = mixer[:, span] + half_product(1 - core, span)
        mixer[:, span] = part
        square = part * part
        return squares + functools.reduce(jnp.add, [square[:, j * 128:(j + 1) * 128] for j in range(span_w // 128)])

    squares = lax.fori_loop(0, columns // span_w, project, jnp.zeros((keep, 128), jnp.float32))
    mean = jnp.sum(squares, axis=-1, keepdims=True) * (1.0 / columns)
    mixed = (
        residual[...].astype(jnp.float32) + mixer[...] * lax.rsqrt(mean + norm_eps) * gain_mix[...]
    ).astype(jnp.bfloat16)
    mixed_ref[...] = mixed
    routed = rms_scale(mixed.astype(jnp.float32), gain_route[...])


    routed = routed.astype(jnp.bfloat16)
    slot_rows = lax.broadcasted_iota(jnp.int32, (slots, keep), 0).astype(jnp.float32)
    for group in range(depth):
        table_of = jnp.where((slot_rows == routing[1:2]) & (routing[0:1] == group), 1.0, 0.0).astype(jnp.bfloat16)
        out_rows[group] = jnp.dot(table_of, routed, preferred_element_type=jnp.float32).astype(jnp.bfloat16)
    in_rows[mine_z] = out_rows[mine_z]
    metas[mine_z] = out_meta[mine_z]

    parts = recv_rows.shape[1]
    plans, sends = plan_of(depth, parts)
    extent = columns // parts

    def columns_of(part):
        return pl.ds(part * extent, extent)

    def along_rows(other, slot, part):
        return pltpu.make_async_remote_copy(
            src_ref=out_rows.at[other, :, columns_of(part)], dst_ref=in_rows.at[slot, :, columns_of(part)],
            send_sem=send_rows.at[other, part], recv_sem=recv_rows.at[slot, part],
            device_id=(other * plane + me % plane, core), device_id_type=MESH)

    def along_meta(other, slot):
        return pltpu.make_async_remote_copy(
            src_ref=out_meta.at[other], dst_ref=metas.at[slot], send_sem=send_meta.at[other],
            recv_sem=recv_meta.at[slot], device_id=(other * plane + me % plane, core), device_id_type=MESH)

    def outward(source, other, slot, part):
        return pltpu.make_async_remote_copy(
            src_ref=spread.at[source, other, :, columns_of(part)],
            dst_ref=received.at[source, slot, :, columns_of(part)],
            send_sem=send_block.at[source, other, part], recv_sem=recv_block.at[source, slot, part],
            device_id=(mine_z * plane + other // cores, other % cores), device_id_type=MESH)

    def inward(source, other, slot, part):
        return pltpu.make_async_remote_copy(
            src_ref=outs.at[source, other, :, columns_of(part)],
            dst_ref=back.at[source, slot, :, columns_of(part)],
            send_sem=send_back.at[source, other, part], recv_sem=recv_back.at[source, slot, part],
            device_id=(mine_z * plane + other // cores, other % cores), device_id_type=MESH)

    def homeward(other, slot, part):
        return pltpu.make_async_remote_copy(
            src_ref=combined.at[other, :, columns_of(part)], dst_ref=final.at[slot, :, columns_of(part)],
            send_sem=send_home.at[other, part], recv_sem=recv_home.at[slot, part],
            device_id=(other * plane + me % plane, core), device_id_type=MESH)

    steps = distances(depth)
    for index in range(depth - 1):
        other = jnp.int32(0)
        for z in range(depth):
            other = jnp.where(mine_z == z, sends[z][index], other)
        along_meta(other, mine_z).start()
        for part in range(parts):
            along_rows(other, mine_z, part).start()

    def flat(ref, source, span):
        if capacity % 16:
            return jnp.concatenate(
                [ref[source, lane, :, span].astype(jnp.float32) for lane in range(lanes)], axis=0).astype(jnp.bfloat16)
        found = ref[source, :, :, span]
        return found.reshape(count, found.shape[2])

    def split(ref, source, values, span):
        for lane in range(lanes):
            ref[source, lane, :, span] = values[lane * capacity:(lane + 1) * capacity].astype(jnp.bfloat16)

    def expand(source, part):
        span = columns_of(part)

        def landed():
            if part == 0:
                along_meta(source, source).wait_recv()
            along_rows(source, source, part).wait_recv()

        pl.when(source != mine_z)(landed)
        wanted = lax.broadcasted_iota(jnp.int32, (count, slots), 0).astype(jnp.float32) + 1.0
        spots = jnp.where(
            (wanted == metas[source, 0:1, :slots]) | (wanted == metas[source, 1:2, :slots]), 1.0, 0.0
        ).astype(jnp.bfloat16)
        split(spread, source, jnp.dot(spots, in_rows[source, :, span], preferred_element_type=jnp.float32), span)
        received[source, here, :, span] = spread[source, here, :, span]
        for move in range(1, lanes):
            outward(source, (here + move) % lanes, here, part).start()

    tile = 256

    def compute(source):
        for part in range(parts):
            for move in range(1, lanes):
                outward(source, (here + move) % lanes, (here + move) % lanes, part).wait_recv()
        rows = flat(received, source, slice(None))

        def enter(number, _):
            span = pl.ds(pl.multiple_of(number * tile, tile), tile)
            gate = jnp.dot(rows, gate_w[:, span], preferred_element_type=jnp.float32)
            up = jnp.dot(rows, up_w[:, span], preferred_element_type=jnp.float32)
            hidden[:, span] = (jax.nn.silu(gate) * up).astype(jnp.bfloat16)
            return 0

        lax.fori_loop(0, gate_w.shape[1] // tile, enter, 0)
        for part in range(parts):

            def leave(number, _):
                span = pl.ds(pl.multiple_of(part * extent + number * 2 * tile, 2 * tile), 2 * tile)
                split(outs, source, jnp.dot(hidden[...], down_w[:, span], preferred_element_type=jnp.float32), span)
                return 0

            lax.fori_loop(0, extent // (2 * tile), leave, 0)
            span = columns_of(part)
            back[source, here, :, span] = outs[source, here, :, span]
            for move in range(1, lanes):
                inward(source, (here + move) % lanes, here, part).start()

    def combine(source, part):
        span = columns_of(part)
        for move in range(1, lanes):
            inward(source, (here + move) % lanes, (here + move) % lanes, part).wait_recv()
        wanted = lax.broadcasted_iota(jnp.int32, (count, width), 0).astype(jnp.float32) + 1.0
        shares = jnp.where(wanted == metas[source, 0:1, :], metas[source, 2:3, :], 0.0)
        shares = shares + jnp.where(wanted == metas[source, 1:2, :], metas[source, 3:4, :], 0.0)
        shares = shares.T[:slots]
        high = shares.astype(jnp.bfloat16)
        low = (shares - high.astype(jnp.float32)).astype(jnp.bfloat16)
        picked = flat(back, source, span)
        mixed = jnp.dot(high, picked, preferred_element_type=jnp.float32) + jnp.dot(
            low, picked, preferred_element_type=jnp.float32)

        def away():
            combined[source, :, span] = mixed.astype(jnp.bfloat16)
            homeward(source, mine_z, part).start()

        def stay():
            final[source, :, span] = mixed.astype(jnp.bfloat16)

        pl.when(source != mine_z)(away)
        pl.when(source == mine_z)(stay)


    def turn_of(turn, _):
        found = jnp.int32(0)
        for z in range(depth):
            for index, (kind, source) in enumerate(plans[z]):
                found = jnp.where((mine_z == z) & (turn == index), kind * depth + source, found)
        kind = found // depth
        source = found % depth
        pl.when(kind == 0)(lambda: compute(source))
        for part in range(parts):
            pl.when(kind == 1 + part)(functools.partial(expand, source, part))
            pl.when(kind == 1 + parts + part)(functools.partial(combine, source, part))
        return 0

    for load in expert_loads:
        load.wait()
    lax.fori_loop(0, (1 + 2 * parts) * depth, turn_of, 0)
    for step in steps[1:]:
        other = mine_z + step

        def settle(other=other):
            along_meta(other, mine_z).wait_send()
            for part in range(parts):
                homeward(other, other, part).wait_recv()
                homeward(other, mine_z, part).wait_send()
                along_rows(other, mine_z, part).wait_send()

        pl.when((other >= 0) & (other < depth))(settle)
    for source in range(depth):
        for move in range(1, lanes):
            for part in range(parts):
                outward(source, (here + move) % lanes, here, part).wait_send()
                inward(source, (here + move) % lanes, here, part).wait_send()
    for step in range(1, depth):

        def sent_up(step=step):
            for copy in far(step):
                copy.wait_send()

        pl.when(mine_z + step < depth)(sent_up)

    def sent(behind, _):
        for shard, target, slot in both_ways(behind):
            for copy in copies(shard, target, send_near.at[behind, slot]):
                copy.wait_send()
        for slot in range(near, near + near_y * near_x):
            for copy in copies(me, me, send_near.at[behind, slot]):
                copy.wait_send()

        def crossed(number, _):
            shard = (mine_z - behind) * plane + number
            pl.when(shard != me)(lambda: across(shard, core).wait_send())
            return 0

        lax.fori_loop(0, plane, crossed, 0)
        return 0

    lax.fori_loop(0, mine_z + 1, sent, 0)
    for copy in swap(core):
        copy.wait_send()
    eye = lax.broadcasted_iota(jnp.int32, (keep, keep), 0) == lax.broadcasted_iota(jnp.int32, (keep, keep), 1)
    slot_all = lax.broadcasted_iota(jnp.int32, (keep, depth * slots), 1).astype(jnp.float32)
    places = jnp.where(slot_all == as_column(routing[0:1] * slots + routing[1:2], eye), 1.0, 0.0).astype(jnp.bfloat16)
    blended = jnp.dot(places, final[...].reshape(depth * slots, columns), preferred_element_type=jnp.float32)
    result_ref[...] = (
        mixed_ref[...].astype(jnp.float32) + rms_scale(blended, gain_ref[...])
    ).astype(jnp.bfloat16)


def layer(dims, queries_small, queries_large, kv_small, kv_large, cum_small, cum_large, residual, gain_mix, gain_route, route, bias, gain_blend, out_small, out_large, w_gate, w_up, w_down):
    shards = lax.axis_size("sp")
    depth, rows_y, rows_x = dims
    tokens = queries_small.shape[0]
    heads_small = cum_small.shape[0]
    heads_large = cum_large.shape[0]
    size_small = kv_small.shape[1] // 2
    size_large = kv_large.shape[1] // 2
    heads = heads_small + heads_large
    extra_s = round_up(3 * heads_small, 32)
    extra_l = round_up(3 * heads_large, 16)
    table_rows = extra_s + 2 * size_small + 2 * size_large + extra_l
    near = rows_y + rows_x - 2 + (rows_y - 1) * (rows_x - 1)
    keep, columns = residual.shape
    lanes = lax.axis_size(("sp", "tp")) // depth
    capacity = 4 * keep // (depth * lanes)
    slots = capacity * lanes // 2
    width = round_up(slots, 128)
    parts = 2
    inner = w_gate.shape[2]
    joined = out_small.shape[0] + out_large.shape[0]
    dma = pltpu.SemaphoreType.DMA
    vmem = pl.BlockSpec(memory_space=pltpu.VMEM)
    hbm = pl.BlockSpec(memory_space=pltpu.HBM)
    bf16, f32 = jnp.bfloat16, jnp.float32
    rows = pltpu.VMEM((depth, slots, columns), bf16)
    blocks = pltpu.VMEM((depth, lanes, capacity, columns), bf16)
    meta = pltpu.VMEM((depth, 8, width), f32)
    scratch = [
        pltpu.VMEM(queries_small.shape, bf16),
        pltpu.VMEM(queries_large.shape, bf16),
        pltpu.VMEM(kv_small.shape, bf16),
        pltpu.VMEM(kv_large.shape, bf16),
        pltpu.VMEM(cum_small.shape, f32),
        pltpu.VMEM(cum_large.shape, f32),
        pltpu.VMEM(residual.shape, bf16),
        pltpu.VMEM((1, columns), f32),
        pltpu.VMEM((1, columns), f32),
        pltpu.VMEM(route.shape, route.dtype),
        pltpu.VMEM((1, keep), f32),
        pltpu.VMEM((1, columns), f32),
        pltpu.VMEM((shards, table_rows, tokens), bf16),
        pltpu.VMEM((shards, heads, tokens), f32),
        pltpu.VMEM((heads_small, tokens, extra_s + size_small), bf16),
        pltpu.VMEM((heads_large, tokens, size_large + extra_l), bf16),
        pltpu.VMEM((heads, tokens, 128), f32),
        pltpu.VMEM((heads, tokens, 128), f32),
        pltpu.VMEM((heads_small, tokens, size_small), f32),
        pltpu.VMEM((heads_large, tokens, size_large), f32),
        pltpu.VMEM((keep, heads_small * size_small + heads_large * size_large), bf16),
        pltpu.VMEM((keep, joined), bf16),
        pltpu.VMEM((joined, columns), bf16),
        pltpu.VMEM((keep, columns), f32),
        pltpu.VMEM((keep, columns), bf16),
        pltpu.VMEM((8, keep), f32),
        rows, rows, meta, meta, blocks, blocks, blocks, blocks, rows, rows,
        pltpu.VMEM((lanes * capacity, inner), bf16),
        pltpu.VMEM((columns, inner), bf16),
        pltpu.VMEM((columns, inner), bf16),
        pltpu.VMEM((inner, columns), bf16),
        dma((depth, 2)), dma((depth, near, 2)), dma((shards,)), dma((shards,)), dma((shards,)), dma((shards,)),
        dma((2,)), dma((2,)), dma((5,)), dma((12,)),
        dma((depth, parts)), dma((depth, parts)), dma((depth,)), dma((depth,)),
        dma((depth, lanes, parts)), dma((depth, lanes, parts)), dma((depth, lanes, parts)), dma((depth, lanes, parts)),
        dma((depth, parts)), dma((depth, parts)),
    ]
    return pl.pallas_call(
        functools.partial(layer_kernel, dims, (heads_small, heads_large, size_small, size_large)),
        out_shape=jax.ShapeDtypeStruct(residual.shape, bf16),
        in_specs=[hbm] * 17,
        out_specs=vmem,
        scratch_shapes=scratch,
        compiler_params=pltpu.CompilerParams(
            collective_id=0, has_side_effects=True, vmem_limit_bytes=66 * 1000 * 1000),
        name="layer",
    )(queries_small, queries_large, kv_small, kv_large, cum_small, cum_large, residual,
      gain_mix.reshape(1, columns), gain_route.reshape(1, columns), route, bias.reshape(1, keep),
      gain_blend.reshape(1, columns), out_small, out_large, w_gate, w_up, w_down)


def on_device(
    dims,
    queries_small,
    queries_large,
    kv_small,
    kv_large,
    cum_small,
    cum_large,
    residual,
    out_small,
    out_large,
    gain_mix,
    gain_route,
    gain_blend,
    w_gate,
    w_up,
    w_down,
    route,
    route_bias,
):
    return layer(
        dims, queries_small, queries_large, kv_small, kv_large, cum_small, cum_large, residual,
        gain_mix, gain_route, route, route_bias, gain_blend, out_small, out_large, w_gate, w_up, w_down,
    )


def solution(mesh):
    in_specs = (
        P("sp", "tp"),
        P("sp", "tp"),
        P("sp", None),
        P("sp", None),
        P("tp", "sp"),
        P("tp", "sp"),
        P(("sp", "tp"), None),
        P(),
        P(),
        P(),
        P(),
        P(),
        P(("sp", "tp"), None, None),
        P(("sp", "tp"), None, None),
        P(("sp", "tp"), None, None),
        P(None, ("sp", "tp")),
        P(("sp", "tp")),
    )
    out_specs = P(("sp", "tp"), None)
    return jax.shard_map(
        functools.partial(on_device, mesh_shape(mesh)), mesh=mesh, in_specs=in_specs, out_specs=out_specs, check_vma=False
    )
```

```python
import functools
import math

import jax
import jax.numpy as jnp
from jax import lax
from jax.experimental import pallas as pl
from jax.experimental.pallas import tpu as pltpu
from jax.sharding import PartitionSpec as P

norm_eps = 1e-06
far_score = -1e30
log2e = math.log2(math.e)
MESH = pl.DeviceIdType.MESH


def rms_scale(values, gain_row):
    return (
        values * lax.rsqrt(jnp.mean(values * values, axis=-1, keepdims=True) + norm_eps) * gain_row
    )


def mesh_shape(mesh):
    coords = [tuple(device.coords) for device in mesh.devices.reshape(-1)]
    return tuple(1 + max(c[axis] for c in coords) - min(c[axis] for c in coords) for axis in (2, 1, 0))


def bf16_pieces(values):
    high = values.astype(jnp.bfloat16)
    rest = values - high.astype(jnp.float32)
    middle = rest.astype(jnp.bfloat16)
    low = (rest - middle.astype(jnp.float32)).astype(jnp.bfloat16)
    return [high.astype(jnp.float32), middle.astype(jnp.float32), low.astype(jnp.float32)]


def round_up(value, unit):
    return -(-value // unit) * unit


def greet(depth, plane, cores, me, core):
    barrier = pltpu.get_barrier_semaphore()
    lanes = plane * cores
    here = me % plane * cores + core
    for step in range(1, depth):
        target = (me // plane + step) % depth * plane + me % plane
        pl.semaphore_signal(barrier, inc=1, device_id=(target, core), device_id_type=MESH)
    for step in range(1, lanes):
        other = (here + step) % lanes
        target = me // plane * plane + other // cores
        pl.semaphore_signal(barrier, inc=1, device_id=(target, other % cores), device_id_type=MESH)
    return depth - 1 + lanes - 1


def distances(depth):
    found = [0]
    for step in range(1, depth):
        found += [step, -step]
    return found


def as_column(row, eye):
    return jnp.sum(jnp.where(eye, row, 0.0), axis=1, keepdims=True)


def plan_of(depth, parts):
    if depth == 4 and parts == 2:
        coded = (
            (5, 4, 9, 6, 10, 1, 2, 14, 13, 7, 11, 18, 8, 17, 3, 0, 15, 19, 12, 16),
            (5, 4, 8, 0, 9, 7, 11, 6, 10, 3, 1, 15, 12, 19, 2, 13, 16, 14, 17, 18),
            (6, 5, 9, 4, 8, 10, 0, 1, 12, 13, 16, 7, 11, 3, 17, 2, 15, 19, 14, 18),
            (4, 8, 6, 5, 9, 7, 10, 1, 2, 11, 13, 14, 17, 0, 18, 3, 12, 16, 15, 19),
        )
        sends = ((3, 1, 2), (2, 0, 3), (0, 3, 1), (2, 1, 0))
        return [[(code // depth, code % depth) for code in plan] for plan in coded], sends
    plans, sends = [], []
    for z in range(depth):
        order = [z + step for step in distances(depth) if 0 <= z + step < depth]
        plan = []
        for turn in range(depth + 2):
            if turn < depth:
                plan += [(1 + part, order[turn]) for part in range(parts)]
            if 1 <= turn <= depth:
                plan += [(0, order[turn - 1])]
            if turn >= 2:
                plan += [(1 + parts + part, order[turn - 2]) for part in range(parts)]
        plans.append(plan)
        sends.append(order[1:])
    return plans, sends


def layer_kernel(
    dims, head_shape,
    q_small_in, q_large_in, kv_small_in, kv_large_in, cum_small_in, cum_large_in, residual_in, gain_mix_in, gain_route_in, route_ref_in, bias_ref_in, gain_ref_in,
    out_small, out_large, w_gate, w_up, w_down,
    result_ref,
    q_small, q_large, kv_small, kv_large, cum_small, cum_large, residual, gain_mix, gain_route, route_ref, bias_ref, gain_ref,
    table, cums, qs, ql, top, total, acc_s, acc_l, stage, whole, weights, mixer, mixed_ref, routing,
    out_rows, in_rows, out_meta, metas, spread, received, outs, back, combined, final, hidden, gate_w, up_w, down_w,
    send_far, send_near, send_core, recv_kv, recv_cum, recv_core, swap_send, swap_recv, load_sem,
    operand_sem, send_rows, recv_rows, send_meta, recv_meta, send_block, recv_block, send_back, recv_back, send_home, recv_home,
):
    heads_small, heads_large, size_small, size_large = head_shape
    depth, rows_y, rows_x = dims
    plane = rows_y * rows_x
    me = lax.axis_index("sp")
    core = lax.axis_index("tp")
    mine_z = me // plane
    mine_y = me % plane // rows_x
    mine_x = me % rows_x
    tokens = q_small.shape[0]
    _, lanes, capacity, columns = spread.shape
    cores = lanes // (dims[1] * dims[2])
    slots = in_rows.shape[1]
    width = metas.shape[2]
    keep = residual.shape[0]
    count = lanes * capacity
    here = me % plane * cores + core
    heads = heads_small + heads_large
    extra_s = round_up(3 * heads_small, 32)
    extra_l = round_up(3 * heads_large, 16)
    wire = 2 * size_small + 2 * size_large
    half = wire // 2
    small_v = extra_s + size_small
    large_v = small_v + size_small
    large_k = large_v + size_large
    gate_l = extra_s + wire

    loads = (
        pltpu.make_async_copy(out_small, weights.at[pl.ds(0, out_small.shape[0])], load_sem.at[0]),
        pltpu.make_async_copy(
            out_large, weights.at[pl.ds(out_small.shape[0], out_large.shape[0])], load_sem.at[1]),
    )
    expert_loads = (
        pltpu.make_async_copy(w_gate.at[0], gate_w, load_sem.at[2]),
        pltpu.make_async_copy(w_up.at[0], up_w, load_sem.at[3]),
        pltpu.make_async_copy(w_down.at[0], down_w, load_sem.at[4]),
    )
    moved = (
        (kv_small_in, kv_small), (kv_large_in, kv_large), (cum_small_in, cum_small), (cum_large_in, cum_large),
        (route_ref_in, route_ref), (bias_ref_in, bias_ref), (q_small_in, q_small), (q_large_in, q_large),
        (residual_in, residual), (gain_mix_in, gain_mix), (gain_route_in, gain_route), (gain_ref_in, gain_ref),
    )
    moves = [pltpu.make_async_copy(source, target, operand_sem.at[n]) for n, (source, target) in enumerate(moved)]
    for move in moves:
        move.start()
    greeted = greet(depth, plane, cores, me, core)
    for move in moves[:4]:
        move.wait()
    def turned(block):
        width = block.shape[1]
        eye = jnp.where(
            lax.broadcasted_iota(jnp.int32, (width, width), 0) == lax.broadcasted_iota(jnp.int32, (width, width), 1),
            1.0, 0.0).astype(jnp.bfloat16)
        return lax.dot_general(
            eye, block, (((1,), (1,)), ((), ())), preferred_element_type=jnp.float32).astype(jnp.bfloat16)

    table[me, extra_s:large_v, :] = turned(kv_small[...])
    table[me, large_k:gate_l, :] = turned(kv_large[:, :size_large])
    table[me, large_v:large_k, :] = turned(kv_large[:, size_large:])
    cums[me, :heads_small] = cum_small[...]
    cums[me, heads_small:heads] = cum_large[...]

    for move in moves[4:]:
        move.wait()
    for load in loads + expert_loads:
        load.start()
    lanes_s = lax.broadcasted_iota(jnp.int32, (tokens, extra_s), 1)
    lanes_l = lax.broadcasted_iota(jnp.int32, (tokens, extra_l), 1)
    for h in range(heads_small):
        picks = jnp.where((lanes_s % heads_small == h) & (lanes_s < 3 * heads_small), 1.0, 0.0)
        qs[h] = jnp.concatenate(
            [picks.astype(jnp.bfloat16), q_small[:, h * size_small:(h + 1) * size_small]], axis=1)
    for h in range(heads_large):
        picks = jnp.where((lanes_l % heads_large == h) & (lanes_l < 3 * heads_large), 1.0, 0.0)
        ql[h] = jnp.concatenate(
            [q_large[:, h * size_large:(h + 1) * size_large], picks.astype(jnp.bfloat16)], axis=1)
    row_of = lax.broadcasted_iota(jnp.int32, (keep, keep), 0)
    lane_of = lax.broadcasted_iota(jnp.int32, (keep, keep), 1)
    eye = row_of == lane_of
    before = row_of < lane_of
    ids = route_ref[...].astype(jnp.float32)
    first, second = ids[0:1], ids[1:2]
    groups = jnp.floor((first + 0.5) * (1.0 / lanes))
    groups_col = as_column(groups, eye)
    first_col = as_column(first, eye)
    second_col = as_column(second, eye)

    def total_rows(mask):
        return jnp.sum(jnp.where(mask, 1.0, 0.0), axis=0, keepdims=True)

    ranks = total_rows((groups_col == groups) & before)
    places_first = (first - groups * lanes) * capacity + total_rows((first_col == first) & before) + 1.0
    places_second = (
        (second - groups * lanes) * capacity
        + total_rows(first_col == second) + total_rows((second_col == second) & before) + 1.0
    )
    bias = bias_ref[...]
    facts = [as_column(fact, eye) for fact in (places_first, places_second, jax.nn.sigmoid(bias), jax.nn.sigmoid(-bias))]
    ranks_col = as_column(ranks, eye)
    slot_lanes = lax.broadcasted_iota(jnp.int32, (keep, width), 1).astype(jnp.float32)
    for group in range(depth):
        chosen = (slot_lanes == ranks_col) & (groups_col == group)
        rows = [jnp.sum(jnp.where(chosen, fact, 0.0), axis=0, keepdims=True) for fact in facts]
        out_meta[group] = jnp.concatenate(rows + [jnp.zeros((4, width), jnp.float32)], axis=0)
    routing[0:1] = groups
    routing[1:2] = ranks
    pl.semaphore_wait(pltpu.get_barrier_semaphore(), greeted)

    def place(behind, off_y, off_x):
        return (mine_z - behind) * plane + (mine_y + off_y) % rows_y * rows_x + (mine_x + off_x) % rows_x

    def copies(shard, target, sems):
        part = table.at[shard, pl.ds(extra_s + core * half, half)]
        return (
            pltpu.make_async_remote_copy(
                src_ref=part, dst_ref=part, send_sem=sems.at[0], recv_sem=recv_kv.at[shard],
                device_id=(target, core), device_id_type=MESH),
            pltpu.make_async_remote_copy(
                src_ref=cums.at[shard], dst_ref=cums.at[shard], send_sem=sems.at[1],
                recv_sem=recv_cum.at[shard], device_id=(target, core), device_id_type=MESH),
        )

    def start(shard, target, sems):
        for copy in copies(shard, target, sems):
            copy.start()

    def across(shard, which):
        part = table.at[shard, pl.ds(extra_s + which * half, half)]
        return pltpu.make_async_remote_copy(
            src_ref=part, dst_ref=part, send_sem=send_core.at[shard], recv_sem=recv_core.at[shard],
            device_id=(me, 1 - core), device_id_type=MESH)

    def arrived(shard):
        for copy in copies(shard, me, send_far.at[0]):
            copy.wait_recv()
        across(shard, core).start()

    near_y = rows_y - 1
    near_x = rows_x - 1
    near = near_y + near_x

    def both_ways(behind):
        shard = place(behind, 0, 0)
        for step in range(1, rows_x):
            yield shard, place(0, 0, step), near_y + step - 1
        for step in range(1, rows_y):
            yield shard, place(0, step, 0), step - 1

    def onward(behind, first_axis):
        if first_axis == "y":
            for step_a in range(1, rows_y):
                for step_b in range(1, rows_x):
                    yield place(behind, step_a, 0), place(0, 0, step_b), near + (step_a - 1) * near_x + step_b - 1
        else:
            for step_a in range(1, rows_x):
                for step_b in range(1, rows_y):
                    yield place(behind, 0, step_a), place(0, step_b, 0), near + (step_a - 1) * near_y + step_b - 1

    def column(behind):
        if not isinstance(behind, int):
            arrived(place(behind, 0, 0))
        for shard, target, slot in both_ways(behind):
            start(shard, target, send_near.at[behind, slot])

    def neighbours(behind):
        def along(first_axis):
            for shard, target, slot in onward(behind, first_axis):
                inner = (rows_x if first_axis == "y" else rows_y) - 1
                if (slot - near) % inner == 0:
                    arrived(shard)
                start(shard, target, send_near.at[behind, slot])
            if first_axis == "y":
                if near_x == 0:
                    for step in range(1, rows_y):
                        arrived(place(behind, step, 0))
                for step in range(1, rows_x):
                    arrived(place(behind, 0, step))
            else:
                if near_y == 0:
                    for step in range(1, rows_x):
                        arrived(place(behind, 0, step))
                for step in range(1, rows_y):
                    arrived(place(behind, step, 0))

        pl.when(core == 0)(functools.partial(along, "y"))
        pl.when(core == 1)(functools.partial(along, "x"))

    def corners(behind):
        for off_y in range(1, rows_y):
            for off_x in range(1, rows_x):
                arrived(place(behind, off_y, off_x))

    def far(step):
        return copies(me, (mine_z + step) * plane + me % plane, send_far.at[step])

    column(0)
    for step in range(1, depth):

        def send_up(step=step):
            for copy in far(step):
                copy.start()

        pl.when(mine_z + step < depth)(send_up)

    def attend(shard, own):
        gates = cums[shard]
        picked = bf16_pieces(gates[:heads_small] * (-math.sqrt(size_small)))
        if extra_s > 3 * heads_small:
            picked.append(jnp.zeros((extra_s - 3 * heads_small, tokens), jnp.float32))
        table[shard, :extra_s, :] = jnp.concatenate(picked, axis=0).astype(jnp.bfloat16)
        picked = bf16_pieces(gates[heads_small:heads] * (-math.sqrt(size_large)))
        if extra_l > 3 * heads_large:
            picked.append(jnp.zeros((extra_l - 3 * heads_large, tokens), jnp.float32))
        table[shard, gate_l:, :] = jnp.concatenate(picked, axis=0).astype(jnp.bfloat16)
        for h in range(heads):
            small = h < heads_small
            size = size_small if small else size_large
            scale = size ** (-0.5) * log2e
            query = qs[h] if small else ql[h - heads_small]
            keys = table[shard, :small_v, :] if small else table[shard, large_k:, :]
            values = table[shard, small_v:large_v, :] if small else table[shard, large_v:large_k, :]
            acc_ref, number = (acc_s, h) if small else (acc_l, h - heads_small)
            scores = jnp.dot(query, keys, preferred_element_type=jnp.float32)
            if own:
                key_pos = lax.broadcasted_iota(jnp.int32, (tokens, tokens), 1)
                query_pos = lax.broadcasted_iota(jnp.int32, (tokens, tokens), 0)
                scores = jnp.where(key_pos <= query_pos, scores, far_score)
            parts = [scores[:, j * 128:(j + 1) * 128] for j in range(tokens // 128)]
            newest = jnp.max(functools.reduce(jnp.maximum, parts), axis=-1, keepdims=True)
            if own:
                newest = jnp.broadcast_to(newest, (tokens, 128))
            else:
                before = top[h]
                newest = jnp.maximum(before, newest)
                factor = jnp.exp2((before - newest) * scale)
            scaled = newest * scale
            found = [jnp.exp2(part * scale - scaled) for part in parts]
            partial_sum = functools.reduce(jnp.add, found)
            product = lax.dot_general(
                jnp.concatenate(found, axis=1).astype(jnp.bfloat16), values,
                (((1,), (1,)), ((), ())), preferred_element_type=jnp.float32)
            top[h] = newest
            if own:
                total[h] = partial_sum
                acc_ref[number] = product
            else:
                total[h] = total[h] * factor + partial_sum
                acc_ref[number] = acc_ref[number] * factor[:, :size] + product

    attend(me, True)
    neighbours(0)
    order = [(0, 0)] + [(step, 0) for step in range(1, rows_y)] + [(0, step) for step in range(1, rows_x)]
    order += [(a, b) for a in range(1, rows_y) for b in range(1, rows_x)]

    def step_of(number, _):
        behind = number // plane
        turn = number % plane
        pl.when((turn == jnp.where(behind == 0, min(1, plane - 1), 0)) & (behind + 1 <= mine_z))(lambda: column(behind + 1))
        pl.when(turn == min(2, plane - 1))(lambda: corners(behind))
        pl.when((turn == plane - 1) & (behind + 1 <= mine_z))(lambda: neighbours(behind + 1))
        off_y = jnp.int32(0)
        off_x = jnp.int32(0)
        for index, (a, b) in enumerate(order):
            off_y = jnp.where(turn == index, a, off_y)
            off_x = jnp.where(turn == index, b, off_x)
        shard = place(behind, off_y, off_x)
        across(shard, 1 - core).wait_recv()
        pl.when(shard < me)(lambda: attend(shard, False))
        return 0

    lax.fori_loop(1, (mine_z + 1) * plane, step_of, 0)

    width_s = heads_small * size_small
    width_l = heads_large * size_large
    for mine in (False, True):
        rows = pl.ds(pl.multiple_of((core if mine else 1 - core) * keep, keep), keep)
        shown = []
        for h in range(heads):
            small = h < heads_small
            sums = jnp.sum(total[h, rows, :], axis=-1, keepdims=True)
            values = acc_s[h, rows, :] if small else acc_l[h - heads_small, rows, :]
            shown.append((values / sums).astype(jnp.bfloat16))
        joined_s = jnp.concatenate(shown[:heads_small], axis=1)
        joined_l = jnp.concatenate(shown[heads_small:], axis=1)
        if mine:
            whole[:, pl.ds(pl.multiple_of(core * width_s, 128), width_s)] = joined_s
            whole[:, pl.ds(pl.multiple_of(2 * width_s + core * width_l, 128), width_l)] = joined_l
        else:
            stage[:, :width_s] = joined_s
            stage[:, width_s:] = joined_l

    def swap(which):
        return (
            pltpu.make_async_remote_copy(
                src_ref=stage.at[:, pl.ds(0, width_s)],
                dst_ref=whole.at[:, pl.ds(pl.multiple_of(which * width_s, 128), width_s)],
                send_sem=swap_send.at[0], recv_sem=swap_recv.at[0],
                device_id=(me, 1 - core), device_id_type=MESH),
            pltpu.make_async_remote_copy(
                src_ref=stage.at[:, pl.ds(width_s, width_l)],
                dst_ref=whole.at[:, pl.ds(pl.multiple_of(2 * width_s + which * width_l, 128), width_l)],
                send_sem=swap_send.at[1], recv_sem=swap_recv.at[1],
                device_id=(me, 1 - core), device_id_type=MESH),
        )

    for copy in swap(core):
        copy.start()
    for load in loads:
        load.wait()
    span_w = 512

    def half_product(which, span):
        cols_s = pl.ds(pl.multiple_of(which * width_s, 128), width_s)
        cols_l = pl.ds(pl.multiple_of(2 * width_s + which * width_l, 128), width_l)
        return jnp.dot(whole[:, cols_s], weights[cols_s, span], preferred_element_type=jnp.float32) + jnp.dot(
            whole[:, cols_l], weights[cols_l, span], preferred_element_type=jnp.float32)

    def project_own(number, _):
        span = pl.ds(pl.multiple_of(number * span_w, span_w), span_w)
        mixer[:, span] = half_product(core, span)
        return 0

    lax.fori_loop(0, columns // span_w, project_own, 0)
    for copy in swap(1 - core):
        copy.wait_recv()

    def project(number, squares):
        span = pl.ds(pl.multiple_of(number * span_w, span_w), span_w)
        part = mixer[:, span] + half_product(1 - core, span)
        mixer[:, span] = part
        square = part * part
        return squares + functools.reduce(jnp.add, [square[:, j * 128:(j + 1) * 128] for j in range(span_w // 128)])

    squares = lax.fori_loop(0, columns // span_w, project, jnp.zeros((keep, 128), jnp.float32))
    mean = jnp.sum(squares, axis=-1, keepdims=True) * (1.0 / columns)
    mixed = (
        residual[...].astype(jnp.float32) + mixer[...] * lax.rsqrt(mean + norm_eps) * gain_mix[...]
    ).astype(jnp.bfloat16)
    mixed_ref[...] = mixed
    routed = rms_scale(mixed.astype(jnp.float32), gain_route[...])


    routed = routed.astype(jnp.bfloat16)
    slot_rows = lax.broadcasted_iota(jnp.int32, (slots, keep), 0).astype(jnp.float32)
    for group in range(depth):
        table_of = jnp.where((slot_rows == routing[1:2]) & (routing[0:1] == group), 1.0, 0.0).astype(jnp.bfloat16)
        out_rows[group] = jnp.dot(table_of, routed, preferred_element_type=jnp.float32).astype(jnp.bfloat16)
    in_rows[mine_z] = out_rows[mine_z]
    metas[mine_z] = out_meta[mine_z]

    parts = recv_rows.shape[1]
    plans, sends = plan_of(depth, parts)
    extent = columns // parts

    def columns_of(part):
        return pl.ds(part * extent, extent)

    def along_rows(other, slot, part):
        return pltpu.make_async_remote_copy(
            src_ref=out_rows.at[other, :, columns_of(part)], dst_ref=in_rows.at[slot, :, columns_of(part)],
            send_sem=send_rows.at[other, part], recv_sem=recv_rows.at[slot, part],
            device_id=(other * plane + me % plane, core), device_id_type=MESH)

    def along_meta(other, slot):
        return pltpu.make_async_remote_copy(
            src_ref=out_meta.at[other], dst_ref=metas.at[slot], send_sem=send_meta.at[other],
            recv_sem=recv_meta.at[slot], device_id=(other * plane + me % plane, core), device_id_type=MESH)

    def outward(source, other, slot, part):
        return pltpu.make_async_remote_copy(
            src_ref=spread.at[source, other, :, columns_of(part)],
            dst_ref=received.at[source, slot, :, columns_of(part)],
            send_sem=send_block.at[source, other, part], recv_sem=recv_block.at[source, slot, part],
            device_id=(mine_z * plane + other // cores, other % cores), device_id_type=MESH)

    def inward(source, other, slot, part):
        return pltpu.make_async_remote_copy(
            src_ref=outs.at[source, other, :, columns_of(part)],
            dst_ref=back.at[source, slot, :, columns_of(part)],
            send_sem=send_back.at[source, other, part], recv_sem=recv_back.at[source, slot, part],
            device_id=(mine_z * plane + other // cores, other % cores), device_id_type=MESH)

    def homeward(other, slot, part):
        return pltpu.make_async_remote_copy(
            src_ref=combined.at[other, :, columns_of(part)], dst_ref=final.at[slot, :, columns_of(part)],
            send_sem=send_home.at[other, part], recv_sem=recv_home.at[slot, part],
            device_id=(other * plane + me % plane, core), device_id_type=MESH)

    steps = distances(depth)
    for index in range(depth - 1):
        other = jnp.int32(0)
        for z in range(depth):
            other = jnp.where(mine_z == z, sends[z][index], other)
        along_meta(other, mine_z).start()
        for part in range(parts):
            along_rows(other, mine_z, part).start()

    def flat(ref, source, span):
        if capacity % 16:
            return jnp.concatenate(
                [ref[source, lane, :, span].astype(jnp.float32) for lane in range(lanes)], axis=0).astype(jnp.bfloat16)
        found = ref[source, :, :, span]
        return found.reshape(count, found.shape[2])

    def split(ref, source, values, span):
        for lane in range(lanes):
            ref[source, lane, :, span] = values[lane * capacity:(lane + 1) * capacity].astype(jnp.bfloat16)

    def expand(source, part):
        span = columns_of(part)

        def landed():
            if part == 0:
                along_meta(source, source).wait_recv()
            along_rows(source, source, part).wait_recv()

        pl.when(source != mine_z)(landed)
        wanted = lax.broadcasted_iota(jnp.int32, (count, slots), 0).astype(jnp.float32) + 1.0
        spots = jnp.where(
            (wanted == metas[source, 0:1, :slots]) | (wanted == metas[source, 1:2, :slots]), 1.0, 0.0
        ).astype(jnp.bfloat16)
        split(spread, source, jnp.dot(spots, in_rows[source, :, span], preferred_element_type=jnp.float32), span)
        received[source, here, :, span] = spread[source, here, :, span]
        for move in range(1, lanes):
            outward(source, (here + move) % lanes, here, part).start()

    tile = 256

    def compute(source):
        for part in range(parts):
            for move in range(1, lanes):
                outward(source, (here + move) % lanes, (here + move) % lanes, part).wait_recv()
        rows = flat(received, source, slice(None))

        def enter(number, _):
            span = pl.ds(pl.multiple_of(number * tile, tile), tile)
            gate = jnp.dot(rows, gate_w[:, span], preferred_element_type=jnp.float32)
            up = jnp.dot(rows, up_w[:, span], preferred_element_type=jnp.float32)
            hidden[:, span] = (jax.nn.silu(gate) * up).astype(jnp.bfloat16)
            return 0

        lax.fori_loop(0, gate_w.shape[1] // tile, enter, 0)
        for part in range(parts):

            def leave(number, _):
                span = pl.ds(pl.multiple_of(part * extent + number * 2 * tile, 2 * tile), 2 * tile)
                split(outs, source, jnp.dot(hidden[...], down_w[:, span], preferred_element_type=jnp.float32), span)
                return 0

            lax.fori_loop(0, extent // (2 * tile), leave, 0)
            span = columns_of(part)
            back[source, here, :, span] = outs[source, here, :, span]
            for move in range(1, lanes):
                inward(source, (here + move) % lanes, here, part).start()

    def combine(source, part):
        span = columns_of(part)
        for move in range(1, lanes):
            inward(source, (here + move) % lanes, (here + move) % lanes, part).wait_recv()
        wanted = lax.broadcasted_iota(jnp.int32, (count, width), 0).astype(jnp.float32) + 1.0
        shares = jnp.where(wanted == metas[source, 0:1, :], metas[source, 2:3, :], 0.0)
        shares = shares + jnp.where(wanted == metas[source, 1:2, :], metas[source, 3:4, :], 0.0)
        shares = shares.T[:slots]
        high = shares.astype(jnp.bfloat16)
        low = (shares - high.astype(jnp.float32)).astype(jnp.bfloat16)
        picked = flat(back, source, span)
        mixed = jnp.dot(high, picked, preferred_element_type=jnp.float32) + jnp.dot(
            low, picked, preferred_element_type=jnp.float32)

        def away():
            combined[source, :, span] = mixed.astype(jnp.bfloat16)
            homeward(source, mine_z, part).start()

        def stay():
            final[source, :, span] = mixed.astype(jnp.bfloat16)

        pl.when(source != mine_z)(away)
        pl.when(source == mine_z)(stay)


    def turn_of(turn, _):
        found = jnp.int32(0)
        for z in range(depth):
            for index, (kind, source) in enumerate(plans[z]):
                found = jnp.where((mine_z == z) & (turn == index), kind * depth + source, found)
        kind = found // depth
        source = found % depth
        pl.when(kind == 0)(lambda: compute(source))
        for part in range(parts):
            pl.when(kind == 1 + part)(functools.partial(expand, source, part))
            pl.when(kind == 1 + parts + part)(functools.partial(combine, source, part))
        return 0

    for load in expert_loads:
        load.wait()
    lax.fori_loop(0, (1 + 2 * parts) * depth, turn_of, 0)
    for step in steps[1:]:
        other = mine_z + step

        def settle(other=other):
            along_meta(other, mine_z).wait_send()
            for part in range(parts):
                homeward(other, other, part).wait_recv()
                homeward(other, mine_z, part).wait_send()
                along_rows(other, mine_z, part).wait_send()

        pl.when((other >= 0) & (other < depth))(settle)
    for source in range(depth):
        for move in range(1, lanes):
            for part in range(parts):
                outward(source, (here + move) % lanes, here, part).wait_send()
                inward(source, (here + move) % lanes, here, part).wait_send()
    for step in range(1, depth):

        def sent_up(step=step):
            for copy in far(step):
                copy.wait_send()

        pl.when(mine_z + step < depth)(sent_up)

    def sent(behind, _):
        for shard, target, slot in both_ways(behind):
            for copy in copies(shard, target, send_near.at[behind, slot]):
                copy.wait_send()
        for slot in range(near, near + near_y * near_x):
            for copy in copies(me, me, send_near.at[behind, slot]):
                copy.wait_send()

        def crossed(number, _):
            shard = (mine_z - behind) * plane + number
            pl.when(shard != me)(lambda: across(shard, core).wait_send())
            return 0

        lax.fori_loop(0, plane, crossed, 0)
        return 0

    lax.fori_loop(0, mine_z + 1, sent, 0)
    for copy in swap(core):
        copy.wait_send()
    eye = lax.broadcasted_iota(jnp.int32, (keep, keep), 0) == lax.broadcasted_iota(jnp.int32, (keep, keep), 1)
    slot_all = lax.broadcasted_iota(jnp.int32, (keep, depth * slots), 1).astype(jnp.float32)
    places = jnp.where(slot_all == as_column(routing[0:1] * slots + routing[1:2], eye), 1.0, 0.0).astype(jnp.bfloat16)
    blended = jnp.dot(places, final[...].reshape(depth * slots, columns), preferred_element_type=jnp.float32)
    result_ref[...] = (
        mixed_ref[...].astype(jnp.float32) + rms_scale(blended, gain_ref[...])
    ).astype(jnp.bfloat16)


def layer(dims, queries_small, queries_large, kv_small, kv_large, cum_small, cum_large, residual, gain_mix, gain_route, route, bias, gain_blend, out_small, out_large, w_gate, w_up, w_down):
    shards = lax.axis_size("sp")
    depth, rows_y, rows_x = dims
    tokens = queries_small.shape[0]
    heads_small = cum_small.shape[0]
    heads_large = cum_large.shape[0]
    size_small = kv_small.shape[1] // 2
    size_large = kv_large.shape[1] // 2
    heads = heads_small + heads_large
    extra_s = round_up(3 * heads_small, 32)
    extra_l = round_up(3 * heads_large, 16)
    table_rows = extra_s + 2 * size_small + 2 * size_large + extra_l
    near = rows_y + rows_x - 2 + (rows_y - 1) * (rows_x - 1)
    keep, columns = residual.shape
    lanes = lax.axis_size(("sp", "tp")) // depth
    capacity = 4 * keep // (depth * lanes)
    slots = capacity * lanes // 2
    width = round_up(slots, 128)
    parts = 2
    inner = w_gate.shape[2]
    joined = out_small.shape[0] + out_large.shape[0]
    dma = pltpu.SemaphoreType.DMA
    vmem = pl.BlockSpec(memory_space=pltpu.VMEM)
    hbm = pl.BlockSpec(memory_space=pltpu.HBM)
    bf16, f32 = jnp.bfloat16, jnp.float32
    rows = pltpu.VMEM((depth, slots, columns), bf16)
    blocks = pltpu.VMEM((depth, lanes, capacity, columns), bf16)
    meta = pltpu.VMEM((depth, 8, width), f32)
    scratch = [
        pltpu.VMEM(queries_small.shape, bf16),
        pltpu.VMEM(queries_large.shape, bf16),
        pltpu.VMEM(kv_small.shape, bf16),
        pltpu.VMEM(kv_large.shape, bf16),
        pltpu.VMEM(cum_small.shape, f32),
        pltpu.VMEM(cum_large.shape, f32),
        pltpu.VMEM(residual.shape, bf16),
        pltpu.VMEM((1, columns), f32),
        pltpu.VMEM((1, columns), f32),
        pltpu.VMEM(route.shape, route.dtype),
        pltpu.VMEM((1, keep), f32),
        pltpu.VMEM((1, columns), f32),
        pltpu.VMEM((shards, table_rows, tokens), bf16),
        pltpu.VMEM((shards, heads, tokens), f32),
        pltpu.VMEM((heads_small, tokens, extra_s + size_small), bf16),
        pltpu.VMEM((heads_large, tokens, size_large + extra_l), bf16),
        pltpu.VMEM((heads, tokens, 128), f32),
        pltpu.VMEM((heads, tokens, 128), f32),
        pltpu.VMEM((heads_small, tokens, size_small), f32),
        pltpu.VMEM((heads_large, tokens, size_large), f32),
        pltpu.VMEM((keep, heads_small * size_small + heads_large * size_large), bf16),
        pltpu.VMEM((keep, joined), bf16),
        pltpu.VMEM((joined, columns), bf16),
        pltpu.VMEM((keep, columns), f32),
        pltpu.VMEM((keep, columns), bf16),
        pltpu.VMEM((8, keep), f32),
        rows, rows, meta, meta, blocks, blocks, blocks, blocks, rows, rows,
        pltpu.VMEM((lanes * capacity, inner), bf16),
        pltpu.VMEM((columns, inner), bf16),
        pltpu.VMEM((columns, inner), bf16),
        pltpu.VMEM((inner, columns), bf16),
        dma((depth, 2)), dma((depth, near, 2)), dma((shards,)), dma((shards,)), dma((shards,)), dma((shards,)),
        dma((2,)), dma((2,)), dma((5,)), dma((12,)),
        dma((depth, parts)), dma((depth, parts)), dma((depth,)), dma((depth,)),
        dma((depth, lanes, parts)), dma((depth, lanes, parts)), dma((depth, lanes, parts)), dma((depth, lanes, parts)),
        dma((depth, parts)), dma((depth, parts)),
    ]
    return pl.pallas_call(
        functools.partial(layer_kernel, dims, (heads_small, heads_large, size_small, size_large)),
        out_shape=jax.ShapeDtypeStruct(residual.shape, bf16),
        in_specs=[hbm] * 17,
        out_specs=vmem,
        scratch_shapes=scratch,
        compiler_params=pltpu.CompilerParams(
            collective_id=0, has_side_effects=True, vmem_limit_bytes=66 * 1000 * 1000),
        name="layer",
    )(queries_small, queries_large, kv_small, kv_large, cum_small, cum_large, residual,
      gain_mix.reshape(1, columns), gain_route.reshape(1, columns), route, bias.reshape(1, keep),
      gain_blend.reshape(1, columns), out_small, out_large, w_gate, w_up, w_down)


def on_device(
    dims,
    queries_small,
    queries_large,
    kv_small,
    kv_large,
    cum_small,
    cum_large,
    residual,
    out_small,
    out_large,
    gain_mix,
    gain_route,
    gain_blend,
    w_gate,
    w_up,
    w_down,
    route,
    route_bias,
):
    return layer(
        dims, queries_small, queries_large, kv_small, kv_large, cum_small, cum_large, residual,
        gain_mix, gain_route, route, route_bias, gain_blend, out_small, out_large, w_gate, w_up, w_down,
    )


def solution(mesh):
    in_specs = (
        P("sp", "tp"),
        P("sp", "tp"),
        P("sp", None),
        P("sp", None),
        P("tp", "sp"),
        P("tp", "sp"),
        P(("sp", "tp"), None),
        P(),
        P(),
        P(),
        P(),
        P(),
        P(("sp", "tp"), None, None),
        P(("sp", "tp"), None, None),
        P(("sp", "tp"), None, None),
        P(None, ("sp", "tp")),
        P(("sp", "tp")),
    )
    out_specs = P(("sp", "tp"), None)
    return jax.shard_map(
        functools.partial(on_device, mesh_shape(mesh)), mesh=mesh, in_specs=in_specs, out_specs=out_specs, check_vma=False
    )
```
